128 devices in a mesh: sp: 16 (over z, x), tp: 8 (over y, core).
Axes of the slice: x: 4, y: 4, z: 4, core: 2. Of those that a mesh axis runs over, the one named last changes fastest.
Arguments:
- query_wide: bfloat16 [12288, 8, 256], P('sp', 'tp'), may hold values from -6 to 6
- key_wide: bfloat16 [12288, 8, 256], P('sp', 'tp'), may hold values from -6 to 6
- value_wide: bfloat16 [12288, 8, 256], P('sp', 'tp'), may hold values from -6 to 6
- query_narrow: bfloat16 [12288, 8, 128], P('sp', 'tp'), may hold values from -6 to 6
- key_narrow: bfloat16 [12288, 8, 128], P('sp', 'tp'), may hold values from -6 to 6
- value_narrow: bfloat16 [12288, 8, 128], P('sp', 'tp'), may hold values from -6 to 6
- mix_lambda: float32 [2, 8], P(None, 'tp'), may hold values from 0.3 to 0.8
- residual_in: bfloat16 [12288, 2048], P(('sp', 'tp')), may hold values from -6 to 6
- out_wide: bfloat16 [2048, 2048], P('tp'), may hold values from -0.109375 to 0.109375
- out_narrow: bfloat16 [1024, 2048], P('tp'), may hold values from -0.109375 to 0.109375
- ffn_gain: float32 [2048], replicated, may hold values from 0.1 to 1.9
- expert_ids: int32 [12288, 2], P(('sp', 'tp')), may hold values from 0 to 127, as said below
- expert_weights: float32 [12288, 2], P(('sp', 'tp')), may hold values from 0.1 to 1
- gate_weight: bfloat16 [128, 2048, 1024], P(('sp', 'tp')), may hold values from -0.125 to 0.125
- up_weight: bfloat16 [128, 2048, 1024], P(('sp', 'tp')), may hold values from -0.125 to 0.125
- down_weight: bfloat16 [128, 1024, 2048], P(('sp', 'tp')), may hold values from -0.1875 to 0.1875
Outputs:
- layer_out: bfloat16 [12288, 2048], P(('sp', 'tp'))
The draws below stay inside these ranges and needn't reach their ends.
Inputs may be any that keep to these rules, and one draw needn't show every extreme that they name: `expert_ids`: A row's two experts differ and lie in the same group of 4 consecutive experts (32 groups). In each aligned block of 96 rows (the rows of one device) no expert is named by more than 3 rows, and in every block some expert is named by exactly 3 rows.
All inputs are finite; a program needn't handle non-finite values.
Results may differ from the reference program's by a relative error of at most 0.015.
Values may be sent and summed in bfloat16 or wider, within the bound.
No kernel may reach another device: no remote copies, remote signals or barrier semaphores. Data moves between devices by JAX's collectives and lax.ppermute only.
A program may use at most 192 MiB of HBM per device.

```python
import math
import jax
import jax.numpy as jnp
from jax import lax

D = 2048
HEADS = 8
DA = 128
DB = 64
VA = 256
VB = 128
FF = 1024
GROUP_SIZE = 4
TOKENS = 12288
TOK_LOC = 96
EXPERTS = 128
CAP = 3


def query_draw(key, salt, head_size):
    values_drawn = jnp.clip(jax.random.normal(jax.random.fold_in(key, salt + 100), (TOKENS, HEADS, 2 * head_size), jnp.float32) * 1.3, -6.0, 6.0)
    return values_drawn.astype(jnp.bfloat16)


def key_draw(key, salt, head_size):
    values_drawn = jnp.clip(jax.random.normal(jax.random.fold_in(key, salt + 200), (TOKENS, HEADS, 2 * head_size), jnp.float32) * 1.3, -6.0, 6.0)
    return values_drawn.astype(jnp.bfloat16)


def draw_query_wide(key, part):
    return query_draw(key, 5, DA)


def draw_key_wide(key, part):
    return key_draw(key, 5, DA)


def draw_query_narrow(key, part):
    return query_draw(key, 9, DB)


def draw_key_narrow(key, part):
    return key_draw(key, 9, DB)


def draw_expert_ids(key, part):
    positions = EXPERTS * CAP // 2
    blocks = TOKENS // TOK_LOC
    forced = jax.random.randint(jax.random.fold_in(key, 31), (), 0, EXPERTS)
    pair_first = jnp.array([[0, 2], [0, 1], [0, 1]], jnp.int32)
    pair_second = jnp.array([[1, 3], [2, 3], [3, 2]], jnp.int32)

    def one_block(block_key):
        key_kind, key_score, key_order, key_flip = jax.random.split(block_key, 4)
        position = jnp.arange(positions, dtype=jnp.int32)
        group_index = position // (2 * CAP)
        level_index = position % (2 * CAP) // 2
        which_pair = position % 2
        pair_kind = jax.random.randint(key_kind, (EXPERTS // GROUP_SIZE, CAP), 0, 3)
        kinds = pair_kind[group_index, level_index]
        first_expert = pair_first[kinds, which_pair] + group_index * GROUP_SIZE
        second_expert = pair_second[kinds, which_pair] + group_index * GROUP_SIZE
        hit = ((first_expert == forced) | (second_expert == forced)).astype(jnp.int32)
        priority = jax.random.randint(key_score, (positions,), 0, 2 ** 20) * 1024 + position + hit * 2 ** 30
        _, chosen = lax.top_k(priority, TOK_LOC)
        shuffle = jax.random.permutation(key_order, TOK_LOC)
        picked = chosen[shuffle]
        flipped = jax.random.randint(key_flip, (TOK_LOC,), 0, 2)
        left_expert = first_expert[picked]
        right_expert = second_expert[picked]
        low_expert = jnp.where(flipped == 1, right_expert, left_expert)
        high_expert = jnp.where(flipped == 1, left_expert, right_expert)
        return jnp.stack([low_expert, high_expert], axis=-1)
    block_keys = jax.random.split(jax.random.fold_in(key, 32), blocks)
    return jax.vmap(one_block)(block_keys).reshape(TOKENS, 2).astype(jnp.int32)


def steps_of(stream_key, dims, cuts, smallest, top_value):
    gain, own = 1.0, jax.random.fold_in(stream_key, 6)
    for dim, shards_of in cuts:
        steps = jnp.exp(jax.random.uniform(jax.random.fold_in(own, dim), (shards_of,), jnp.float32, smallest / len(cuts), top_value / len(cuts)))
        gain = gain * jnp.repeat(steps, dims[dim] // shards_of).reshape([-1 if axis == dim else 1 for axis in range(len(dims))])
    return gain


def centred(stream_key, dims, spread, reach, pieces=(), kind=jnp.bfloat16):
    values = spread * jax.random.normal(stream_key, dims, jnp.float32)
    if pieces:
        values = values * steps_of(stream_key, dims, pieces, -0.22, 0.18)
    return jnp.clip(values, -reach, reach).astype(kind)


def setup_inputs(seed: int = 0) -> dict:
    streams_of = jax.random.split(jax.random.key(seed), 17)
    return {
        "query_wide": draw_query_wide(jax.random.fold_in(streams_of[16], 71), 0),
        "key_wide": draw_key_wide(jax.random.fold_in(streams_of[16], 71), 0),
        "value_wide": centred(streams_of[2], (TOKENS, HEADS, VA), 1.0, 6.0, ((0, 16), (1, 8))),
        "query_narrow": draw_query_narrow(jax.random.fold_in(streams_of[16], 71), 0),
        "key_narrow": draw_key_narrow(jax.random.fold_in(streams_of[16], 71), 0),
        "value_narrow": centred(streams_of[5], (TOKENS, HEADS, VB), 1.0, 6.0, ((0, 16), (1, 8))),
        "mix_lambda": jnp.clip(0.3 + 0.5 * jax.random.uniform(streams_of[6], (2, HEADS), jnp.float32) ** steps_of(streams_of[6], (2, HEADS), ((1, 8),), -0.2, 0.2), 0.3, 0.8),
        "residual_in": centred(streams_of[7], (TOKENS, D), 1.0, 6.0, ((0, 128),)),
        "out_wide": centred(streams_of[8], (HEADS * VA, D), (HEADS * VA + HEADS * VB) ** -0.5, 0.109375, ((0, 8),)),
        "out_narrow": centred(streams_of[9], (HEADS * VB, D), (HEADS * VA + HEADS * VB) ** -0.5, 0.109375, ((0, 8),)),
        "ffn_gain": jnp.clip(1.0 + 0.18 * jax.random.normal(streams_of[10], (D,), jnp.float32), 0.1, 1.9),
        "expert_ids": draw_expert_ids(jax.random.fold_in(streams_of[16], 71), 0),
        "expert_weights": jnp.clip(0.1 + 0.9 * jax.random.uniform(streams_of[12], (TOKENS, 2), jnp.float32) ** steps_of(streams_of[12], (TOKENS, 2), ((0, 128),), -0.2, 0.2), 0.1, 1.0),
        "gate_weight": centred(streams_of[13], (EXPERTS, D, FF), D ** -0.5, 0.125, ((0, 128),)),
        "up_weight": centred(streams_of[14], (EXPERTS, D, FF), D ** -0.5, 0.125, ((0, 128),)),
        "down_weight": centred(streams_of[15], (EXPERTS, FF, D), FF ** -0.5, 0.1875, ((0, 128),)),
    }


def head_group(query, keys, values, lam_row, head_size):
    score_scale = head_size ** (-0.5)
    query_block = math.gcd(TOKENS, 512)
    query_f = query.astype(jnp.float32)
    keys_f = keys.astype(jnp.float32)
    values_f = values.astype(jnp.float32)
    key_pos = jnp.arange(TOKENS, dtype=jnp.int32)

    def block_read(number):
        query_rows = lax.dynamic_slice_in_dim(query_f, number * query_block, query_block, 0)
        query_pos = number * query_block + jnp.arange(query_block, dtype=jnp.int32)
        causal = key_pos[None, :] <= query_pos[:, None]
        reads = []
        for which_map in range(2):
            lower_edge = which_map * head_size
            scores = jnp.einsum('qhd,khd->hqk', query_rows[..., lower_edge:lower_edge + head_size], keys_f[..., lower_edge:lower_edge + head_size]) * score_scale
            scores = jnp.where(causal[None], scores, -jnp.inf)
            new_peak = lax.optimization_barrier(jnp.max(scores, axis=-1, keepdims=True))
            expo = jnp.exp(scores - new_peak)
            totals = lax.optimization_barrier(jnp.sum(expo, axis=-1))
            rounded = lax.optimization_barrier(expo.astype(jnp.bfloat16)).astype(jnp.float32)
            reads.append(jnp.einsum('hqk,khv->hqv', rounded, values_f) / totals[..., None])
        mixed_read = reads[0] - lam_row[:, None, None] * reads[1]
        normed = mixed_read * lax.rsqrt(lax.optimization_barrier(jnp.mean(mixed_read * mixed_read, axis=-1, keepdims=True)) + 1e-06)
        return jnp.transpose(normed.astype(jnp.bfloat16), (1, 0, 2))
    outputs = lax.map(block_read, jnp.arange(TOKENS // query_block, dtype=jnp.int32))
    return outputs.reshape(TOKENS, -1)

def reference(query_wide, key_wide, value_wide, query_narrow, key_narrow, value_narrow, mix_lambda, residual_in, out_wide, out_narrow, ffn_gain, expert_ids, expert_weights, gate_weight, up_weight, down_weight):
    heads_wide = head_group(query_wide, key_wide, value_wide, mix_lambda[0], DA)
    heads_narrow = head_group(query_narrow, key_narrow, value_narrow, mix_lambda[1], DB)
    projected = jnp.dot(heads_wide, out_wide, preferred_element_type=jnp.float32) + jnp.dot(heads_narrow, out_narrow, preferred_element_type=jnp.float32)
    stream = (projected + residual_in.astype(jnp.float32)).astype(jnp.bfloat16)
    stream_f = stream.astype(jnp.float32)
    normed = (stream_f * lax.rsqrt(lax.optimization_barrier(jnp.mean(stream_f * stream_f, axis=-1, keepdims=True)) + 1e-06) * ffn_gain).astype(jnp.bfloat16)
    flat_expert = expert_ids.reshape(-1)
    flat_token = jnp.repeat(jnp.arange(TOKENS, dtype=jnp.int32), 2)
    flat_weight = expert_weights.reshape(-1)
    slots = EXPERTS * CAP

    def one_expert(running, expert):
        chosen = flat_expert == expert
        count = jnp.sum(chosen.astype(jnp.int32))
        position = jnp.nonzero(chosen, size=slots, fill_value=0)[0].astype(jnp.int32)
        token_rows = flat_token[position]
        rows = normed[token_rows]
        gate_part = jnp.dot(rows, gate_weight[expert], preferred_element_type=jnp.float32)
        up_part = jnp.dot(rows, up_weight[expert], preferred_element_type=jnp.float32)
        hidden = (jax.nn.silu(gate_part) * up_part).astype(jnp.bfloat16)
        result = jnp.dot(hidden, down_weight[expert], preferred_element_type=jnp.float32)
        result = lax.optimization_barrier(result.astype(jnp.bfloat16)).astype(jnp.float32)
        share = jnp.where(jnp.arange(slots, dtype=jnp.int32) < count, flat_weight[position], 0.0)
        return (running.at[token_rows].add(share[:, None] * result), None)
    summed, _ = lax.scan(one_expert, jnp.zeros((TOKENS, D), jnp.float32), jnp.arange(EXPERTS, dtype=jnp.int32))
    return (stream_f + summed).astype(jnp.bfloat16)
```

```python
import math

import jax
import jax.numpy as jnp
from jax import lax
from jax.experimental import pallas as pl
from jax.experimental.pallas import tpu as pltpu
from jax.sharding import Mesh
from jax.sharding import PartitionSpec as P

TP = ("y", "c")
SP_TP = ("z", "x", "y", "c")
RING = 4
LOG2E = 1.4426950408889634
NEG_FILL = -1e30
STAT_ROWS = 16


def attend_kernel(plan, q_ref, *refs, slots, size, width, q_block, chunk):
    k_refs = refs[:slots]
    v_refs = refs[slots : 2 * slots]
    out_ref = refs[2 * slots]
    q_scr, k_scr, v_scr, acc, out_scr, sems = refs[2 * slots + 1 :]
    first, last, diagonal = plan[0], plan[1], plan[2]
    active = plan[3]
    scale = size ** (-0.5) * LOG2E
    piece = min(q_block, chunk)

    def copies():
        made = [pltpu.make_async_copy(q_ref, q_scr, sems.at[0])]
        for s in range(slots):
            made.append(pltpu.make_async_copy(k_refs[s], k_scr.at[s], sems.at[1 + s]))
            made.append(pltpu.make_async_copy(v_refs[s], v_scr.at[s], sems.at[1 + slots + s]))
        return made

    @pl.when(active > 0)
    def _():
        for made in copies():
            made.start()
        for made in copies():
            made.wait()

        def one_query_block(number, _):
            q_rows = q_scr[pl.ds(number * q_block, q_block), :]
            if size % 128:
                lane = lax.broadcasted_iota(jnp.int32, q_rows.shape, 1)
                q_maps = [
                    jnp.where((lane >= m * size) & (lane < (m + 1) * size), q_rows, 0)
                    for m in range(2)
                ]
            else:
                q_maps = [q_rows[:, m * size : (m + 1) * size] for m in range(2)]
            acc[...] = jnp.zeros_like(acc)

            def advance(slot, start, length, masked, state):
                result = []
                for m in range(2):
                    peak, total = state[2 * m], state[2 * m + 1]
                    if size % 128:
                        rows = k_scr[slot, pl.ds(start, length), :]
                    else:
                        rows = k_scr[slot, pl.ds(start, length), m * size : (m + 1) * size]
                    scores = lax.dot_general(
                        rows, q_maps[m], (((1,), (1,)), ((), ())), preferred_element_type=jnp.float32
                    )
                    if masked:
                        key_pos = start + lax.broadcasted_iota(jnp.int32, scores.shape, 0)
                        query_pos = number * q_block + lax.broadcasted_iota(
                            jnp.int32, scores.shape, 1
                        )
                        scores = jnp.where(key_pos <= query_pos, scores, NEG_FILL)
                    new_peak = jnp.maximum(peak, jnp.max(scores, axis=0, keepdims=True) * scale)
                    factor = jnp.exp2(peak - new_peak)
                    weights = jnp.exp2(scores * scale - new_peak)
                    total = factor * total + jnp.sum(weights, axis=0, keepdims=True)
                    read = jnp.dot(
                        v_scr[slot, :, pl.ds(start, length)],
                        weights.astype(jnp.bfloat16),
                        preferred_element_type=jnp.float32,
                    )
                    acc[m] = acc[m] * factor + read
                    result += [new_peak, total]
                return tuple(result)

            empty = jnp.full((1, q_block), NEG_FILL, jnp.float32)
            none = jnp.zeros((1, q_block), jnp.float32)
            state = (empty, none, empty, none)

            def whole(number, state):
                slot = lax.rem(plan[4] + plan[5] * number + 8, slots) if slots > 1 else 0
                return advance(slot, 0, chunk, False, state)

            state = lax.fori_loop(first, last, whole, state)

            def part(inner, state):
                return advance(0, pl.multiple_of(inner * piece, piece), piece, True, state)

            state = lax.fori_loop(0, jnp.where(diagonal > 0, number + 1, 0), part, state)
            columns = pl.ds(pl.multiple_of(number * q_block, q_block), q_block)
            stats = []
            for m in range(2):
                peak, total = state[2 * m], state[2 * m + 1]
                out_scr[m * width : (m + 1) * width, columns] = (acc[m] / total).astype(jnp.bfloat16)
                level = peak + jnp.log2(total)
                for _ in range(3):
                    term = level.astype(jnp.bfloat16)
                    stats.append(term.astype(jnp.float32))
                    level = level - term.astype(jnp.float32)
            row = lax.broadcasted_iota(jnp.int32, (STAT_ROWS, q_block), 0)
            packed = jnp.zeros((STAT_ROWS, q_block), jnp.float32)
            for k, term in enumerate(stats):
                packed = jnp.where(row == k, term, packed)
            out_scr[2 * width :, columns] = packed.astype(jnp.bfloat16)
            return 0

        lax.fori_loop(0, chunk // q_block, one_query_block, 0)

    @pl.when(active == 0)
    def _():
        out_scr[: 2 * width, :] = jnp.zeros((2 * width, chunk), jnp.bfloat16)
        row = lax.broadcasted_iota(jnp.int32, (STAT_ROWS, chunk), 0)
        out_scr[2 * width :, :] = jnp.where((row == 0) | (row == 3), NEG_FILL, 0.0).astype(
            jnp.bfloat16
        )

    sent = pltpu.make_async_copy(out_scr, out_ref, sems.at[0])
    sent.start()
    sent.wait()


def attend(plan, queries, keys, values, size, name):
    slots = len(keys)
    chunk = queries.shape[0]
    width = values[0].shape[0]
    q_block = math.gcd(chunk, 256)
    body = lambda *refs: attend_kernel(
        *refs, slots=slots, size=size, width=width, q_block=q_block, chunk=chunk
    )
    area = chunk * chunk * slots * 2
    return pl.pallas_call(
        body,
        out_shape=jax.ShapeDtypeStruct((2 * width + STAT_ROWS, chunk), jnp.bfloat16),
        in_specs=[pl.BlockSpec(memory_space=pltpu.SMEM)]
        + [pl.BlockSpec(memory_space=pl.ANY)] * (1 + 2 * slots),
        out_specs=pl.BlockSpec(memory_space=pl.ANY),
        scratch_shapes=[
            pltpu.VMEM(queries.shape, jnp.bfloat16),
            pltpu.VMEM((slots,) + keys[0].shape, jnp.bfloat16),
            pltpu.VMEM((slots,) + values[0].shape, jnp.bfloat16),
            pltpu.VMEM((2, width, q_block), jnp.float32),
            pltpu.VMEM((2 * width + STAT_ROWS, chunk), jnp.bfloat16),
            pltpu.SemaphoreType.DMA((1 + 2 * slots,)),
        ],
        cost_estimate=pl.CostEstimate(
            flops=2 * area * (size + width),
            transcendentals=area,
            bytes_accessed=slots * chunk * 2 * (2 * size + width),
        ),
        name=name,
    )(plan, queries, *keys, *values)


def merge_kernel(valid, lam, *refs, widths, counts):
    out_ref = refs[-1]
    begin = 0
    column = 0
    for group, (width, count) in enumerate(zip(widths, counts)):
        parts = refs[begin : begin + count]
        begin += count
        reads = []
        for m in range(2):
            levels = []
            for k, part in enumerate(parts):
                stats = part[2 * width :, :].astype(jnp.float32)
                level = stats[3 * m : 3 * m + 1] + stats[3 * m + 1 : 3 * m + 2] + stats[
                    3 * m + 2 : 3 * m + 3
                ]
                levels.append(jnp.where(valid[group, k] > 0, level, NEG_FILL))
            top = levels[0]
            for level in levels[1:]:
                top = jnp.maximum(top, level)
            shares = [jnp.exp2(level - top) for level in levels]
            whole = shares[0]
            for share in shares[1:]:
                whole = whole + share
            read = None
            for share, part in zip(shares, parts):
                term = part[m * width : (m + 1) * width, :].astype(jnp.float32) * (share / whole)
                read = term if read is None else read + term
            reads.append(read)
        mixed = reads[0] - lam[group, 0] * reads[1]
        normed = mixed * lax.rsqrt(jnp.mean(mixed * mixed, axis=0, keepdims=True) + 1e-06)
        out_ref[:, column : column + width] = normed.T.astype(jnp.bfloat16)
        column += width


def merge(valid, lam, groups, widths):
    chunk = groups[0][0].shape[1]
    counts = [len(parts) for parts in groups]
    flat = [part for parts in groups for part in parts]
    body = lambda *refs: merge_kernel(*refs, widths=widths, counts=counts)
    block = math.gcd(chunk, 256)
    return pl.pallas_call(
        body,
        grid=(chunk // block,),
        out_shape=jax.ShapeDtypeStruct((chunk, sum(widths)), jnp.bfloat16),
        in_specs=[pl.BlockSpec(memory_space=pltpu.SMEM)] * 2
        + [pl.BlockSpec((part.shape[0], block), lambda i: (0, i)) for part in flat],
        out_specs=pl.BlockSpec((block, sum(widths)), lambda i: (i, 0)),
        name="merge_reads",
    )(valid, lam, *flat)


def around(array, axis, by):
    return lax.ppermute(array, axis, [(k, (k + by) % RING) for k in range(RING)])


def onward(array, axis, by):
    return lax.ppermute(
        array, axis, [(k, k + by) for k in range(RING) if 0 <= k + by < RING]
    )


def attention(
    query_wide, key_wide, value_wide, query_narrow, key_narrow, value_narrow, mix_lambda
):
    z = lax.axis_index("z")
    x = lax.axis_index("x")
    size_wide = query_wide.shape[1] // 2
    size_narrow = query_narrow.shape[1] // 2
    value_wide_t = value_wide.T
    value_narrow_t = value_narrow.T

    keys_near = around(key_wide, "x", 1)
    vals_near = around(value_wide_t, "x", 1)
    keys_back = around(key_wide, "x", -1)
    vals_back = around(value_wide_t, "x", -1)
    q_later = {d: onward(query_wide, "z", -d) for d in (3, 2, 1)}
    keys_far = around(keys_near, "x", 1)
    vals_far = around(vals_back, "x", -1)
    keys_below = [key_narrow] + [onward(key_narrow, "z", d) for d in (1, 2, 3)]
    vals_below = [value_narrow_t] + [onward(value_narrow_t, "z", d) for d in (1, 2, 3)]
    q_side = {s: around(query_narrow, "x", s) for s in (1, 2, 3)}

    keys_all = [key_wide, keys_near, keys_far, keys_back]
    vals_all = [value_wide_t, vals_near, vals_far, vals_back]

    def plan(*numbers):
        return jnp.stack([jnp.asarray(n, jnp.int32) for n in numbers])

    wide_parts = []
    for d in (3, 2, 1):
        there = (z + d < RING).astype(jnp.int32)
        made = attend(
            plan(0, RING, 0, there, x, -1), q_later[d], keys_all, vals_all, size_wide, f"wide_{d}"
        )
        wide_parts.append(onward(made, "z", d))
    narrow_parts = []
    for s in (1, 2, 3):
        source = lax.rem(x - s + RING, RING)
        own = (source > x).astype(jnp.int32)
        made = attend(
            plan(1 - own, z + 1, 0, ((z > 0) | (own > 0)), 0, 1),
            q_side[s],
            keys_below,
            vals_below,
            size_narrow,
            f"narrow_{s}",
        )
        narrow_parts.append(around(made, "x", -s))
    own_wide = attend(
        plan(0, x, 1, 1, x, -1), query_wide, keys_all, vals_all, size_wide, "wide_0"
    )
    own_narrow = attend(
        plan(1, z + 1, 1, 1, 0, 1), query_narrow, keys_below, vals_below, size_narrow, "narrow_0"
    )
    one = jnp.int32(1)
    valid = jnp.stack(
        [
            jnp.stack([one] + [(z >= d).astype(jnp.int32) for d in (3, 2, 1)]),
            jnp.stack([one] * 4),
        ]
    )
    return merge(
        valid,
        mix_lambda,
        ([own_wide] + wide_parts, [own_narrow] + narrow_parts),
        (value_wide.shape[1], value_narrow.shape[1]),
    )


def shards(
    query_wide,
    key_wide,
    value_wide,
    query_narrow,
    key_narrow,
    value_narrow,
    mix_lambda,
    residual_in,
    out_wide,
    out_narrow,
    ffn_gain,
    expert_ids,
    expert_weights,
    gate_weight,
    up_weight,
    down_weight,
):
    heads = attention(
        query_wide[:, 0],
        key_wide[:, 0],
        value_wide[:, 0],
        query_narrow[:, 0],
        key_narrow[:, 0],
        value_narrow[:, 0],
        mix_lambda,
    )
    tp_size = lax.axis_size(TP)
    local_rows = heads.shape[0] // tp_size
    out_both = lax.all_gather(
        jnp.concatenate([out_wide, out_narrow], axis=0), TP, axis=0, tiled=True
    )
    mine = lax.all_to_all(
        heads.reshape(tp_size, local_rows, -1), TP, split_axis=0, concat_axis=0, tiled=True
    )
    mine = jnp.transpose(mine, (1, 0, 2)).reshape(local_rows, -1)
    projected = jnp.dot(mine, out_both, preferred_element_type=jnp.float32)
    stream = (projected + residual_in.astype(jnp.float32)).astype(jnp.bfloat16)
    stream_f = stream.astype(jnp.float32)
    normed = (
        stream_f
        * lax.rsqrt(jnp.mean(stream_f * stream_f, axis=-1, keepdims=True) + 1e-06)
        * ffn_gain
    ).astype(jnp.bfloat16)
    experts_all = lax.axis_size(SP_TP)
    capacity = max(2, 4 * local_rows // experts_all)
    model_width = normed.shape[1]
    flat_expert = expert_ids.reshape(-1)
    expert_hot = (flat_expert[:, None] == jnp.arange(experts_all, dtype=jnp.int32)[None, :]).astype(
        jnp.int32
    )
    slot_rank = jnp.sum((jnp.cumsum(expert_hot, axis=0) - 1) * expert_hot, axis=1)
    flat_slot = flat_expert * capacity + slot_rank
    slot_ids = jnp.arange(experts_all * capacity, dtype=jnp.int32)
    placed = slot_ids[:, None] == flat_slot[None, :]
    dispatch = jnp.any(placed.reshape(experts_all * capacity, local_rows, 2), axis=2).astype(
        jnp.bfloat16
    )
    outgoing = jnp.dot(dispatch, normed, preferred_element_type=jnp.float32).astype(jnp.bfloat16)
    outgoing = outgoing.reshape(experts_all, capacity, model_width)
    arrived = lax.all_to_all(outgoing, SP_TP, split_axis=0, concat_axis=0, tiled=True)
    flat_rows = arrived.reshape(experts_all * capacity, model_width)
    gate_part = jnp.dot(flat_rows, gate_weight[0], preferred_element_type=jnp.float32)
    up_part = jnp.dot(flat_rows, up_weight[0], preferred_element_type=jnp.float32)
    hidden = (jax.nn.silu(gate_part) * up_part).astype(jnp.bfloat16)
    result = jnp.dot(hidden, down_weight[0], preferred_element_type=jnp.float32).astype(
        jnp.bfloat16
    )
    returned = lax.all_to_all(
        result.reshape(experts_all, capacity, model_width),
        SP_TP,
        split_axis=0,
        concat_axis=0,
        tiled=True,
    )
    slot_hot = (flat_slot[:, None] == slot_ids[None, :]).astype(
        jnp.float32
    ) * expert_weights.reshape(-1)[:, None]
    combine = jnp.sum(slot_hot.reshape(local_rows, 2, experts_all * capacity), axis=1)
    summed = jnp.dot(
        combine, returned.reshape(experts_all * capacity, model_width).astype(jnp.float32)
    )
    return (stream_f + summed).astype(jnp.bfloat16)


def solution(mesh):
    finer = Mesh(mesh.devices.reshape(4, 4, 4, 2), SP_TP)
    sp = ("z", "x")
    placed = (
        P(sp, TP, None),
        P(sp, TP, None),
        P(sp, TP, None),
        P(sp, TP, None),
        P(sp, TP, None),
        P(sp, TP, None),
        P(None, TP),
        P(SP_TP, None),
        P(TP, None),
        P(TP, None),
        P(),
        P(SP_TP, None),
        P(SP_TP, None),
        P(SP_TP, None, None),
        P(SP_TP, None, None),
        P(SP_TP, None, None),
    )
    return jax.shard_map(
        shards, mesh=finer, in_specs=placed, out_specs=P(SP_TP, None), check_vma=False
    )
```

```python
import jax
import jax.numpy as jnp
from jax import lax
from jax.experimental import pallas as pl
from jax.experimental.pallas import tpu as pltpu
from jax.sharding import Mesh
from jax.sharding import PartitionSpec as P

TP = ("y", "c")
SP_TP = ("z", "x", "y", "c")
RING = 4
LOG2E = 1.4426950408889634
NEG_FILL = -1e30
STAT_ROWS = 16
LANES = 128
BLOCK = 256
LEAST_TOTAL = 2.0**-60
MOST_TOTAL = 2.0**100


def pack_kernel(q_wide, k_wide, v_wide, q_narrow, k_narrow, v_narrow, x_out, z_out):
    chunk = q_wide.shape[0]
    half = chunk // 2
    width, width_narrow = v_wide.shape[1], v_narrow.shape[1]
    x_out[:chunk, :] = k_wide[...]
    z_out[:chunk, :] = q_wide[...]
    for j in range(chunk // BLOCK):
        rows = slice(j * BLOCK, (j + 1) * BLOCK)
        x_out[chunk + j * width : chunk + (j + 1) * width, :] = v_wide[rows, :].T
        begin = chunk + half + j * width_narrow
        z_out[begin : begin + width_narrow, :] = v_narrow[rows, :].T
    begin = chunk + chunk // BLOCK * width
    for side in range(2):
        lanes = slice(side * LANES, (side + 1) * LANES)
        x_out[begin : begin + half, lanes] = q_narrow[side * half : (side + 1) * half, :]
        z_out[chunk : chunk + half, lanes] = k_narrow[side * half : (side + 1) * half, :]


def pack(*arrays):
    chunk = arrays[0].shape[0]
    rows_x = chunk + chunk // BLOCK * arrays[2].shape[1] + chunk // 2
    rows_z = chunk + chunk // 2 + chunk // BLOCK * arrays[5].shape[1]
    return pl.pallas_call(
        pack_kernel,
        out_shape=(
            jax.ShapeDtypeStruct((rows_x, 2 * LANES), jnp.bfloat16),
            jax.ShapeDtypeStruct((rows_z, 2 * LANES), jnp.bfloat16),
        ),
        name="pack",
    )(*arrays)


def attend_kernel(plan, q_ref, *refs, slots, q_begin, wide, own, size, width, chunk):
    n_refs = sum(len(pieces) for pieces in slots)
    src_refs = refs[:n_refs]
    out_ref = refs[n_refs]
    q_scr, kv_scr, acc, out_scr, sems, q_sem = refs[n_refs + 1 :]
    active, count, offset = plan[0], plan[1], plan[2]
    scale = size ** (-0.5) * LOG2E
    key_rows = chunk if wide else chunk // 2
    total_rows = kv_scr.shape[1]

    def start_slot(slot):
        base = sum(len(pieces) for pieces in slots[:slot])
        begin = 0
        for k, (first, rows) in enumerate(slots[slot]):
            pltpu.make_async_copy(
                src_refs[base + k].at[pl.ds(first, rows), :],
                kv_scr.at[slot, pl.ds(begin, rows), :],
                sems.at[slot],
            ).start()
            begin += rows

    def wait_slot(slot):
        pltpu.make_async_copy(
            src_refs[0].at[pl.ds(slots[0][0][0], total_rows), :], kv_scr.at[slot], sems.at[slot]
        ).wait()

    def needed(slot):
        used = (slot >= offset) & (slot < offset + count)
        return used | (slot == 0) if own else used

    def maps_of(rows, m):
        if wide:
            return rows[:, m * size : (m + 1) * size]
        lane = lax.broadcasted_iota(jnp.int32, rows.shape, 1)
        return jnp.where((lane >= m * size) & (lane < (m + 1) * size), rows, 0)

    def scores_of(slot, queries, m):
        if wide:
            parts = [kv_scr[slot, :key_rows, m * size : (m + 1) * size]]
        else:
            parts = [
                kv_scr[slot, :key_rows, side * LANES : (side + 1) * LANES] for side in range(2)
            ]
        made = [
            lax.dot_general(part, queries, (((1,), (1,)), ((), ())), preferred_element_type=jnp.float32)
            for part in parts
        ]
        return made[0] if wide else jnp.concatenate(made, axis=0)

    def read_of(slot, weights):
        values = jnp.concatenate(
            [
                kv_scr[slot, key_rows + j * width : key_rows + (j + 1) * width, :]
                for j in range(chunk // BLOCK)
            ],
            axis=1,
        )
        return jnp.dot(values, weights, preferred_element_type=jnp.float32)

    def store_result(m, columns, read, total, level):
        out_scr[m * width : (m + 1) * width, columns] = (read * (1.0 / total)).astype(jnp.bfloat16)
        row = lax.broadcasted_iota(jnp.int32, (8, total.shape[1]), 0)
        packed = jnp.zeros((8, total.shape[1]), jnp.float32)
        for k in range(3):
            term = level.astype(jnp.bfloat16).astype(jnp.float32)
            packed = jnp.where(row == k, term, packed)
            level = level - term
        return packed

    @pl.when(active > 0)
    def _():
        got_q = pltpu.make_async_copy(q_ref.at[pl.ds(q_begin, q_scr.shape[0]), :], q_scr, q_sem)
        got_q.start()
        for slot in range(RING):
            pl.when(needed(slot))(lambda slot=slot: start_slot(slot))
        got_q.wait()

        def queries():
            if wide:
                return q_scr[...]
            return jnp.concatenate([q_scr[:, :LANES], q_scr[:, LANES:]], axis=0)

        def queries_at(number):
            halves = []
            for k in range(2):
                piece = number * 2 + k
                pieces = q_scr.shape[0] // LANES
                place = pl.ds(pl.multiple_of(lax.rem(piece, pieces) * LANES, LANES), LANES)
                halves.append(
                    jnp.where(piece < pieces, q_scr[place, :LANES], q_scr[place, LANES:])
                )
            return halves

        def add_slot(slot, totals, masked):
            result = []
            for m in range(2):
                scores = scores_of(slot, maps_of(queries(), m), m) * scale
                if masked:
                    key_pos = lax.broadcasted_iota(jnp.int32, scores.shape, 0)
                    query_pos = lax.broadcasted_iota(jnp.int32, scores.shape, 1)
                    scores = jnp.where(key_pos <= query_pos, scores, NEG_FILL)
                weights = jnp.exp2(scores)
                result.append(
                    totals[m] + jnp.sum(weights.reshape(chunk // 8, 8, chunk), axis=0)
                )
                acc[m] = acc[m] + read_of(slot, weights.astype(jnp.bfloat16))
            return tuple(result)

        acc[...] = jnp.zeros_like(acc)
        none = jnp.zeros((8, chunk), jnp.float32)
        totals = (none, none)
        if own:
            wait_slot(0)
            totals = add_slot(0, totals, True)

        def whole(number, totals):
            slot = number + offset
            wait_slot(slot)
            return add_slot(slot, totals, False)

        totals = lax.fori_loop(0, count, whole, totals)
        outside = jnp.zeros((1, chunk), jnp.float32)
        stats = []
        for m in range(2):
            total = jnp.sum(totals[m], axis=0, keepdims=True)
            inside = (total >= LEAST_TOTAL) & (total <= MOST_TOTAL)
            outside = jnp.maximum(outside, jnp.where(inside, 0.0, 1.0))
            stats.append(store_result(m, slice(None), acc[m], total, jnp.log2(total)))
        out_scr[2 * width :, :] = jnp.concatenate(stats, axis=0).astype(jnp.bfloat16)

        @pl.when(jnp.max(outside) > 0)
        def _():
            def one_query_block(number, _):
                begin = pl.multiple_of(number * BLOCK, BLOCK)
                if wide:
                    q_rows = q_scr[pl.ds(begin, BLOCK), :]
                else:
                    halves = queries_at(number)
                    q_rows = jnp.concatenate(halves, axis=0)

                def careful(slot, state):
                    result = []
                    for m in range(2):
                        peak, total, read = state[3 * m : 3 * m + 3]
                        scores = scores_of(slot, maps_of(q_rows, m), m) * scale
                        if own:
                            key_pos = lax.broadcasted_iota(jnp.int32, scores.shape, 0)
                            query_pos = begin + lax.broadcasted_iota(jnp.int32, scores.shape, 1)
                            limit = jnp.where(slot == 0, 0, chunk)
                            scores = jnp.where(key_pos <= query_pos + limit, scores, NEG_FILL)
                        new_peak = jnp.maximum(peak, jnp.max(scores, axis=0, keepdims=True))
                        factor = jnp.exp2(peak - new_peak)
                        weights = jnp.exp2(scores - new_peak)
                        result += [
                            new_peak,
                            factor * total + jnp.sum(weights, axis=0, keepdims=True),
                            factor * read + read_of(slot, weights.astype(jnp.bfloat16)),
                        ]
                    return tuple(result)

                empty = (
                    jnp.full((1, BLOCK), NEG_FILL, jnp.float32),
                    jnp.zeros((1, BLOCK), jnp.float32),
                    jnp.zeros((width, BLOCK), jnp.float32),
                )
                low = 0 if own else offset
                state = lax.fori_loop(low, offset + count, careful, empty + empty)
                columns = pl.ds(begin, BLOCK)
                stats = []
                for m in range(2):
                    peak, total, read = state[3 * m : 3 * m + 3]
                    stats.append(store_result(m, columns, read, total, peak + jnp.log2(total)))
                out_scr[2 * width :, columns] = jnp.concatenate(stats, axis=0).astype(jnp.bfloat16)
                return 0

            lax.fori_loop(0, chunk // BLOCK, one_query_block, 0)

    @pl.when(active == 0)
    def _():
        out_scr[: 2 * width, :] = jnp.zeros((2 * width, chunk), jnp.bfloat16)
        row = lax.broadcasted_iota(jnp.int32, (STAT_ROWS, chunk), 0)
        out_scr[2 * width :, :] = jnp.where((row == 0) | (row == 8), NEG_FILL, 0.0).astype(
            jnp.bfloat16
        )

    sent = pltpu.make_async_copy(out_scr, out_ref, q_sem)
    sent.start()
    sent.wait()


def attend(plan, queries, q_begin, sources, wide, own, size, width, chunk, name):
    slots = [[(first, rows) for _, first, rows in pieces] for pieces in sources]
    flat = [array for pieces in sources for array, _, _ in pieces]
    q_rows = chunk if wide else chunk // 2
    kv_rows = sum(rows for _, rows in slots[0])
    body = lambda *refs: attend_kernel(
        *refs,
        slots=slots,
        q_begin=q_begin,
        wide=wide,
        own=own,
        size=size,
        width=width,
        chunk=chunk,
    )
    area = chunk * chunk * 2 * 2
    return pl.pallas_call(
        body,
        out_shape=jax.ShapeDtypeStruct((2 * width + STAT_ROWS, chunk), jnp.bfloat16),
        in_specs=[pl.BlockSpec(memory_space=pltpu.SMEM)]
        + [pl.BlockSpec(memory_space=pl.ANY)] * (1 + len(flat)),
        out_specs=pl.BlockSpec(memory_space=pl.ANY),
        scratch_shapes=[
            pltpu.VMEM((q_rows, 2 * LANES), jnp.bfloat16),
            pltpu.VMEM((RING, kv_rows, 2 * LANES), jnp.bfloat16),
            pltpu.VMEM((2, width, chunk), jnp.float32),
            pltpu.VMEM((2 * width + STAT_ROWS, chunk), jnp.bfloat16),
            pltpu.SemaphoreType.DMA((RING,)),
            pltpu.SemaphoreType.DMA,
        ],
        cost_estimate=pl.CostEstimate(
            flops=2 * area * (size + width),
            transcendentals=area,
            bytes_accessed=RING * kv_rows * 512,
        ),
        name=name,
    )(plan, queries, *flat)


def merge_kernel(valid, lam, *refs, widths, counts):
    out_ref = refs[-1]
    begin = 0
    column = 0
    for group, (width, count) in enumerate(zip(widths, counts)):
        parts = refs[begin : begin + count]
        begin += count
        reads = []
        for m in range(2):
            levels = []
            for k, part in enumerate(parts):
                stats = part[2 * width :, :].astype(jnp.float32)
                level = stats[8 * m : 8 * m + 1] + stats[8 * m + 1 : 8 * m + 2] + stats[
                    8 * m + 2 : 8 * m + 3
                ]
                levels.append(jnp.where(valid[group, k] > 0, level, NEG_FILL))
            top = levels[0]
            for level in levels[1:]:
                top = jnp.maximum(top, level)
            shares = [jnp.exp2(level - top) for level in levels]
            whole = shares[0]
            for share in shares[1:]:
                whole = whole + share
            read = None
            for share, part in zip(shares, parts):
                term = part[m * width : (m + 1) * width, :].astype(jnp.float32) * (share / whole)
                read = term if read is None else read + term
            reads.append(read)
        mixed = reads[0] - lam[group, 0] * reads[1]
        normed = mixed * lax.rsqrt(jnp.mean(mixed * mixed, axis=0, keepdims=True) + 1e-06)
        out_ref[:, column : column + width] = normed.T.astype(jnp.bfloat16)
        column += width


def merge(valid, lam, groups, widths):
    chunk = groups[0][0].shape[1]
    counts = [len(parts) for parts in groups]
    flat = [part for parts in groups for part in parts]
    body = lambda *refs: merge_kernel(*refs, widths=widths, counts=counts)
    return pl.pallas_call(
        body,
        grid=(chunk // BLOCK,),
        out_shape=jax.ShapeDtypeStruct((chunk, sum(widths)), jnp.bfloat16),
        in_specs=[pl.BlockSpec(memory_space=pltpu.SMEM)] * 2
        + [pl.BlockSpec((part.shape[0], BLOCK), lambda i: (0, i)) for part in flat],
        out_specs=pl.BlockSpec((BLOCK, sum(widths)), lambda i: (i, 0)),
        name="merge_reads",
    )(valid, lam, *flat)


def around(array, axis, by):
    return lax.ppermute(array, axis, [(k, (k + by) % RING) for k in range(RING)])


def onward(array, axis, by):
    return lax.ppermute(
        array, axis, [(k, k + by) for k in range(RING) if 0 <= k + by < RING]
    )


def ring(array, axis, split):
    near = around(array, axis, 1)
    back = around(array, axis, -1)
    far_first = around(near[:split], axis, 1)
    far_second = around(back[split:], axis, -1)
    return near, back, far_first, far_second


def attention(
    query_wide, key_wide, value_wide, query_narrow, key_narrow, value_narrow, mix_lambda
):
    z = lax.axis_index("z")
    x = lax.axis_index("x")
    chunk = query_wide.shape[0]
    half = chunk // 2
    size_wide = query_wide.shape[1] // 2
    size_narrow = query_narrow.shape[1] // 2
    width_wide, width_narrow = value_wide.shape[1], value_narrow.shape[1]
    x_pack, z_pack = pack(query_wide, key_wide, value_wide, query_narrow, key_narrow, value_narrow)

    kv_wide = chunk + chunk // BLOCK * width_wide
    kv_narrow = half + chunk // BLOCK * width_narrow
    split = chunk + width_wide
    x_near, x_back, x_far_a, x_far_b = ring(x_pack, "x", split)
    z_near, z_back, z_far_a, z_far_b = ring(z_pack, "z", chunk)

    wide_sources = [
        [(x_pack, 0, kv_wide)],
        [(x_near, 0, kv_wide)],
        [(x_far_a, 0, split), (x_far_b, 0, kv_wide - split)],
        [(x_back, 0, kv_wide)],
    ]
    narrow_sources = [
        [(z_pack, chunk, kv_narrow)],
        [(z_near, chunk, kv_narrow)],
        [(z_far_b, 0, kv_narrow)],
        [(z_back, chunk, kv_narrow)],
    ]
    wide_queries = {0: z_pack, 1: z_back, 2: z_far_a, 3: z_near}
    narrow_queries = {
        0: (x_pack, kv_wide),
        1: (x_near, kv_wide),
        2: (x_far_b, kv_wide - split),
        3: (x_back, kv_wide),
    }

    def plan(*numbers):
        return jnp.stack([jnp.asarray(n, jnp.int32) for n in numbers])

    def wide(d):
        if d:
            numbers = plan((z + d < RING), RING, 0)
        else:
            numbers = plan(1, x, 1)
        return attend(
            numbers, wide_queries[d], 0, wide_sources, True, d == 0, size_wide, width_wide, chunk,
            f"wide_{d}",
        )

    def narrow(s):
        if s:
            level = (lax.rem(x - s + RING, RING) > x).astype(jnp.int32)
            numbers = plan((z > 0) | (level > 0), z + level, 1 - level)
        else:
            numbers = plan(1, z, 1)
        source, begin = narrow_queries[s]
        return attend(
            numbers, source, begin, narrow_sources, False, s == 0, size_narrow, width_narrow, chunk,
            f"narrow_{s}",
        )

    wide_parts, narrow_parts = [], []
    made = wide(2)
    made = lax.ppermute(made, "z", [(0, 3), (1, 2)])
    wide_parts.append(lax.ppermute(made, "z", [(3, 2), (2, 3)]))
    narrow_parts.append(around(narrow(2), "x", -2))
    wide_parts.append(onward(wide(1), "z", 1))
    narrow_parts.append(around(narrow(1), "x", -1))
    wide_parts.append(onward(wide(3), "z", 3))
    narrow_parts.append(around(narrow(3), "x", -3))
    own_wide = wide(0)
    own_narrow = narrow(0)
    one = jnp.int32(1)
    valid = jnp.stack(
        [
            jnp.stack([one] + [(z >= d).astype(jnp.int32) for d in (2, 1, 3)]),
            jnp.stack([one] * 4),
        ]
    )
    return merge(
        valid,
        mix_lambda,
        ([own_wide] + wide_parts, [own_narrow] + narrow_parts),
        (width_wide, width_narrow),
    )


def project_kernel(
    token_of, mine, weight, residual, gain, stream_out, rows_out, stream_scr, squares, flat_scr, rows
):
    step = pl.program_id(0)
    heads, tokens, depth = mine.shape
    columns = weight.shape[1]
    model = stream_scr.shape[1]
    tiles = model // LANES
    made = residual[...].astype(jnp.float32)
    for h in range(heads):
        made = made + jnp.dot(
            mine[h], weight[h * depth : (h + 1) * depth, :], preferred_element_type=jnp.float32
        )
    rounded = made.astype(jnp.bfloat16)
    stream_out[...] = rounded
    stream = rounded.astype(jnp.float32)
    stream_scr[:, pl.ds(pl.multiple_of(step * columns, columns), columns)] = stream
    square = jnp.sum(stream * stream, axis=1, keepdims=True)

    @pl.when(step == 0)
    def _():
        squares[...] = jnp.broadcast_to(square, squares.shape)

    @pl.when(step > 0)
    def _():
        squares[...] = squares[...] + square

    @pl.when(step == pl.num_programs(0) - 1)
    def _():
        inverse = lax.rsqrt(squares[...] / model + 1e-06)
        for j in range(tiles):
            lanes = slice(j * LANES, (j + 1) * LANES)
            flat_scr[pl.ds(j, tokens, stride=tiles), :] = (
                stream_scr[:, lanes] * inverse * gain[:, lanes]
            )
        rows[...] = flat_scr[...].reshape(tokens, tiles, LANES).astype(jnp.bfloat16)

        def copy_row(slot, _):
            rows_out[slot] = rows[token_of[slot]]
            return 0

        lax.fori_loop(0, rows_out.shape[0], copy_row, 0, unroll=16)


def project(token_of, mine, weight, residual, gain):
    heads, tokens, depth = mine.shape
    model = weight.shape[1]
    slots = token_of.shape[0]
    tiles = model // LANES
    columns = 2 * BLOCK
    return pl.pallas_call(
        project_kernel,
        grid=(model // columns,),
        out_shape=(
            jax.ShapeDtypeStruct((tokens, model), jnp.bfloat16),
            jax.ShapeDtypeStruct((slots, tiles, LANES), jnp.bfloat16),
        ),
        in_specs=[
            pl.BlockSpec(memory_space=pltpu.SMEM),
            pl.BlockSpec((heads, tokens, depth), lambda i: (0, 0, 0)),
            pl.BlockSpec((heads * depth, columns), lambda i: (0, i)),
            pl.BlockSpec((tokens, columns), lambda i: (0, i)),
            pl.BlockSpec((1, model), lambda i: (0, 0)),
        ],
        out_specs=(
            pl.BlockSpec((tokens, columns), lambda i: (0, i)),
            pl.BlockSpec((slots, tiles, LANES), lambda i: (0, 0, 0)),
        ),
        scratch_shapes=[
            pltpu.VMEM((tokens, model), jnp.float32),
            pltpu.VMEM((tokens, LANES), jnp.float32),
            pltpu.VMEM((tokens * tiles, LANES), jnp.float32),
            pltpu.VMEM((tokens, tiles, LANES), jnp.bfloat16),
        ],
        name="project",
    )(token_of, mine, weight, residual, gain)


def expert_kernel(
    arrived, gate, up, down, out, gate_scr, up_scr, down_scr, flat, rows, hidden, sems
):
    count, tiles, _ = arrived.shape
    model, inner = gate.shape
    steps = inner // BLOCK
    out_columns = model // steps

    def copies(k):
        part = pl.ds(k * BLOCK, BLOCK)
        return (
            pltpu.make_async_copy(gate.at[:, part], gate_scr.at[:, part], sems.at[3 * k]),
            pltpu.make_async_copy(up.at[:, part], up_scr.at[:, part], sems.at[3 * k + 1]),
        )

    def down_copy(k):
        part = pl.ds(k * out_columns, out_columns)
        return pltpu.make_async_copy(down.at[:, part], down_scr.at[:, part], sems.at[3 * k + 2])

    for k in range(steps):
        for made in copies(k):
            made.start()
    for k in range(steps):
        down_copy(k).start()
    flat[...] = arrived[...].astype(jnp.float32).reshape(count * tiles, LANES)
    for j in range(tiles):
        rows[:, j * LANES : (j + 1) * LANES] = flat[pl.ds(j, count, stride=tiles), :].astype(
            jnp.bfloat16
        )
    for k in range(steps):
        for made in copies(k):
            made.wait()
        part = slice(k * BLOCK, (k + 1) * BLOCK)
        gate_part = jnp.dot(rows[...], gate_scr[:, part], preferred_element_type=jnp.float32)
        up_part = jnp.dot(rows[...], up_scr[:, part], preferred_element_type=jnp.float32)
        hidden[:, part] = (gate_part * jax.nn.sigmoid(gate_part) * up_part).astype(jnp.bfloat16)
    for k in range(steps):
        down_copy(k).wait()
        result = jnp.dot(
            hidden[...],
            down_scr[:, k * out_columns : (k + 1) * out_columns],
            preferred_element_type=jnp.float32,
        )
        for j in range(out_columns // LANES):
            flat[pl.ds(k * out_columns // LANES + j, count, stride=tiles), :] = result[
                :, j * LANES : (j + 1) * LANES
            ]
    out[...] = flat[...].reshape(count, tiles, LANES).astype(jnp.bfloat16)


def experts(arrived, gate, up, down):
    count, tiles, _ = arrived.shape
    model, inner = gate.shape
    steps = inner // BLOCK
    return pl.pallas_call(
        expert_kernel,
        out_shape=jax.ShapeDtypeStruct(arrived.shape, jnp.bfloat16),
        in_specs=[pl.BlockSpec(memory_space=pltpu.VMEM)]
        + [pl.BlockSpec(memory_space=pl.ANY)] * 3,
        out_specs=pl.BlockSpec(memory_space=pltpu.VMEM),
        scratch_shapes=[
            pltpu.VMEM((model, inner), jnp.bfloat16),
            pltpu.VMEM((model, inner), jnp.bfloat16),
            pltpu.VMEM((inner, model), jnp.bfloat16),
            pltpu.VMEM((count * tiles, LANES), jnp.float32),
            pltpu.VMEM((count, model), jnp.bfloat16),
            pltpu.VMEM((count, inner), jnp.bfloat16),
            pltpu.SemaphoreType.DMA((3 * steps,)),
        ],
        name="experts",
    )(arrived, gate, up, down)


def combine_kernel(slot_of, share_of, returned, stream, out, flat):
    tokens, model = stream.shape
    tiles = model // LANES

    def one_token(token, _):
        total = share_of[2 * token] * returned[slot_of[2 * token]].astype(jnp.float32)
        total = total + share_of[2 * token + 1] * returned[slot_of[2 * token + 1]].astype(
            jnp.float32
        )
        flat[pl.ds(pl.multiple_of(token * tiles, tiles), tiles), :] = total
        return 0

    lax.fori_loop(0, tokens, one_token, 0, unroll=8)
    for j in range(tiles):
        lanes = slice(j * LANES, (j + 1) * LANES)
        out[:, lanes] = (
            stream[:, lanes].astype(jnp.float32) + flat[pl.ds(j, tokens, stride=tiles), :]
        ).astype(jnp.bfloat16)


def combine(slot_of, share_of, returned, stream):
    tokens, model = stream.shape
    return pl.pallas_call(
        combine_kernel,
        out_shape=jax.ShapeDtypeStruct(stream.shape, jnp.bfloat16),
        in_specs=[pl.BlockSpec(memory_space=pltpu.SMEM)] * 2
        + [pl.BlockSpec(memory_space=pltpu.VMEM)] * 2,
        out_specs=pl.BlockSpec(memory_space=pltpu.VMEM),
        scratch_shapes=[pltpu.VMEM((tokens * (model // LANES), LANES), jnp.float32)],
        name="combine",
    )(slot_of, share_of, returned, stream)


def slot_tables(expert_ids, experts_all, capacity):
    flat_expert = expert_ids.reshape(-1)
    order = jnp.arange(flat_expert.shape[0], dtype=jnp.int32)
    earlier = (flat_expert[:, None] == flat_expert[None, :]) & (order[None, :] < order[:, None])
    slot_of = flat_expert * capacity + jnp.sum(earlier.astype(jnp.int32), axis=1)
    slot_ids = jnp.arange(experts_all * capacity, dtype=jnp.int32)
    placed = slot_ids[:, None] == slot_of[None, :]
    token_of = jnp.sum(jnp.where(placed, order[None, :] // 2, 0), axis=1)
    return slot_of, token_of


def shards(
    query_wide,
    key_wide,
    value_wide,
    query_narrow,
    key_narrow,
    value_narrow,
    mix_lambda,
    residual_in,
    out_wide,
    out_narrow,
    ffn_gain,
    expert_ids,
    expert_weights,
    gate_weight,
    up_weight,
    down_weight,
):
    heads = attention(
        query_wide[:, 0],
        key_wide[:, 0],
        value_wide[:, 0],
        query_narrow[:, 0],
        key_narrow[:, 0],
        value_narrow[:, 0],
        mix_lambda,
    )
    tp_size = lax.axis_size(TP)
    local_rows = heads.shape[0] // tp_size
    experts_all = lax.axis_size(SP_TP)
    capacity = max(2, 4 * local_rows // experts_all)
    slot_of, token_of = slot_tables(expert_ids, experts_all, capacity)
    out_both = lax.all_gather(
        jnp.concatenate([out_wide, out_narrow], axis=0), TP, axis=0, tiled=True
    )
    mine = lax.all_to_all(
        heads.reshape(tp_size, local_rows, -1), TP, split_axis=0, concat_axis=0, tiled=True
    )
    stream, outgoing = project(token_of, mine, out_both, residual_in, ffn_gain[None, :])

    def exchanged(rows):
        shape = rows.shape
        moved = lax.all_to_all(
            rows.reshape(experts_all, -1, LANES), SP_TP, split_axis=0, concat_axis=0, tiled=True
        )
        return moved.reshape(shape)

    result = experts(exchanged(outgoing), gate_weight[0], up_weight[0], down_weight[0])
    return combine(slot_of, expert_weights.reshape(-1), exchanged(result), stream)


def solution(mesh):
    finer = Mesh(mesh.devices.reshape(4, 4, 4, 2), SP_TP)
    sp = ("z", "x")
    placed = (
        P(sp, TP, None),
        P(sp, TP, None),
        P(sp, TP, None),
        P(sp, TP, None),
        P(sp, TP, None),
        P(sp, TP, None),
        P(None, TP),
        P(SP_TP, None),
        P(TP, None),
        P(TP, None),
        P(),
        P(SP_TP, None),
        P(SP_TP, None),
        P(SP_TP, None, None),
        P(SP_TP, None, None),
        P(SP_TP, None, None),
    )
    return jax.shard_map(
        shards, mesh=finer, in_specs=placed, out_specs=P(SP_TP, None), check_vma=False
    )
```

```python
import jax
import jax.numpy as jnp
from jax import lax
from jax.experimental import pallas as pl
from jax.experimental.pallas import tpu as pltpu
from jax.sharding import Mesh
from jax.sharding import PartitionSpec as P

TP = ("y", "c")
SP_TP = ("z", "x", "y", "c")
RING = 4
LOG2E = 1.4426950408889634
NEG_FILL = -1e30
STAT_ROWS = 16
LANES = 128
BLOCK = 256
SOME = 48
LEAST_TOTAL = 2.0**-60
MOST_TOTAL = 2.0**100


def pack_kernel(v_wide, k_narrow, v_narrow, v_out, kv_out):
    chunk, width = v_wide.shape
    half = chunk // 2
    width_narrow = v_narrow.shape[1]
    for j in range(chunk // BLOCK):
        rows = slice(j * BLOCK, (j + 1) * BLOCK)
        v_out[j * width : (j + 1) * width, :] = v_wide[rows, :].T
        begin = half + j * width_narrow
        kv_out[begin : begin + width_narrow, :] = v_narrow[rows, :].T
    for side in range(2):
        lanes = slice(side * LANES, (side + 1) * LANES)
        kv_out[:half, lanes] = k_narrow[side * half : (side + 1) * half, :]


def pack(v_wide, k_narrow, v_narrow):
    chunk, width = v_wide.shape
    rows = chunk // 2 + chunk // BLOCK * v_narrow.shape[1]
    return pl.pallas_call(
        pack_kernel,
        out_shape=(
            jax.ShapeDtypeStruct((chunk // BLOCK * width, BLOCK), jnp.bfloat16),
            jax.ShapeDtypeStruct((rows, BLOCK), jnp.bfloat16),
        ),
        name="pack",
    )(v_wide, k_narrow, v_narrow)


def attend_kernel(plan, q_ref, *refs, pieces, wide, diagonal, fill, size, width, chunk):
    slots = len(refs[: -7]) // pieces
    src_refs = refs[: slots * pieces]
    out_ref = refs[slots * pieces]
    q_scr, kv_scr, acc, out_scr, sems, q_sem = refs[slots * pieces + 1 :]
    active, count, offset = plan[0], plan[1], plan[2]
    scale = size ** (-0.5) * LOG2E
    key_rows = chunk if wide else chunk // 2
    halves = key_rows // LANES

    def slot_copies(slot):
        made = []
        begin = 0
        for k in range(pieces):
            source = src_refs[slot * pieces + k]
            rows = source.shape[0]
            made.append(
                pltpu.make_async_copy(
                    source, kv_scr.at[slot, pl.ds(begin, rows), :], sems.at[slot, k]
                )
            )
            begin += rows
        return made

    def wait_slot(slot):
        begin = 0
        for k in range(pieces):
            source = src_refs[k]
            rows = source.shape[0]
            pltpu.make_async_copy(
                source, kv_scr.at[slot, pl.ds(begin, rows), :], sems.at[slot, k]
            ).wait()
            begin += rows

    def only_map(rows, m):
        lane = lax.broadcasted_iota(jnp.int32, rows.shape, 1)
        return jnp.where((lane >= m * size) & (lane < (m + 1) * size), rows, 0)

    def dot_nt(left, right):
        return lax.dot_general(
            left, right, (((1,), (1,)), ((), ())), preferred_element_type=jnp.float32
        )

    def value_block(slot, j):
        return kv_scr[slot, pl.ds(key_rows + j * width, width), :]

    def store_result(m, columns, read, total, level):
        out_scr[pl.ds(m * width, width), columns] = (read * (1.0 / total)).astype(jnp.bfloat16)
        row = lax.broadcasted_iota(jnp.int32, (8, total.shape[1]), 0)
        packed = jnp.zeros((8, total.shape[1]), jnp.float32)
        for k in range(3):
            term = level.astype(jnp.bfloat16).astype(jnp.float32)
            packed = jnp.where(row == k, term, packed)
            level = level - term
        return packed

    @pl.when(active > 0)
    def _():
        got_q = pltpu.make_async_copy(q_ref, q_scr, q_sem)
        got_q.start()
        for slot in range(slots):

            @pl.when((slot >= offset) & (slot < offset + count))
            def _(slot=slot):
                for made in slot_copies(slot):
                    made.start()

        acc[...] = jnp.zeros_like(acc)
        got_q.wait()

        def add_slot(number, totals):
            slot = 0 if diagonal else number + offset
            wait_slot(slot)
            values = jnp.concatenate(
                [value_block(slot, j) for j in range(chunk // BLOCK)], axis=1
            )
            result = []
            for m in range(2):
                if wide:
                    lanes = slice(m * size, (m + 1) * size)
                    scores = dot_nt(kv_scr[slot, :key_rows, lanes], q_scr[:, lanes])
                else:
                    queries = only_map(q_scr[...], m)
                    scores = jnp.concatenate(
                        [
                            dot_nt(kv_scr[slot, :key_rows, side * LANES : (side + 1) * LANES], queries)
                            for side in range(2)
                        ],
                        axis=0,
                    )
                scores = scores * scale
                if diagonal:
                    key_pos = lax.broadcasted_iota(jnp.int32, scores.shape, 0)
                    query_pos = lax.broadcasted_iota(jnp.int32, scores.shape, 1)
                    scores = jnp.where(key_pos <= query_pos, scores, NEG_FILL)
                weights = jnp.exp2(scores)
                result.append(totals[m] + jnp.sum(weights.reshape(chunk // 8, 8, chunk), axis=0))
                acc[m] = acc[m] + jnp.dot(
                    values, weights.astype(jnp.bfloat16), preferred_element_type=jnp.float32
                )
            return tuple(result)

        none = jnp.zeros((8, chunk), jnp.float32)
        if diagonal:
            totals = add_slot(0, (none, none))
        else:
            totals = lax.fori_loop(0, count, add_slot, (none, none))
        outside = jnp.zeros((1, chunk), jnp.float32)
        stats = []
        for m in range(2):
            total = jnp.sum(totals[m], axis=0, keepdims=True)
            inside = (total >= LEAST_TOTAL) & (total <= MOST_TOTAL)
            outside = jnp.maximum(outside, jnp.where(inside, 0.0, 1.0))
            stats.append(store_result(m, slice(None), acc[m], total, jnp.log2(total)))
        out_scr[2 * width :, :] = jnp.concatenate(stats, axis=0).astype(jnp.bfloat16)

        @pl.when(jnp.max(outside) > 0)
        def _():
            def packed_rows(take, number):
                made = []
                for k in range(2):
                    piece = number * 2 + k
                    place = pl.ds(pl.multiple_of(lax.rem(piece, halves) * LANES, LANES), LANES)
                    first, second = take(place)
                    made.append(jnp.where(piece < halves, first, second))
                return jnp.concatenate(made, axis=0)

            def keys_at(slot, number):
                return packed_rows(
                    lambda place: (kv_scr[slot, place, :LANES], kv_scr[slot, place, LANES:]), number
                )

            def one_query_block(number, _):
                begin = pl.multiple_of(number * BLOCK, BLOCK)
                columns = pl.ds(begin, BLOCK)

                def one_map(m, packed):
                    acc[m, :, columns] = jnp.zeros((width, BLOCK), jnp.float32)

                    def careful(index, state):
                        peak, total = state
                        slot = index // (chunk // BLOCK) + offset
                        block = lax.rem(index, chunk // BLOCK)
                        place = pl.ds(pl.multiple_of(block * BLOCK, BLOCK), BLOCK)
                        if wide:
                            lanes = pl.ds(pl.multiple_of(m * size, size), size)
                            scores = dot_nt(kv_scr[slot, place, lanes], q_scr[columns, lanes])
                        else:
                            scores = dot_nt(keys_at(slot, block), only_map(q_scr[columns, :], m))
                        scores = scores * scale
                        if diagonal:
                            key_pos = block * BLOCK + lax.broadcasted_iota(
                                jnp.int32, scores.shape, 0
                            )
                            query_pos = begin + lax.broadcasted_iota(jnp.int32, scores.shape, 1)
                            scores = jnp.where(key_pos <= query_pos, scores, NEG_FILL)
                        new_peak = jnp.maximum(peak, jnp.max(scores, axis=0, keepdims=True))
                        factor = jnp.exp2(peak - new_peak)
                        weights = jnp.exp2(scores - new_peak)
                        acc[m, :, columns] = factor * acc[m, :, columns] + jnp.dot(
                            value_block(slot, block),
                            weights.astype(jnp.bfloat16),
                            preferred_element_type=jnp.float32,
                        )
                        return new_peak, factor * total + jnp.sum(weights, axis=0, keepdims=True)

                    peak, total = lax.fori_loop(
                        0,
                        count * (chunk // BLOCK),
                        careful,
                        (
                            jnp.full((1, BLOCK), NEG_FILL, jnp.float32),
                            jnp.zeros((1, BLOCK), jnp.float32),
                        ),
                    )
                    rows = store_result(
                        m, columns, acc[m, :, columns], total, peak + jnp.log2(total)
                    )
                    both = jnp.concatenate([rows, rows], axis=0)
                    row = lax.broadcasted_iota(jnp.int32, both.shape, 0)
                    return jnp.where((row >= 8 * m) & (row < 8 * m + 8), both, packed)

                packed = lax.fori_loop(
                    0, 2, one_map, jnp.zeros((STAT_ROWS, BLOCK), jnp.float32)
                )
                out_scr[2 * width :, columns] = packed.astype(jnp.bfloat16)
                return 0

            lax.fori_loop(0, chunk // BLOCK, one_query_block, 0)

    if fill:

        @pl.when(active == 0)
        def _():
            out_scr[...] = jnp.zeros_like(out_scr)

    @pl.when((active > 0) | fill)
    def _():
        sent = pltpu.make_async_copy(out_scr, out_ref, q_sem)
        sent.start()
        sent.wait()


def attend(plan, queries, sources, wide, diagonal, fill, size, width):
    chunk = queries.shape[0]
    pieces = len(sources[0])
    flat = [array for group in sources for array in group]
    kv_rows = sum(array.shape[0] for array in sources[0])
    body = lambda *refs: attend_kernel(
        *refs,
        pieces=pieces,
        wide=wide,
        diagonal=diagonal,
        fill=fill,
        size=size,
        width=width,
        chunk=chunk,
    )
    area = chunk * chunk * 2 * 2
    return pl.pallas_call(
        body,
        out_shape=jax.ShapeDtypeStruct((2 * width + STAT_ROWS, chunk), jnp.bfloat16),
        in_specs=[pl.BlockSpec(memory_space=pltpu.SMEM)]
        + [pl.BlockSpec(memory_space=pl.ANY)] * (1 + len(flat)),
        out_specs=pl.BlockSpec(memory_space=pl.ANY),
        scratch_shapes=[
            pltpu.VMEM(queries.shape, jnp.bfloat16),
            pltpu.VMEM((len(sources), kv_rows, BLOCK), jnp.bfloat16),
            pltpu.VMEM((2, width, chunk), jnp.float32),
            pltpu.VMEM((2 * width + STAT_ROWS, chunk), jnp.bfloat16),
            pltpu.SemaphoreType.DMA((len(sources), pieces)),
            pltpu.SemaphoreType.DMA,
        ],
        cost_estimate=pl.CostEstimate(
            flops=2 * area * (size + width),
            transcendentals=area,
            bytes_accessed=len(sources) * kv_rows * 512,
        ),
    )(plan, queries, *flat)


def merge_kernel(valid, lam, *refs, widths, counts):
    out_ref = refs[-1]
    guarded = (1, None)
    begin = 0
    column = 0
    for group, (width, count) in enumerate(zip(widths, counts)):
        parts = refs[begin : begin + count]
        begin += count
        reads = []
        for m in range(2):
            levels = []
            for k, part in enumerate(parts):
                stats = part[2 * width :, :].astype(jnp.float32)
                level = stats[8 * m : 8 * m + 1] + stats[8 * m + 1 : 8 * m + 2] + stats[
                    8 * m + 2 : 8 * m + 3
                ]
                levels.append(jnp.where(valid[group, k] > 0, level, NEG_FILL))
            top = levels[0]
            for level in levels[1:]:
                top = jnp.maximum(top, level)
            shares = [jnp.exp2(level - top) for level in levels]
            whole = shares[0]
            for share in shares[1:]:
                whole = whole + share
            read = None
            for k, (share, part) in enumerate(zip(shares, parts)):
                term = part[m * width : (m + 1) * width, :].astype(jnp.float32) * (share / whole)
                if read is None:
                    read = term
                elif guarded[group] == k:
                    read = read + jnp.where(valid[group, k] > 0, term, 0.0)
                else:
                    read = read + term
            reads.append(read)
        mixed = reads[0] - lam[group, 0] * reads[1]
        normed = mixed * lax.rsqrt(jnp.mean(mixed * mixed, axis=0, keepdims=True) + 1e-06)
        out_ref[:, column : column + width] = normed.T.astype(jnp.bfloat16)
        column += width


def merge(valid, lam, groups, widths):
    chunk = groups[0][0].shape[1]
    counts = [len(parts) for parts in groups]
    flat = [part for parts in groups for part in parts]
    body = lambda *refs: merge_kernel(*refs, widths=widths, counts=counts)
    return pl.pallas_call(
        body,
        grid=(chunk // BLOCK,),
        out_shape=jax.ShapeDtypeStruct((chunk, sum(widths)), jnp.bfloat16),
        in_specs=[pl.BlockSpec(memory_space=pltpu.SMEM)] * 2
        + [pl.BlockSpec((part.shape[0], BLOCK), lambda i: (0, i)) for part in flat],
        out_specs=pl.BlockSpec((BLOCK, sum(widths)), lambda i: (i, 0)),
        name="merge_reads",
    )(valid, lam, *flat)


def around(array, axis, by):
    return lax.ppermute(array, axis, [(k, (k + by) % RING) for k in range(RING)])


def onward(array, axis, by):
    return lax.ppermute(
        array, axis, [(k, k + by) for k in range(RING) if 0 <= k + by < RING]
    )


def after(array, *others):
    return lax.optimization_barrier((array,) + others)[0]


def attention(
    query_wide, key_wide, value_wide, query_narrow, key_narrow, value_narrow, mix_lambda
):
    z = lax.axis_index("z")
    x = lax.axis_index("x")
    size_wide = query_wide.shape[1] // 2
    size_narrow = query_narrow.shape[1] // 2
    width_wide, width_narrow = value_wide.shape[1], value_narrow.shape[1]

    xk_near = around(key_wide, "x", 1)
    q_later = {d: onward(query_wide, "z", -d) for d in (1, 2, 3)}
    values, kv_narrow = pack(value_wide, key_narrow, value_narrow)
    xv_back = around(values, "x", -1)
    xv_near = around(values, "x", 1)
    xk_back = around(key_wide, "x", -1)
    kv_below = {d: onward(kv_narrow, "z", d) for d in (1, 2, 3)}
    xk_far = around(xk_near, "x", 1)
    xv_far = around(xv_back, "x", -1)
    q_side = {s: around(query_narrow, "x", s) for s in (1, 2, 3)}

    wide_sources = [(key_wide, values), (xk_near, xv_near), (xk_far, xv_far), (xk_back, xv_back)]
    narrow_sources = [(kv_narrow,)] + [(kv_below[d],) for d in (1, 2, 3)]

    def plan(*numbers):
        return jnp.stack([jnp.asarray(n, jnp.int32) for n in numbers])

    def wide(numbers, queries, sources, diagonal):
        return attend(numbers, queries, sources, True, diagonal, False, size_wide, width_wide)

    def narrow(numbers, queries, sources, diagonal, fill):
        return attend(numbers, queries, sources, False, diagonal, fill, size_narrow, width_narrow)

    one = jnp.int32(1)
    diag_wide = wide(plan(1, 1, 0), query_wide, wide_sources[:1], True)
    diag_narrow = narrow(
        after(plan(1, 1, 0), diag_wide), query_narrow, narrow_sources[:1], True, False,
    )
    last = diag_narrow
    made = {}
    for d in (2, 1, 3):
        numbers = plan((z + d < RING), RING, 0)
        last = wide(after(numbers, last), q_later[d], wide_sources, False)
        made[d] = last
    relayed = lax.ppermute(made[2], "z", [(0, 3), (1, 2)])
    sent = {d: onward(made[d], "z", d) for d in (1, 3)}
    narrow_parts = []
    for s in (2, 1, 3):
        level = (lax.rem(x - s + RING, RING) > x).astype(jnp.int32)
        numbers = plan((z > 0) | (level > 0), z + level, 1 - level)
        last = narrow(after(numbers, last), q_side[s], narrow_sources, False, True)
        narrow_parts.append(around(last, "x", -s))
    sent[2] = lax.ppermute(after(relayed, last), "z", [(3, 2), (2, 3)])
    rest_narrow = narrow(
        after(plan((z > 0), z, 1), last), query_narrow, narrow_sources, False, True
    )
    rest_wide = wide(after(plan((x > 0), x, 1), rest_narrow), query_wide, wide_sources, False)
    valid = jnp.stack(
        [
            jnp.stack([one, x > 0] + [z >= d for d in (2, 1, 3)]).astype(jnp.int32),
            jnp.stack(
                [one, z > 0] + [(z > 0) | (lax.rem(x + s, RING) < x) for s in (2, 1, 3)]
            ).astype(jnp.int32),
        ]
    )
    return merge(
        valid,
        mix_lambda,
        (
            [diag_wide, rest_wide] + [sent[d] for d in (2, 1, 3)],
            [diag_narrow, rest_narrow] + narrow_parts,
        ),
        (width_wide, width_narrow),
    )


def project_kernel(
    token_of, mine, weight_wide, weight_narrow, residual, gain, stream_out, rows_out, stream_scr, squares, flat_scr, rows
):
    step = pl.program_id(0)
    heads, tokens, _ = mine.shape
    columns = weight_wide.shape[1]
    wide = weight_wide.shape[0] // heads
    model = stream_scr.shape[1]
    tiles = model // LANES
    made = residual[...].astype(jnp.float32)
    for h in range(heads):
        made = made + jnp.dot(
            mine[h, :, :wide],
            weight_wide[h * wide : (h + 1) * wide, :],
            preferred_element_type=jnp.float32,
        )
    stacked = jnp.concatenate([mine[h, :, wide:] for h in range(heads)], axis=1)
    made = made + jnp.dot(stacked, weight_narrow[...], preferred_element_type=jnp.float32)
    rounded = made.astype(jnp.bfloat16)
    stream_out[...] = rounded
    stream = rounded.astype(jnp.float32)
    stream_scr[:, pl.ds(pl.multiple_of(step * columns, columns), columns)] = stream
    square = jnp.sum(stream * stream, axis=1, keepdims=True)

    @pl.when(step == 0)
    def _():
        squares[...] = jnp.broadcast_to(square, squares.shape)

    @pl.when(step > 0)
    def _():
        squares[...] = squares[...] + square

    @pl.when(step == pl.num_programs(0) - 1)
    def _():
        inverse = lax.rsqrt(squares[...] / model + 1e-06)
        for j in range(tiles):
            lanes = slice(j * LANES, (j + 1) * LANES)
            flat_scr[pl.ds(j, tokens, stride=tiles), :] = (
                stream_scr[:, lanes] * inverse * gain[:, lanes]
            )
        rows[...] = flat_scr[...].reshape(tokens, tiles, LANES).astype(jnp.bfloat16)

        def copy_row(slot, _):
            rows_out[slot] = rows[token_of[slot]]
            return 0

        lax.fori_loop(0, rows_out.shape[0], copy_row, 0, unroll=16)


def project(token_of, mine, weight_wide, weight_narrow, residual, gain):
    heads, tokens, depth = mine.shape
    model = weight_wide.shape[1]
    slots = token_of.shape[0]
    tiles = model // LANES
    columns = 2 * BLOCK
    return pl.pallas_call(
        project_kernel,
        grid=(model // columns,),
        out_shape=(
            jax.ShapeDtypeStruct((tokens, model), jnp.bfloat16),
            jax.ShapeDtypeStruct((slots, tiles, LANES), jnp.bfloat16),
        ),
        in_specs=[
            pl.BlockSpec(memory_space=pltpu.SMEM),
            pl.BlockSpec((heads, tokens, depth), lambda i: (0, 0, 0)),
            pl.BlockSpec((weight_wide.shape[0], columns), lambda i: (0, i)),
            pl.BlockSpec((weight_narrow.shape[0], columns), lambda i: (0, i)),
            pl.BlockSpec((tokens, columns), lambda i: (0, i)),
            pl.BlockSpec((1, model), lambda i: (0, 0)),
        ],
        out_specs=(
            pl.BlockSpec((tokens, columns), lambda i: (0, i)),
            pl.BlockSpec((slots, tiles, LANES), lambda i: (0, 0, 0)),
        ),
        scratch_shapes=[
            pltpu.VMEM((tokens, model), jnp.float32),
            pltpu.VMEM((tokens, LANES), jnp.float32),
            pltpu.VMEM((tokens * tiles, LANES), jnp.float32),
            pltpu.VMEM((tokens, tiles, LANES), jnp.bfloat16),
        ],
        name="project",
    )(token_of, mine, weight_wide, weight_narrow, residual, gain)


def expert_kernel(
    arrived, gate, up, down, out, gate_scr, up_scr, down_scr, flat, rows, hidden, sems
):
    count, tiles, _ = arrived.shape
    model, inner = gate.shape
    steps = inner // BLOCK
    columns = model // steps

    def inner_part(k):
        return pl.ds(pl.multiple_of(k * BLOCK, BLOCK), BLOCK)

    def outer_part(k):
        return pl.ds(pl.multiple_of(k * columns, columns), columns)

    def in_copies(k):
        part = inner_part(k)
        return (
            pltpu.make_async_copy(gate.at[:, part], gate_scr.at[:, part], sems.at[0, k]),
            pltpu.make_async_copy(up.at[:, part], up_scr.at[:, part], sems.at[1, k]),
        )

    def out_copy(k):
        part = outer_part(k)
        return pltpu.make_async_copy(down.at[:, part], down_scr.at[:, part], sems.at[2, k])

    def spread(k, _):
        some = arrived[pl.ds(k * SOME, SOME)].astype(jnp.float32)
        flat[pl.ds(pl.multiple_of(k * SOME * tiles, LANES), SOME * tiles), :] = some.reshape(
            SOME * tiles, LANES
        )
        return 0

    def gathered(k, _):
        some = flat[pl.ds(pl.multiple_of(k * SOME * tiles, LANES), SOME * tiles), :]
        out[pl.ds(k * SOME, SOME)] = some.reshape(SOME, tiles, LANES).astype(jnp.bfloat16)
        return 0

    for k in range(steps):
        for made in in_copies(k):
            made.start()
    for k in range(steps):
        out_copy(k).start()
    lax.fori_loop(0, count // SOME, spread, 0)
    for j in range(tiles):
        rows[:, j * LANES : (j + 1) * LANES] = flat[pl.ds(j, count, stride=tiles), :].astype(
            jnp.bfloat16
        )

    def widen(k, _):
        for made in in_copies(k):
            made.wait()
        part = inner_part(k)
        gate_part = jnp.dot(rows[...], gate_scr[:, part], preferred_element_type=jnp.float32)
        up_part = jnp.dot(rows[...], up_scr[:, part], preferred_element_type=jnp.float32)
        hidden[:, part] = (gate_part * jax.nn.sigmoid(gate_part) * up_part).astype(jnp.bfloat16)
        return 0

    def narrow(k, _):
        out_copy(k).wait()
        result = jnp.dot(
            hidden[...], down_scr[:, outer_part(k)], preferred_element_type=jnp.float32
        )
        for j in range(columns // LANES):
            flat[pl.ds(k * (columns // LANES) + j, count, stride=tiles), :] = result[
                :, j * LANES : (j + 1) * LANES
            ]
        return 0

    lax.fori_loop(0, steps, widen, 0)
    lax.fori_loop(0, steps, narrow, 0)
    lax.fori_loop(0, count // SOME, gathered, 0)


def experts(arrived, gate, up, down):
    count, tiles, _ = arrived.shape
    model, inner = gate.shape
    steps = inner // BLOCK
    return pl.pallas_call(
        expert_kernel,
        out_shape=jax.ShapeDtypeStruct(arrived.shape, jnp.bfloat16),
        in_specs=[pl.BlockSpec(memory_space=pltpu.VMEM)]
        + [pl.BlockSpec(memory_space=pl.ANY)] * 3,
        out_specs=pl.BlockSpec(memory_space=pltpu.VMEM),
        scratch_shapes=[
            pltpu.VMEM((model, inner), jnp.bfloat16),
            pltpu.VMEM((model, inner), jnp.bfloat16),
            pltpu.VMEM((inner, model), jnp.bfloat16),
            pltpu.VMEM((count * tiles, LANES), jnp.float32),
            pltpu.VMEM((count, model), jnp.bfloat16),
            pltpu.VMEM((count, inner), jnp.bfloat16),
            pltpu.SemaphoreType.DMA((3, steps)),
        ],
        name="experts",
    )(arrived, gate, up, down)


def combine_kernel(slot_of, share_of, returned, stream, out, flat):
    tokens, model = stream.shape
    tiles = model // LANES

    def one_token(token, _):
        total = share_of[2 * token] * returned[slot_of[2 * token]].astype(jnp.float32)
        total = total + share_of[2 * token + 1] * returned[slot_of[2 * token + 1]].astype(
            jnp.float32
        )
        flat[pl.ds(pl.multiple_of(token * tiles, tiles), tiles), :] = total
        return 0

    lax.fori_loop(0, tokens, one_token, 0, unroll=8)
    for j in range(tiles):
        lanes = slice(j * LANES, (j + 1) * LANES)
        out[:, lanes] = (
            stream[:, lanes].astype(jnp.float32) + flat[pl.ds(j, tokens, stride=tiles), :]
        ).astype(jnp.bfloat16)


def combine(slot_of, share_of, returned, stream):
    tokens, model = stream.shape
    return pl.pallas_call(
        combine_kernel,
        out_shape=jax.ShapeDtypeStruct(stream.shape, jnp.bfloat16),
        in_specs=[pl.BlockSpec(memory_space=pltpu.SMEM)] * 2
        + [pl.BlockSpec(memory_space=pltpu.VMEM)] * 2,
        out_specs=pl.BlockSpec(memory_space=pltpu.VMEM),
        scratch_shapes=[pltpu.VMEM((tokens * (model // LANES), LANES), jnp.float32)],
        name="combine",
    )(slot_of, share_of, returned, stream)


def slot_tables(expert_ids, experts_all, capacity):
    flat_expert = expert_ids.reshape(-1)
    order = jnp.arange(flat_expert.shape[0], dtype=jnp.int32)
    earlier = (flat_expert[:, None] == flat_expert[None, :]) & (order[None, :] < order[:, None])
    slot_of = flat_expert * capacity + jnp.sum(earlier.astype(jnp.int32), axis=1)
    slot_ids = jnp.arange(experts_all * capacity, dtype=jnp.int32)
    placed = slot_ids[:, None] == slot_of[None, :]
    token_of = jnp.sum(jnp.where(placed, order[None, :] // 2, 0), axis=1)
    return slot_of, token_of


def shards(
    query_wide,
    key_wide,
    value_wide,
    query_narrow,
    key_narrow,
    value_narrow,
    mix_lambda,
    residual_in,
    out_wide,
    out_narrow,
    ffn_gain,
    expert_ids,
    expert_weights,
    gate_weight,
    up_weight,
    down_weight,
):
    heads = attention(
        query_wide[:, 0],
        key_wide[:, 0],
        value_wide[:, 0],
        query_narrow[:, 0],
        key_narrow[:, 0],
        value_narrow[:, 0],
        mix_lambda,
    )
    tp_size = lax.axis_size(TP)
    local_rows = heads.shape[0] // tp_size
    experts_all = lax.axis_size(SP_TP)
    capacity = max(2, 4 * local_rows // experts_all)
    slot_of, token_of = slot_tables(expert_ids, experts_all, capacity)
    whole_wide = lax.all_gather(out_wide, TP, axis=0, tiled=True)
    whole_narrow = lax.all_gather(out_narrow, TP, axis=0, tiled=True)
    mine = lax.all_to_all(
        heads.reshape(tp_size, local_rows, -1), TP, split_axis=0, concat_axis=0, tiled=True
    )
    stream, outgoing = project(
        token_of, mine, whole_wide, whole_narrow, residual_in, ffn_gain[None, :]
    )

    def exchanged(rows):
        shape = rows.shape
        moved = lax.all_to_all(
            rows.reshape(experts_all, -1, LANES), SP_TP, split_axis=0, concat_axis=0, tiled=True
        )
        return moved.reshape(shape)

    result = experts(exchanged(outgoing), gate_weight[0], up_weight[0], down_weight[0])
    return combine(slot_of, expert_weights.reshape(-1), exchanged(result), stream)


def solution(mesh):
    finer = Mesh(mesh.devices.reshape(4, 4, 4, 2), SP_TP)
    sp = ("z", "x")
    placed = (
        P(sp, TP, None),
        P(sp, TP, None),
        P(sp, TP, None),
        P(sp, TP, None),
        P(sp, TP, None),
        P(sp, TP, None),
        P(None, TP),
        P(SP_TP, None),
        P(TP, None),
        P(TP, None),
        P(),
        P(SP_TP, None),
        P(SP_TP, None),
        P(SP_TP, None, None),
        P(SP_TP, None, None),
        P(SP_TP, None, None),
    )
    return jax.shard_map(
        shards, mesh=finer, in_specs=placed, out_specs=P(SP_TP, None), check_vma=False
    )
```

```python
import jax
import jax.numpy as jnp
from jax import lax
from jax.experimental import pallas as pl
from jax.experimental.pallas import tpu as pltpu
from jax.sharding import Mesh
from jax.sharding import PartitionSpec as P

TP = ("y", "c")
SP_TP = ("z", "x", "y", "c")
RING = 4
LOG2E = 1.4426950408889634
NEG_FILL = -1e30
STAT_ROWS = 16
LANES = 128
BLOCK = 256
SOME = 48
VALID_ROW = 8
LEAST_TOTAL = 2.0**-60
MOST_TOTAL = 2.0**100


def pack_kernel(v_wide, k_narrow, v_narrow, v_out, kv_out):
    chunk, width = v_wide.shape
    half = chunk // 2
    width_narrow = v_narrow.shape[1]
    for j in range(chunk // BLOCK):
        rows = slice(j * BLOCK, (j + 1) * BLOCK)
        v_out[j * width : (j + 1) * width, :] = v_wide[rows, :].T
        begin = half + j * width_narrow
        kv_out[begin : begin + width_narrow, :] = v_narrow[rows, :].T
    for side in range(2):
        lanes = slice(side * LANES, (side + 1) * LANES)
        kv_out[:half, lanes] = k_narrow[side * half : (side + 1) * half, :]


def pack(v_wide, k_narrow, v_narrow):
    chunk, width = v_wide.shape
    rows = chunk // 2 + chunk // BLOCK * v_narrow.shape[1]
    return pl.pallas_call(
        pack_kernel,
        out_shape=(
            jax.ShapeDtypeStruct((chunk // BLOCK * width, BLOCK), jnp.bfloat16),
            jax.ShapeDtypeStruct((rows, BLOCK), jnp.bfloat16),
        ),
        name="pack",
    )(v_wide, k_narrow, v_narrow)


def attend_kernel(table, *refs, rows, slots, pieces, wide, diagonal, fill, size, width, chunk):
    chunks = len(rows)
    q_refs = refs[:chunks]
    src_refs = refs[chunks : chunks + slots * pieces]
    out_refs = refs[chunks + slots * pieces : 2 * chunks + slots * pieces]
    q_scr, kv_scr, acc, out_scr, sems, q_sems, out_sems = refs[2 * chunks + slots * pieces :]
    plans = [(table[row, 0], table[row, 1], table[row, 2]) for row in rows]
    scale = size ** (-0.5) * LOG2E
    key_rows = chunk if wide else chunk // 2
    halves = key_rows // LANES

    def slot_copies(slot):
        made = []
        begin = 0
        for k in range(pieces):
            source = src_refs[slot * pieces + k]
            rows = source.shape[0]
            made.append(
                pltpu.make_async_copy(
                    source, kv_scr.at[slot, pl.ds(begin, rows), :], sems.at[slot, k]
                )
            )
            begin += rows
        return made

    def wait_slot(slot):
        begin = 0
        for k in range(pieces):
            source = src_refs[k]
            rows = source.shape[0]
            pltpu.make_async_copy(
                source, kv_scr.at[slot, pl.ds(begin, rows), :], sems.at[slot, k]
            ).wait()
            begin += rows

    def only_map(rows, m):
        lane = lax.broadcasted_iota(jnp.int32, rows.shape, 1)
        return jnp.where((lane >= m * size) & (lane < (m + 1) * size), rows, 0)

    def dot_nt(left, right):
        return lax.dot_general(
            left, right, (((1,), (1,)), ((), ())), preferred_element_type=jnp.float32
        )

    def value_block(slot, j):
        return kv_scr[slot, pl.ds(key_rows + j * width, width), :]

    def store_result(n, m, columns, read, total, level):
        out_scr[n, pl.ds(m * width, width), columns] = (read * (1.0 / total)).astype(jnp.bfloat16)
        row = lax.broadcasted_iota(jnp.int32, (8, total.shape[1]), 0)
        packed = jnp.zeros((8, total.shape[1]), jnp.float32)
        for k in range(3):
            term = level.astype(jnp.bfloat16).astype(jnp.float32)
            packed = jnp.where(row == k, term, packed)
            level = level - term
        return packed

    def within(slot, plan):
        active, count, offset = plan
        return (active > 0) & (slot >= offset) & (slot < offset + count)

    for n in range(chunks):

        @pl.when(plans[n][0] > 0)
        def _(n=n):
            pltpu.make_async_copy(q_refs[n], q_scr.at[n], q_sems.at[n]).start()

    for slot in range(slots):
        used = within(slot, plans[0])
        for plan in plans[1:]:
            used = used | within(slot, plan)

        @pl.when(used)
        def _(slot=slot):
            for made in slot_copies(slot):
                made.start()

    def one_chunk(n, _):
        row = rows[0] + n
        active, count, offset = table[row, 0], table[row, 1], table[row, 2]
        pl.when(active > 0)(lambda: attend_chunk(n, count, offset))
        if fill:

            @pl.when(active == 0)
            def _():
                out_scr[n] = jnp.zeros(out_scr.shape[1:], out_scr.dtype)

        for k in range(chunks):

            @pl.when((n == k) & ((active > 0) | fill))
            def _(k=k):
                pltpu.make_async_copy(out_scr.at[k], out_refs[k], out_sems.at[k]).start()

        return 0

    def attend_chunk(n, count, offset):
        acc[...] = jnp.zeros_like(acc)
        pltpu.make_async_copy(q_refs[0], q_scr.at[n], q_sems.at[n]).wait()

        def add_slot(number, totals):
            slot = 0 if diagonal else number + offset
            if chunks > 1:
                pl.when((n == 0) | jnp.logical_not(within(slot, plans[0])))(
                    lambda: wait_slot(slot)
                )
            else:
                wait_slot(slot)
            values = jnp.concatenate(
                [value_block(slot, j) for j in range(chunk // BLOCK)], axis=1
            )
            result = []
            for m in range(2):
                if wide:
                    lanes = slice(m * size, (m + 1) * size)
                    scores = dot_nt(kv_scr[slot, :key_rows, lanes], q_scr[n, :, lanes])
                else:
                    queries = only_map(q_scr[n], m)
                    scores = jnp.concatenate(
                        [
                            dot_nt(kv_scr[slot, :key_rows, side * LANES : (side + 1) * LANES], queries)
                            for side in range(2)
                        ],
                        axis=0,
                    )
                scores = scores * scale
                if diagonal:
                    key_pos = lax.broadcasted_iota(jnp.int32, scores.shape, 0)
                    query_pos = lax.broadcasted_iota(jnp.int32, scores.shape, 1)
                    scores = jnp.where(key_pos <= query_pos, scores, NEG_FILL)
                weights = jnp.exp2(scores)
                result.append(totals[m] + jnp.sum(weights.reshape(chunk // 8, 8, chunk), axis=0))
                acc[m] = acc[m] + jnp.dot(
                    values, weights.astype(jnp.bfloat16), preferred_element_type=jnp.float32
                )
            return tuple(result)

        none = jnp.zeros((8, chunk), jnp.float32)
        if diagonal:
            totals = add_slot(0, (none, none))
        else:
            totals = lax.fori_loop(0, count, add_slot, (none, none))
        outside = jnp.zeros((1, chunk), jnp.float32)
        stats = []
        for m in range(2):
            total = jnp.sum(totals[m], axis=0, keepdims=True)
            inside = (total >= LEAST_TOTAL) & (total <= MOST_TOTAL)
            outside = jnp.maximum(outside, jnp.where(inside, 0.0, 1.0))
            stats.append(store_result(n, m, slice(None), acc[m], total, jnp.log2(total)))
        out_scr[n, 2 * width :, :] = jnp.concatenate(stats, axis=0).astype(jnp.bfloat16)

        @pl.when(jnp.max(outside) > 0)
        def _():
            def packed_rows(take, number):
                made = []
                for k in range(2):
                    piece = number * 2 + k
                    place = pl.ds(pl.multiple_of(lax.rem(piece, halves) * LANES, LANES), LANES)
                    first, second = take(place)
                    made.append(jnp.where(piece < halves, first, second))
                return jnp.concatenate(made, axis=0)

            def keys_at(slot, number):
                return packed_rows(
                    lambda place: (kv_scr[slot, place, :LANES], kv_scr[slot, place, LANES:]), number
                )

            def one_query_block(number, _):
                begin = pl.multiple_of(number * BLOCK, BLOCK)
                columns = pl.ds(begin, BLOCK)

                def one_map(m, packed):
                    acc[m, :, columns] = jnp.zeros((width, BLOCK), jnp.float32)

                    def careful(index, state):
                        peak, total = state
                        slot = index // (chunk // BLOCK) + offset
                        block = lax.rem(index, chunk // BLOCK)
                        place = pl.ds(pl.multiple_of(block * BLOCK, BLOCK), BLOCK)
                        if wide:
                            lanes = pl.ds(pl.multiple_of(m * size, size), size)
                            scores = dot_nt(kv_scr[slot, place, lanes], q_scr[n, columns, lanes])
                        else:
                            scores = dot_nt(keys_at(slot, block), only_map(q_scr[n, columns, :], m))
                        scores = scores * scale
                        if diagonal:
                            key_pos = block * BLOCK + lax.broadcasted_iota(
                                jnp.int32, scores.shape, 0
                            )
                            query_pos = begin + lax.broadcasted_iota(jnp.int32, scores.shape, 1)
                            scores = jnp.where(key_pos <= query_pos, scores, NEG_FILL)
                        new_peak = jnp.maximum(peak, jnp.max(scores, axis=0, keepdims=True))
                        factor = jnp.exp2(peak - new_peak)
                        weights = jnp.exp2(scores - new_peak)
                        acc[m, :, columns] = factor * acc[m, :, columns] + jnp.dot(
                            value_block(slot, block),
                            weights.astype(jnp.bfloat16),
                            preferred_element_type=jnp.float32,
                        )
                        return new_peak, factor * total + jnp.sum(weights, axis=0, keepdims=True)

                    peak, total = lax.fori_loop(
                        0,
                        count * (chunk // BLOCK),
                        careful,
                        (
                            jnp.full((1, BLOCK), NEG_FILL, jnp.float32),
                            jnp.zeros((1, BLOCK), jnp.float32),
                        ),
                    )
                    rows = store_result(
                        n, m, columns, acc[m, :, columns], total, peak + jnp.log2(total)
                    )
                    both = jnp.concatenate([rows, rows], axis=0)
                    row = lax.broadcasted_iota(jnp.int32, both.shape, 0)
                    return jnp.where((row >= 8 * m) & (row < 8 * m + 8), both, packed)

                packed = lax.fori_loop(
                    0, 2, one_map, jnp.zeros((STAT_ROWS, BLOCK), jnp.float32)
                )
                out_scr[n, 2 * width :, columns] = packed.astype(jnp.bfloat16)
                return 0

            lax.fori_loop(0, chunk // BLOCK, one_query_block, 0)

    if chunks > 1:
        lax.fori_loop(0, chunks, one_chunk, 0)
    else:
        one_chunk(0, 0)
    for n in range(chunks):

        @pl.when((plans[n][0] > 0) | fill)
        def _(n=n):
            pltpu.make_async_copy(out_scr.at[n], out_refs[n], out_sems.at[n]).wait()


def attend(table, rows, queries, sources, wide, diagonal, fill, size, width):
    chunk = queries[0].shape[0]
    pieces = len(sources[0])
    flat = [array for group in sources for array in group]
    kv_rows = sum(array.shape[0] for array in sources[0])
    chunks = len(rows)
    body = lambda *refs: attend_kernel(
        *refs,
        rows=rows,
        slots=len(sources),
        pieces=pieces,
        wide=wide,
        diagonal=diagonal,
        fill=fill,
        size=size,
        width=width,
        chunk=chunk,
    )
    area = chunk * chunk * 2 * 2 * chunks
    out = jax.ShapeDtypeStruct((2 * width + STAT_ROWS, chunk), jnp.bfloat16)
    return pl.pallas_call(
        body,
        out_shape=[out] * chunks,
        in_specs=[pl.BlockSpec(memory_space=pltpu.SMEM)]
        + [pl.BlockSpec(memory_space=pl.ANY)] * (chunks + len(flat)),
        out_specs=[pl.BlockSpec(memory_space=pl.ANY)] * chunks,
        scratch_shapes=[
            pltpu.VMEM((chunks,) + queries[0].shape, jnp.bfloat16),
            pltpu.VMEM((len(sources), kv_rows, BLOCK), jnp.bfloat16),
            pltpu.VMEM((2, width, chunk), jnp.float32),
            pltpu.VMEM((chunks,) + out.shape, jnp.bfloat16),
            pltpu.SemaphoreType.DMA((len(sources), pieces)),
            pltpu.SemaphoreType.DMA((chunks,)),
            pltpu.SemaphoreType.DMA((chunks,)),
        ],
        cost_estimate=pl.CostEstimate(
            flops=2 * area * (size + width),
            transcendentals=area,
            bytes_accessed=len(sources) * kv_rows * 512,
        ),
    )(table, *queries, *flat)


def merge_kernel(table, lam, *refs, widths, counts):
    out_ref = refs[-1]
    guarded = (1, None)
    begin = 0
    column = 0
    for group, (width, count) in enumerate(zip(widths, counts)):
        parts = refs[begin : begin + count]
        begin += count
        reads = []
        for m in range(2):
            levels = []
            for k, part in enumerate(parts):
                stats = part[2 * width :, :].astype(jnp.float32)
                level = stats[8 * m : 8 * m + 1] + stats[8 * m + 1 : 8 * m + 2] + stats[
                    8 * m + 2 : 8 * m + 3
                ]
                levels.append(jnp.where(table[VALID_ROW + group, k] > 0, level, NEG_FILL))
            top = levels[0]
            for level in levels[1:]:
                top = jnp.maximum(top, level)
            shares = [jnp.exp2(level - top) for level in levels]
            whole = shares[0]
            for share in shares[1:]:
                whole = whole + share
            read = None
            for k, (share, part) in enumerate(zip(shares, parts)):
                term = part[m * width : (m + 1) * width, :].astype(jnp.float32) * (share / whole)
                if read is None:
                    read = term
                elif guarded[group] == k:
                    read = read + jnp.where(table[VALID_ROW + group, k] > 0, term, 0.0)
                else:
                    read = read + term
            reads.append(read)
        mixed = reads[0] - lam[group, 0] * reads[1]
        normed = mixed * lax.rsqrt(jnp.mean(mixed * mixed, axis=0, keepdims=True) + 1e-06)
        out_ref[:, column : column + width] = normed.T.astype(jnp.bfloat16)
        column += width


def merge(table, lam, groups, widths):
    chunk = groups[0][0].shape[1]
    counts = [len(parts) for parts in groups]
    flat = [part for parts in groups for part in parts]
    body = lambda *refs: merge_kernel(*refs, widths=widths, counts=counts)
    return pl.pallas_call(
        body,
        grid=(chunk // BLOCK,),
        out_shape=jax.ShapeDtypeStruct((chunk, sum(widths)), jnp.bfloat16),
        in_specs=[pl.BlockSpec(memory_space=pltpu.SMEM)] * 2
        + [pl.BlockSpec((part.shape[0], BLOCK), lambda i: (0, i)) for part in flat],
        out_specs=pl.BlockSpec((BLOCK, sum(widths)), lambda i: (i, 0)),
        name="merge_reads",
    )(table, lam, *flat)


def around(array, axis, by):
    return lax.ppermute(array, axis, [(k, (k + by) % RING) for k in range(RING)])


def onward(array, axis, by):
    return lax.ppermute(
        array, axis, [(k, k + by) for k in range(RING) if 0 <= k + by < RING]
    )


def after(array, *others):
    return lax.optimization_barrier((array,) + others)[0]


WIDE_ORDER = (2, 1, 3)
NARROW_ORDER = (3, 1, 2)


def attention(
    query_wide, key_wide, value_wide, query_narrow, key_narrow, value_narrow, mix_lambda
):
    z = lax.axis_index("z")
    x = lax.axis_index("x")
    size_wide = query_wide.shape[1] // 2
    size_narrow = query_narrow.shape[1] // 2
    width_wide, width_narrow = value_wide.shape[1], value_narrow.shape[1]

    xk_near = around(key_wide, "x", 1)
    q_side = {3: around(query_narrow, "x", 3)}
    q_later = {d: onward(query_wide, "z", -d) for d in WIDE_ORDER}
    values, kv_narrow = pack(value_wide, key_narrow, value_narrow)
    xv_back = around(values, "x", -1)
    xv_near = around(values, "x", 1)
    xk_back = around(key_wide, "x", -1)
    kv_below = {d: onward(kv_narrow, "z", d) for d in (1, 2, 3)}
    xk_far = around(xk_near, "x", 1)
    xv_far = around(xv_back, "x", -1)
    for s in (1, 2):
        q_side[s] = around(query_narrow, "x", s)

    wide_sources = [(key_wide, values), (xk_near, xv_near), (xk_far, xv_far), (xk_back, xv_back)]
    narrow_sources = [(kv_narrow,)] + [(kv_below[d],) for d in (1, 2, 3)]

    one, zero = jnp.int32(1), jnp.int32(0)
    level = {s: (lax.rem(x - s + RING, RING) > x).astype(jnp.int32) for s in NARROW_ORDER}
    lines = [(one, one, zero)]
    lines += [((z + d < RING), RING, 0) for d in WIDE_ORDER]
    lines += [((z > 0) | (level[s] > 0), z + level[s], 1 - level[s]) for s in NARROW_ORDER]
    lines += [((x > 0), x, 1)]
    lines += [[one, x > 0] + [z >= d for d in WIDE_ORDER]]
    lines += [[one, z > 0] + [(z > 0) | (lax.rem(x + s, RING) < x) for s in NARROW_ORDER]]
    lines += [((z > 0), z, 1)]
    table = jnp.stack(
        [
            jnp.stack([jnp.asarray(n, jnp.int32) for n in (tuple(line) + (0, 0))[:5]])
            for line in lines
        ]
    )

    def wide(last, rows, queries, sources, diagonal):
        given = after(table, last) if last is not None else table
        return attend(given, rows, queries, sources, True, diagonal, False, size_wide, width_wide)

    def narrow(last, rows, queries, sources, diagonal):
        return attend(
            after(table, last), rows, queries, sources, False, diagonal, not diagonal, size_narrow,
            width_narrow,
        )

    diag_wide = wide(None, (0,), [query_wide], wide_sources[:1], True)[0]
    diag_narrow = narrow(diag_wide, (0,), [query_narrow], narrow_sources[:1], True)[0]
    side, sent = {}, {}
    side[3] = narrow(diag_narrow, (4,), [q_side[3]], narrow_sources, False)[0]
    sent[2] = wide(side[3], (1,), [q_later[2]], wide_sources, False)[0]
    relayed = lax.ppermute(sent[2], "z", [(0, 3), (1, 2)])
    sent[1], sent[3] = wide(sent[2], (2, 3), [q_later[1], q_later[3]], wide_sources, False)
    side[1], side[2] = narrow(sent[1], (5, 6), [q_side[1], q_side[2]], narrow_sources, False)
    for d in (1, 3):
        sent[d] = onward(sent[d], "z", d)
    sent[2] = lax.ppermute(after(relayed, side[1]), "z", [(3, 2), (2, 3)])
    rest_narrow = narrow(side[1], (10,), [query_narrow], narrow_sources, False)[0]
    rest_wide = wide(rest_narrow, (7,), [query_wide], wide_sources, False)[0]
    side = {s: around(side[s], "x", -s) for s in NARROW_ORDER}
    return merge(
        table,
        mix_lambda,
        (
            [diag_wide, rest_wide] + [sent[d] for d in WIDE_ORDER],
            [diag_narrow, rest_narrow] + [side[s] for s in NARROW_ORDER],
        ),
        (width_wide, width_narrow),
    )


def project_kernel(
    token_of, mine, weight_wide, weight_narrow, residual, gain, stream_out, rows_out,
    weights, left, total, flat_scr, rows, sems,
):
    heads, tokens, _ = mine.shape
    depth, model = weight_wide.shape
    wide = depth // heads
    tiles = model // LANES
    part = weights.shape[1]
    parts = weights.shape[0]
    for k in range(parts):
        if k * part < depth:
            source = weight_wide.at[pl.ds(k * part, part), :]
        else:
            source = weight_narrow.at[pl.ds(k * part - depth, part), :]
        pltpu.make_async_copy(source, weights.at[k], sems.at[k]).start()
    joined = jnp.concatenate(
        [mine[h, :, :wide] for h in range(heads)] + [mine[h, :, wide:] for h in range(heads)], axis=1
    )
    for k in range(parts):
        left[k] = joined[:, k * part : (k + 1) * part]
    total[...] = residual[...].astype(jnp.float32)

    def add_part(k, _):
        pltpu.make_async_copy(
            weight_wide.at[pl.ds(0, part), :], weights.at[k], sems.at[k]
        ).wait()
        total[...] = total[...] + jnp.dot(
            left[k], weights[k], preferred_element_type=jnp.float32
        )
        return 0

    lax.fori_loop(0, parts, add_part, 0)
    rounded = total[...].astype(jnp.bfloat16)
    stream_out[...] = rounded
    stream = rounded.astype(jnp.float32)
    inverse = lax.rsqrt(jnp.mean(stream * stream, axis=1, keepdims=True) + 1e-06)
    for j in range(tiles):
        lanes = slice(j * LANES, (j + 1) * LANES)
        flat_scr[pl.ds(j, tokens, stride=tiles), :] = stream[:, lanes] * inverse * gain[:, lanes]
    rows[...] = flat_scr[...].reshape(tokens, tiles, LANES).astype(jnp.bfloat16)

    def copy_row(slot, _):
        rows_out[slot] = rows[token_of[slot]]
        return 0

    lax.fori_loop(0, rows_out.shape[0], copy_row, 0, unroll=16)


def project(token_of, mine, weight_wide, weight_narrow, residual, gain):
    heads, tokens, depth = mine.shape
    model = weight_wide.shape[1]
    slots = token_of.shape[0]
    tiles = model // LANES
    part = 2 * BLOCK
    parts = heads * depth // part
    return pl.pallas_call(
        project_kernel,
        out_shape=(
            jax.ShapeDtypeStruct((tokens, model), jnp.bfloat16),
            jax.ShapeDtypeStruct((slots, tiles, LANES), jnp.bfloat16),
        ),
        in_specs=[
            pl.BlockSpec(memory_space=pltpu.SMEM),
            pl.BlockSpec(memory_space=pltpu.VMEM),
            pl.BlockSpec(memory_space=pltpu.HBM),
            pl.BlockSpec(memory_space=pltpu.HBM),
            pl.BlockSpec(memory_space=pltpu.VMEM),
            pl.BlockSpec(memory_space=pltpu.VMEM),
        ],
        out_specs=(pl.BlockSpec(memory_space=pltpu.VMEM),) * 2,
        scratch_shapes=[
            pltpu.VMEM((parts, part, model), jnp.bfloat16),
            pltpu.VMEM((parts, tokens, part), jnp.bfloat16),
            pltpu.VMEM((tokens, model), jnp.float32),
            pltpu.VMEM((tokens * tiles, LANES), jnp.float32),
            pltpu.VMEM((tokens, tiles, LANES), jnp.bfloat16),
            pltpu.SemaphoreType.DMA((parts,)),
        ],
        compiler_params=pltpu.CompilerParams(vmem_limit_bytes=49 * 1024 * 1024),
        name="project",
    )(token_of, mine, weight_wide, weight_narrow, residual, gain)


def expert_kernel(arrived, gate, up, down, out, flat, rows, hidden):
    count, tiles, _ = arrived.shape
    model, inner = gate.shape
    steps = inner // BLOCK
    columns = model // steps

    def spread(k, _):
        some = arrived[pl.ds(k * SOME, SOME)].astype(jnp.float32)
        flat[pl.ds(pl.multiple_of(k * SOME * tiles, LANES), SOME * tiles), :] = some.reshape(
            SOME * tiles, LANES
        )
        return 0

    def gathered(k, _):
        some = flat[pl.ds(pl.multiple_of(k * SOME * tiles, LANES), SOME * tiles), :]
        out[pl.ds(k * SOME, SOME)] = some.reshape(SOME, tiles, LANES).astype(jnp.bfloat16)
        return 0

    lax.fori_loop(0, count // SOME, spread, 0)
    for j in range(tiles):
        rows[:, j * LANES : (j + 1) * LANES] = flat[pl.ds(j, count, stride=tiles), :].astype(
            jnp.bfloat16
        )

    def widen(k, _):
        part = pl.ds(pl.multiple_of(k * BLOCK, BLOCK), BLOCK)
        gate_part = jnp.dot(rows[...], gate[:, part], preferred_element_type=jnp.float32)
        up_part = jnp.dot(rows[...], up[:, part], preferred_element_type=jnp.float32)
        hidden[:, part] = (gate_part * jax.nn.sigmoid(gate_part) * up_part).astype(jnp.bfloat16)
        return 0

    def narrow(k, _):
        result = jnp.dot(
            hidden[...],
            down[:, pl.ds(pl.multiple_of(k * columns, columns), columns)],
            preferred_element_type=jnp.float32,
        )
        for j in range(columns // LANES):
            flat[pl.ds(k * (columns // LANES) + j, count, stride=tiles), :] = result[
                :, j * LANES : (j + 1) * LANES
            ]
        return 0

    lax.fori_loop(0, steps, widen, 0)
    lax.fori_loop(0, steps, narrow, 0)
    lax.fori_loop(0, count // SOME, gathered, 0)


def experts(arrived, gate, up, down):
    count, tiles, _ = arrived.shape
    model, inner = gate.shape
    return pl.pallas_call(
        expert_kernel,
        out_shape=jax.ShapeDtypeStruct(arrived.shape, jnp.bfloat16),
        in_specs=[pl.BlockSpec(memory_space=pltpu.VMEM)] * 4,
        out_specs=pl.BlockSpec(memory_space=pltpu.VMEM),
        scratch_shapes=[
            pltpu.VMEM((count * tiles, LANES), jnp.float32),
            pltpu.VMEM((count, model), jnp.bfloat16),
            pltpu.VMEM((count, inner), jnp.bfloat16),
        ],
        compiler_params=pltpu.CompilerParams(vmem_limit_bytes=28*1024*1024),
        name="experts",
    )(arrived, gate, up, down)


def combine_kernel(slot_of, share_of, returned, stream, out, flat):
    tokens, model = stream.shape
    tiles = model // LANES

    def one_token(token, _):
        total = share_of[2 * token] * returned[slot_of[2 * token]].astype(jnp.float32)
        total = total + share_of[2 * token + 1] * returned[slot_of[2 * token + 1]].astype(
            jnp.float32
        )
        flat[pl.ds(pl.multiple_of(token * tiles, tiles), tiles), :] = total
        return 0

    lax.fori_loop(0, tokens, one_token, 0, unroll=8)
    for j in range(tiles):
        lanes = slice(j * LANES, (j + 1) * LANES)
        out[:, lanes] = (
            stream[:, lanes].astype(jnp.float32) + flat[pl.ds(j, tokens, stride=tiles), :]
        ).astype(jnp.bfloat16)


def combine(slot_of, share_of, returned, stream):
    tokens, model = stream.shape
    return pl.pallas_call(
        combine_kernel,
        out_shape=jax.ShapeDtypeStruct(stream.shape, jnp.bfloat16),
        in_specs=[pl.BlockSpec(memory_space=pltpu.SMEM)] * 2
        + [pl.BlockSpec(memory_space=pltpu.VMEM)] * 2,
        out_specs=pl.BlockSpec(memory_space=pltpu.VMEM),
        scratch_shapes=[pltpu.VMEM((tokens * (model // LANES), LANES), jnp.float32)],
        name="combine",
    )(slot_of, share_of, returned, stream)


def slot_tables(expert_ids, experts_all, capacity):
    flat_expert = expert_ids.reshape(-1)
    order = jnp.arange(flat_expert.shape[0], dtype=jnp.int32)
    earlier = (flat_expert[:, None] == flat_expert[None, :]) & (order[None, :] < order[:, None])
    slot_of = flat_expert * capacity + jnp.sum(earlier.astype(jnp.int32), axis=1)
    slot_ids = jnp.arange(experts_all * capacity, dtype=jnp.int32)
    placed = slot_ids[:, None] == slot_of[None, :]
    token_of = jnp.sum(jnp.where(placed, order[None, :] // 2, 0), axis=1)
    return slot_of, token_of


def shards(
    query_wide,
    key_wide,
    value_wide,
    query_narrow,
    key_narrow,
    value_narrow,
    mix_lambda,
    residual_in,
    out_wide,
    out_narrow,
    ffn_gain,
    expert_ids,
    expert_weights,
    gate_weight,
    up_weight,
    down_weight,
):
    heads = attention(
        query_wide[:, 0],
        key_wide[:, 0],
        value_wide[:, 0],
        query_narrow[:, 0],
        key_narrow[:, 0],
        value_narrow[:, 0],
        mix_lambda,
    )
    tp_size = lax.axis_size(TP)
    local_rows = heads.shape[0] // tp_size
    experts_all = lax.axis_size(SP_TP)
    capacity = max(2, 4 * local_rows // experts_all)
    slot_of, token_of = slot_tables(expert_ids, experts_all, capacity)
    whole_wide = lax.all_gather(out_wide, TP, axis=0, tiled=True)
    whole_narrow = lax.all_gather(out_narrow, TP, axis=0, tiled=True)
    mine = lax.all_to_all(
        heads.reshape(tp_size, local_rows, -1), TP, split_axis=0, concat_axis=0, tiled=True
    )
    stream, outgoing = project(
        token_of, mine, whole_wide, whole_narrow, residual_in, ffn_gain[None, :]
    )

    def exchanged(rows):
        shape = rows.shape
        moved = lax.all_to_all(
            rows.reshape(experts_all, -1, LANES), SP_TP, split_axis=0, concat_axis=0, tiled=True
        )
        return moved.reshape(shape)

    result = experts(exchanged(outgoing), gate_weight[0], up_weight[0], down_weight[0])
    return combine(slot_of, expert_weights.reshape(-1), exchanged(result), stream)


def solution(mesh):
    finer = Mesh(mesh.devices.reshape(4, 4, 4, 2), SP_TP)
    sp = ("z", "x")
    placed = (
        P(sp, TP, None),
        P(sp, TP, None),
        P(sp, TP, None),
        P(sp, TP, None),
        P(sp, TP, None),
        P(sp, TP, None),
        P(None, TP),
        P(SP_TP, None),
        P(TP, None),
        P(TP, None),
        P(),
        P(SP_TP, None),
        P(SP_TP, None),
        P(SP_TP, None, None),
        P(SP_TP, None, None),
        P(SP_TP, None, None),
    )
    return jax.shard_map(
        shards, mesh=finer, in_specs=placed, out_specs=P(SP_TP, None), check_vma=False
    )
```

```python
import jax
import jax.numpy as jnp
from jax import lax
from jax.experimental import pallas as pl
from jax.experimental.pallas import tpu as pltpu
from jax.sharding import Mesh
from jax.sharding import PartitionSpec as P

TP = ("y", "c")
SP_TP = ("z", "x", "y", "c")
RING = 4
LOG2E = 1.4426950408889634
NEG_FILL = -1e30
STAT_ROWS = 16
LANES = 128
BLOCK = 256
SOME = 48
WIDE_ORDER = (2, 1, 3)
NARROW_ORDER = (3, 1, 2)
LEAST_TOTAL = 2.0**-60
MOST_TOTAL = 2.0**100


def pack_kernel(
    place, q_wide, v_wide, q_narrow, k_narrow, v_narrow, v_out, kv_out, plus_out, minus_out, two_out
):
    z = place[0]
    chunk, width = v_wide.shape
    half = chunk // 2
    width_narrow = v_narrow.shape[1]
    behind = chunk // BLOCK * width
    for j in range(chunk // BLOCK):
        rows = slice(j * BLOCK, (j + 1) * BLOCK)
        v_out[j * width : (j + 1) * width, :] = v_wide[rows, :].T
        begin = half + j * width_narrow
        kv_out[begin : begin + width_narrow, :] = v_narrow[rows, :].T
    for side in range(2):
        lanes = slice(side * LANES, (side + 1) * LANES)
        rows = slice(side * half, (side + 1) * half)
        kv_out[:half, lanes] = k_narrow[rows, :]
        v_out[behind : behind + half, lanes] = q_narrow[rows, :]
    for out, gives_queries in (
        (plus_out, z == RING - 1),
        (minus_out, z > 0),
        (two_out, z >= RING // 2),
    ):

        @pl.when(gives_queries)
        def _(out=out):
            out[...] = q_wide[...]

        @pl.when(jnp.logical_not(gives_queries))
        def _(out=out):
            out[...] = kv_out[...]


def pack(place, q_wide, v_wide, q_narrow, k_narrow, v_narrow):
    chunk, width = v_wide.shape
    half = chunk // 2
    both = jax.ShapeDtypeStruct(q_wide.shape, jnp.bfloat16)
    assert half + chunk // BLOCK * v_narrow.shape[1] == chunk
    return pl.pallas_call(
        pack_kernel,
        out_shape=(
            jax.ShapeDtypeStruct((chunk // BLOCK * width + half, BLOCK), jnp.bfloat16),
            both,
            both,
            both,
            both,
        ),
        in_specs=[pl.BlockSpec(memory_space=pltpu.SMEM)]
        + [pl.BlockSpec(memory_space=pltpu.VMEM)] * 5,
        name="pack",
    )(place, q_wide, v_wide, q_narrow, k_narrow, v_narrow)


def attend_kernel(place, *refs, plans, slots, pieces, wide, diagonal, fill, size, width, chunk):
    chunks = len(plans)
    q_refs = refs[:chunks]
    src_refs = refs[chunks : chunks + slots * pieces]
    out_refs = refs[chunks + slots * pieces : 2 * chunks + slots * pieces]
    q_scr, kv_scr, acc, out_scr, sems, q_sems, out_sems = refs[2 * chunks + slots * pieces :]
    plans = [plan(place[0], place[1]) for plan in plans]
    scale = size ** (-0.5) * LOG2E
    key_rows = chunk if wide else chunk // 2
    halves = key_rows // LANES

    def slot_copies(slot):
        made = []
        begin = 0
        for k in range(pieces):
            rows = kv_scr.shape[1] // pieces
            source = src_refs[slot * pieces + k].at[pl.ds(0, rows), :]
            made.append(
                pltpu.make_async_copy(
                    source, kv_scr.at[slot, pl.ds(begin, rows), :], sems.at[slot, k]
                )
            )
            begin += rows
        return made

    def wait_slot(slot):
        begin = 0
        for k in range(pieces):
            rows = kv_scr.shape[1] // pieces
            source = src_refs[k].at[pl.ds(0, rows), :]
            pltpu.make_async_copy(
                source, kv_scr.at[slot, pl.ds(begin, rows), :], sems.at[slot, k]
            ).wait()
            begin += rows

    def only_map(rows, m):
        lane = lax.broadcasted_iota(jnp.int32, rows.shape, 1)
        return jnp.where((lane >= m * size) & (lane < (m + 1) * size), rows, 0)

    def dot_nt(left, right):
        return lax.dot_general(
            left, right, (((1,), (1,)), ((), ())), preferred_element_type=jnp.float32
        )

    def value_block(slot, j):
        return kv_scr[slot, pl.ds(key_rows + j * width, width), :]

    def store_result(n, m, columns, read, total, level):
        out_scr[n, pl.ds(m * width, width), columns] = (read * (1.0 / total)).astype(jnp.bfloat16)
        row = lax.broadcasted_iota(jnp.int32, (8, total.shape[1]), 0)
        packed = jnp.zeros((8, total.shape[1]), jnp.float32)
        for k in range(3):
            term = level.astype(jnp.bfloat16).astype(jnp.float32)
            packed = jnp.where(row == k, term, packed)
            level = level - term
        return packed

    def query_copy(source, n):
        rows = q_scr.shape[1]
        begin = 0 if wide else q_refs[source].shape[0] - rows
        return pltpu.make_async_copy(
            q_refs[source].at[pl.ds(begin, rows), :], q_scr.at[n], q_sems.at[n]
        )

    def within(slot, plan):
        active, count, offset = plan
        return (active > 0) & (slot >= offset) & (slot < offset + count)

    for n in range(chunks):

        @pl.when(plans[n][0] > 0)
        def _(n=n):
            query_copy(n, n).start()

    for slot in range(slots):
        used = within(slot, plans[0])
        for plan in plans[1:]:
            used = used | within(slot, plan)

        @pl.when(used)
        def _(slot=slot):
            for made in slot_copies(slot):
                made.start()

    def one_chunk(n, _):
        active, count, offset = plans[0]
        for k in range(1, chunks):
            active, count, offset = (
                jnp.where(n == k, new, old) for new, old in zip(plans[k], (active, count, offset))
            )
        pl.when(active > 0)(lambda: attend_chunk(n, count, offset))
        if fill:

            @pl.when(active == 0)
            def _():
                out_scr[n] = jnp.zeros(out_scr.shape[1:], out_scr.dtype)

        for k in range(chunks):

            @pl.when((n == k) & ((active > 0) | fill))
            def _(k=k):
                pltpu.make_async_copy(out_scr.at[k], out_refs[k], out_sems.at[k]).start()

        return 0

    def attend_chunk(n, count, offset):
        acc[...] = jnp.zeros_like(acc)
        query_copy(0, n).wait()

        def add_slot(number, totals):
            slot = 0 if diagonal else number + offset
            if chunks > 1:
                pl.when((n == 0) | jnp.logical_not(within(slot, plans[0])))(
                    lambda: wait_slot(slot)
                )
            else:
                wait_slot(slot)
            values = jnp.concatenate(
                [value_block(slot, j) for j in range(chunk // BLOCK)], axis=1
            )
            result = []
            for m in range(2):
                if wide:
                    lanes = slice(m * size, (m + 1) * size)
                    scores = dot_nt(kv_scr[slot, :key_rows, lanes], q_scr[n, :, lanes])
                else:
                    queries = only_map(
                        jnp.concatenate([q_scr[n, :, :LANES], q_scr[n, :, LANES:]], axis=0), m
                    )
                    scores = jnp.concatenate(
                        [
                            dot_nt(kv_scr[slot, :key_rows, side * LANES : (side + 1) * LANES], queries)
                            for side in range(2)
                        ],
                        axis=0,
                    )
                scores = scores * scale
                if diagonal:
                    key_pos = lax.broadcasted_iota(jnp.int32, scores.shape, 0)
                    query_pos = lax.broadcasted_iota(jnp.int32, scores.shape, 1)
                    scores = jnp.where(key_pos <= query_pos, scores, NEG_FILL)
                weights = jnp.exp2(scores)
                result.append(totals[m] + jnp.sum(weights.reshape(chunk // 8, 8, chunk), axis=0))
                acc[m] = acc[m] + jnp.dot(
                    values, weights.astype(jnp.bfloat16), preferred_element_type=jnp.float32
                )
            return tuple(result)

        none = jnp.zeros((8, chunk), jnp.float32)
        if diagonal:
            totals = add_slot(0, (none, none))
        else:
            totals = lax.fori_loop(0, count, add_slot, (none, none))
        outside = jnp.zeros((1, chunk), jnp.float32)
        stats = []
        for m in range(2):
            total = jnp.sum(totals[m], axis=0, keepdims=True)
            inside = (total >= LEAST_TOTAL) & (total <= MOST_TOTAL)
            outside = jnp.maximum(outside, jnp.where(inside, 0.0, 1.0))
            stats.append(store_result(n, m, slice(None), acc[m], total, jnp.log2(total)))
        out_scr[n, 2 * width :, :] = jnp.concatenate(stats, axis=0).astype(jnp.bfloat16)

        @pl.when(jnp.max(outside) > 0)
        def _():
            def packed_rows(take, number):
                made = []
                for k in range(2):
                    piece = number * 2 + k
                    place = pl.ds(pl.multiple_of(lax.rem(piece, halves) * LANES, LANES), LANES)
                    first, second = take(place)
                    made.append(jnp.where(piece < halves, first, second))
                return jnp.concatenate(made, axis=0)

            def keys_at(slot, number):
                return packed_rows(
                    lambda place: (kv_scr[slot, place, :LANES], kv_scr[slot, place, LANES:]), number
                )

            def queries_at(number):
                return packed_rows(
                    lambda place: (q_scr[n, place, :LANES], q_scr[n, place, LANES:]), number
                )

            def one_query_block(number, _):
                begin = pl.multiple_of(number * BLOCK, BLOCK)
                columns = pl.ds(begin, BLOCK)

                def one_map(m, packed):
                    acc[m, :, columns] = jnp.zeros((width, BLOCK), jnp.float32)

                    def careful(index, state):
                        peak, total = state
                        slot = index // (chunk // BLOCK) + offset
                        block = lax.rem(index, chunk // BLOCK)
                        place = pl.ds(pl.multiple_of(block * BLOCK, BLOCK), BLOCK)
                        if wide:
                            lanes = pl.ds(pl.multiple_of(m * size, size), size)
                            scores = dot_nt(kv_scr[slot, place, lanes], q_scr[n, columns, lanes])
                        else:
                            scores = dot_nt(keys_at(slot, block), only_map(queries_at(number), m))
                        scores = scores * scale
                        if diagonal:
                            key_pos = block * BLOCK + lax.broadcasted_iota(
                                jnp.int32, scores.shape, 0
                            )
                            query_pos = begin + lax.broadcasted_iota(jnp.int32, scores.shape, 1)
                            scores = jnp.where(key_pos <= query_pos, scores, NEG_FILL)
                        new_peak = jnp.maximum(peak, jnp.max(scores, axis=0, keepdims=True))
                        factor = jnp.exp2(peak - new_peak)
                        weights = jnp.exp2(scores - new_peak)
                        acc[m, :, columns] = factor * acc[m, :, columns] + jnp.dot(
                            value_block(slot, block),
                            weights.astype(jnp.bfloat16),
                            preferred_element_type=jnp.float32,
                        )
                        return new_peak, factor * total + jnp.sum(weights, axis=0, keepdims=True)

                    peak, total = lax.fori_loop(
                        0,
                        count * (chunk // BLOCK),
                        careful,
                        (
                            jnp.full((1, BLOCK), NEG_FILL, jnp.float32),
                            jnp.zeros((1, BLOCK), jnp.float32),
                        ),
                    )
                    rows = store_result(
                        n, m, columns, acc[m, :, columns], total, peak + jnp.log2(total)
                    )
                    both = jnp.concatenate([rows, rows], axis=0)
                    row = lax.broadcasted_iota(jnp.int32, both.shape, 0)
                    return jnp.where((row >= 8 * m) & (row < 8 * m + 8), both, packed)

                packed = lax.fori_loop(
                    0, 2, one_map, jnp.zeros((STAT_ROWS, BLOCK), jnp.float32)
                )
                out_scr[n, 2 * width :, columns] = packed.astype(jnp.bfloat16)
                return 0

            lax.fori_loop(0, chunk // BLOCK, one_query_block, 0)

    if chunks > 1:
        lax.fori_loop(0, chunks, one_chunk, 0)
    else:
        one_chunk(0, 0)
    for n in range(chunks):

        @pl.when((plans[n][0] > 0) | fill)
        def _(n=n):
            pltpu.make_async_copy(out_scr.at[n], out_refs[n], out_sems.at[n]).wait()


def attend(place, plans, queries, sources, wide, diagonal, fill, size, width, chunk):
    pieces = len(sources[0])
    flat = [array for group in sources for array in group]
    kv_rows = pieces * chunk
    chunks = len(plans)
    q_rows = chunk if wide else chunk // 2
    body = lambda *refs: attend_kernel(
        *refs,
        plans=plans,
        slots=len(sources),
        pieces=pieces,
        wide=wide,
        diagonal=diagonal,
        fill=fill,
        size=size,
        width=width,
        chunk=chunk,
    )
    area = chunk * chunk * 2 * 2 * chunks
    out = jax.ShapeDtypeStruct((2 * width + STAT_ROWS, chunk), jnp.bfloat16)
    return pl.pallas_call(
        body,
        out_shape=[out] * chunks,
        in_specs=[pl.BlockSpec(memory_space=pltpu.SMEM)]
        + [pl.BlockSpec(memory_space=pl.ANY)] * (chunks + len(flat)),
        out_specs=[pl.BlockSpec(memory_space=pl.ANY)] * chunks,
        scratch_shapes=[
            pltpu.VMEM((chunks, q_rows, BLOCK), jnp.bfloat16),
            pltpu.VMEM((len(sources), kv_rows, BLOCK), jnp.bfloat16),
            pltpu.VMEM((2, width, chunk), jnp.float32),
            pltpu.VMEM((chunks,) + out.shape, jnp.bfloat16),
            pltpu.SemaphoreType.DMA((len(sources), pieces)),
            pltpu.SemaphoreType.DMA((chunks,)),
            pltpu.SemaphoreType.DMA((chunks,)),
        ],
        cost_estimate=pl.CostEstimate(
            flops=2 * area * (size + width),
            transcendentals=area,
            bytes_accessed=len(sources) * kv_rows * 512,
        ),
    )(place, *queries, *flat)


def merge_kernel(place, lam, *refs, widths, counts):
    z, x = place[0], place[1]
    wide_valid = [z >= 0, x > 0] + [z >= d for d in WIDE_ORDER]
    narrow_valid = [z >= 0, z > 0] + [
        (z > 0) | (lax.rem(x + s, RING) < x) for s in NARROW_ORDER
    ]
    valid = (wide_valid, narrow_valid)
    out_ref = refs[-1]
    guarded = (1, None)
    begin = 0
    column = 0
    for group, (width, count) in enumerate(zip(widths, counts)):
        parts = refs[begin : begin + count]
        begin += count
        reads = []
        for m in range(2):
            levels = []
            for k, part in enumerate(parts):
                stats = part[2 * width :, :].astype(jnp.float32)
                level = stats[8 * m : 8 * m + 1] + stats[8 * m + 1 : 8 * m + 2] + stats[
                    8 * m + 2 : 8 * m + 3
                ]
                levels.append(jnp.where(valid[group][k], level, NEG_FILL))
            top = levels[0]
            for level in levels[1:]:
                top = jnp.maximum(top, level)
            shares = [jnp.exp2(level - top) for level in levels]
            whole = shares[0]
            for share in shares[1:]:
                whole = whole + share
            read = None
            for k, (share, part) in enumerate(zip(shares, parts)):
                term = part[m * width : (m + 1) * width, :].astype(jnp.float32) * (share / whole)
                if read is None:
                    read = term
                elif guarded[group] == k:
                    read = read + jnp.where(valid[group][k], term, 0.0)
                else:
                    read = read + term
            reads.append(read)
        mixed = reads[0] - lam[group, 0] * reads[1]
        normed = mixed * lax.rsqrt(jnp.mean(mixed * mixed, axis=0, keepdims=True) + 1e-06)
        out_ref[:, column : column + width] = normed.T.astype(jnp.bfloat16)
        column += width


def merge(place, lam, groups, widths):
    chunk = groups[0][0].shape[1]
    counts = [len(parts) for parts in groups]
    flat = [part for parts in groups for part in parts]
    body = lambda *refs: merge_kernel(*refs, widths=widths, counts=counts)
    return pl.pallas_call(
        body,
        grid=(chunk // BLOCK,),
        out_shape=jax.ShapeDtypeStruct((chunk, sum(widths)), jnp.bfloat16),
        in_specs=[pl.BlockSpec(memory_space=pltpu.SMEM)] * 2
        + [pl.BlockSpec((part.shape[0], BLOCK), lambda i: (0, i)) for part in flat],
        out_specs=pl.BlockSpec((BLOCK, sum(widths)), lambda i: (i, 0)),
        name="merge_reads",
    )(place, lam, *flat)


def around(array, axis, by):
    return lax.ppermute(array, axis, [(k, (k + by) % RING) for k in range(RING)])


def onward(array, axis, by):
    return lax.ppermute(
        array, axis, [(k, k + by) for k in range(RING) if 0 <= k + by < RING]
    )


def after(array, *others):
    return lax.optimization_barrier((array,) + others)[0]


def attention(
    query_wide, key_wide, value_wide, query_narrow, key_narrow, value_narrow, mix_lambda
):
    z = lax.axis_index("z")
    x = lax.axis_index("x")
    place = jnp.stack([z, x]).astype(jnp.int32)
    chunk = query_wide.shape[0]
    size_wide = query_wide.shape[1] // 2
    size_narrow = query_narrow.shape[1] // 2
    width_wide, width_narrow = value_wide.shape[1], value_narrow.shape[1]

    xk_near = around(key_wide, "x", 1)
    xk_back = around(key_wide, "x", -1)
    values, kv_narrow, plus, minus, two = pack(
        place, query_wide, value_wide, query_narrow, key_narrow, value_narrow
    )
    xv_back = around(values, "x", -1)
    xv_near = around(values, "x", 1)
    z_two = around(two, "z", 2)
    z_plus = around(plus, "z", 1)
    z_minus = around(minus, "z", -1)
    xv_far = around(xv_back[:chunk], "x", -1)
    xk_far = around(xk_near, "x", 1)
    xq_far = around(xv_near[chunk:], "x", 1)

    wide_sources = [(key_wide, values), (xk_near, xv_near), (xk_far, xv_far), (xk_back, xv_back)]
    narrow_sources = [(kv_narrow,), (z_plus,), (z_two,), (z_minus,)]
    q_later = {1: z_minus, 2: z_two, 3: z_plus}
    q_side = {1: xv_near, 2: xq_far, 3: xv_back}

    def wide_plan(d):
        return lambda z, x: ((z + d < RING).astype(jnp.int32), jnp.int32(RING), jnp.int32(0))

    def narrow_plan(s):
        def plan(z, x):
            level = (lax.rem(x - s + RING, RING) > x).astype(jnp.int32)
            return ((z > 0) | (level > 0)).astype(jnp.int32), z + level, 1 - level

        return plan

    def diag_plan(z, x):
        return jnp.int32(1), jnp.int32(1), jnp.int32(0)

    def wide_rest_plan(z, x):
        return (x > 0).astype(jnp.int32), x, jnp.int32(1)

    def narrow_rest_plan(z, x):
        return (z > 0).astype(jnp.int32), z, jnp.int32(1)

    def wide(last, plans, queries, sources, diagonal):
        given = after(place, last) if last is not None else place
        return attend(
            given, plans, queries, sources, True, diagonal, False, size_wide, width_wide, chunk
        )

    def narrow(last, plans, queries, sources, diagonal):
        return attend(
            after(place, last), plans, queries, sources, False, diagonal, not diagonal, size_narrow,
            width_narrow, chunk,
        )

    diag_wide = wide(None, (diag_plan,), [query_wide], wide_sources[:1], True)[0]
    diag_narrow = narrow(diag_wide, (diag_plan,), [values], narrow_sources[:1], True)[0]
    side, sent = {}, {}
    side[3] = narrow(diag_narrow, (narrow_plan(3),), [q_side[3]], narrow_sources, False)[0]
    sent[2] = wide(side[3], (wide_plan(2),), [q_later[2]], wide_sources, False)[0]
    relayed = lax.ppermute(sent[2], "z", [(0, 3), (1, 2)])
    sent[1], sent[3] = wide(
        sent[2], (wide_plan(1), wide_plan(3)), [q_later[1], q_later[3]], wide_sources, False,
    )
    side[1], side[2] = narrow(
        sent[1], (narrow_plan(1), narrow_plan(2)), [q_side[1], q_side[2]], narrow_sources, False,
    )
    for d in (1, 3):
        sent[d] = onward(sent[d], "z", d)
    sent[2] = lax.ppermute(after(relayed, side[1]), "z", [(3, 2), (2, 3)])
    rest_narrow = narrow(side[1], (narrow_rest_plan,), [values], narrow_sources, False)[0]
    rest_wide = wide(rest_narrow, (wide_rest_plan,), [query_wide], wide_sources, False)[0]
    side = {s: around(side[s], "x", -s) for s in NARROW_ORDER}
    return merge(
        place,
        mix_lambda,
        (
            [diag_wide, rest_wide] + [sent[d] for d in WIDE_ORDER],
            [diag_narrow, rest_narrow] + [side[s] for s in NARROW_ORDER],
        ),
        (width_wide, width_narrow),
    )


def project_kernel(
    token_of, mine, weight_wide, weight_narrow, residual, gain, stream_out, rows_out,
    weights, left, total, flat_scr, rows, sems,
):
    heads, tokens, _ = mine.shape
    depth, model = weight_wide.shape
    wide = depth // heads
    tiles = model // LANES
    part = weights.shape[1]
    parts = weights.shape[0]
    for k in range(parts):
        if k * part < depth:
            source = weight_wide.at[pl.ds(k * part, part), :]
        else:
            source = weight_narrow.at[pl.ds(k * part - depth, part), :]
        pltpu.make_async_copy(source, weights.at[k], sems.at[k]).start()
    joined = jnp.concatenate(
        [mine[h, :, :wide] for h in range(heads)] + [mine[h, :, wide:] for h in range(heads)], axis=1
    )
    for k in range(parts):
        left[k] = joined[:, k * part : (k + 1) * part]
    total[...] = residual[...].astype(jnp.float32)

    def add_part(k, _):
        pltpu.make_async_copy(
            weight_wide.at[pl.ds(0, part), :], weights.at[k], sems.at[k]
        ).wait()
        total[...] = total[...] + jnp.dot(
            left[k], weights[k], preferred_element_type=jnp.float32
        )
        return 0

    lax.fori_loop(0, parts, add_part, 0)
    rounded = total[...].astype(jnp.bfloat16)
    stream_out[...] = rounded
    stream = rounded.astype(jnp.float32)
    inverse = lax.rsqrt(jnp.mean(stream * stream, axis=1, keepdims=True) + 1e-06)
    for j in range(tiles):
        lanes = slice(j * LANES, (j + 1) * LANES)
        flat_scr[pl.ds(j, tokens, stride=tiles), :] = stream[:, lanes] * inverse * gain[:, lanes]
    rows[...] = flat_scr[...].reshape(tokens, tiles, LANES).astype(jnp.bfloat16)

    def copy_row(slot, _):
        rows_out[slot] = rows[token_of[slot]]
        return 0

    lax.fori_loop(0, rows_out.shape[0], copy_row, 0, unroll=16)


def project(token_of, mine, weight_wide, weight_narrow, residual, gain):
    heads, tokens, depth = mine.shape
    model = weight_wide.shape[1]
    slots = token_of.shape[0]
    tiles = model // LANES
    part = 2 * BLOCK
    parts = heads * depth // part
    return pl.pallas_call(
        project_kernel,
        out_shape=(
            jax.ShapeDtypeStruct((tokens, model), jnp.bfloat16),
            jax.ShapeDtypeStruct((slots, tiles, LANES), jnp.bfloat16),
        ),
        in_specs=[
            pl.BlockSpec(memory_space=pltpu.SMEM),
            pl.BlockSpec(memory_space=pltpu.VMEM),
            pl.BlockSpec(memory_space=pltpu.HBM),
            pl.BlockSpec(memory_space=pltpu.HBM),
            pl.BlockSpec(memory_space=pltpu.VMEM),
            pl.BlockSpec(memory_space=pltpu.VMEM),
        ],
        out_specs=(pl.BlockSpec(memory_space=pltpu.VMEM),) * 2,
        scratch_shapes=[
            pltpu.VMEM((parts, part, model), jnp.bfloat16),
            pltpu.VMEM((parts, tokens, part), jnp.bfloat16),
            pltpu.VMEM((tokens, model), jnp.float32),
            pltpu.VMEM((tokens * tiles, LANES), jnp.float32),
            pltpu.VMEM((tokens, tiles, LANES), jnp.bfloat16),
            pltpu.SemaphoreType.DMA((parts,)),
        ],
        compiler_params=pltpu.CompilerParams(vmem_limit_bytes=49 * 1024 * 1024),
        name="project",
    )(token_of, mine, weight_wide, weight_narrow, residual, gain)


def expert_kernel(arrived, gate, up, down, out, flat, rows, hidden):
    count, tiles, _ = arrived.shape
    model, inner = gate.shape
    steps = inner // BLOCK
    columns = model // steps

    def spread(k, _):
        some = arrived[pl.ds(k * SOME, SOME)].astype(jnp.float32)
        flat[pl.ds(pl.multiple_of(k * SOME * tiles, LANES), SOME * tiles), :] = some.reshape(
            SOME * tiles, LANES
        )
        return 0

    def gathered(k, _):
        some = flat[pl.ds(pl.multiple_of(k * SOME * tiles, LANES), SOME * tiles), :]
        out[pl.ds(k * SOME, SOME)] = some.reshape(SOME, tiles, LANES).astype(jnp.bfloat16)
        return 0

    lax.fori_loop(0, count // SOME, spread, 0)
    for j in range(tiles):
        rows[:, j * LANES : (j + 1) * LANES] = flat[pl.ds(j, count, stride=tiles), :].astype(
            jnp.bfloat16
        )

    def widen(k, _):
        part = pl.ds(pl.multiple_of(k * BLOCK, BLOCK), BLOCK)
        gate_part = jnp.dot(rows[...], gate[:, part], preferred_element_type=jnp.float32)
        up_part = jnp.dot(rows[...], up[:, part], preferred_element_type=jnp.float32)
        hidden[:, part] = (gate_part * jax.nn.sigmoid(gate_part) * up_part).astype(jnp.bfloat16)
        return 0

    def narrow(k, _):
        result = jnp.dot(
            hidden[...],
            down[:, pl.ds(pl.multiple_of(k * columns, columns), columns)],
            preferred_element_type=jnp.float32,
        )
        for j in range(columns // LANES):
            flat[pl.ds(k * (columns // LANES) + j, count, stride=tiles), :] = result[
                :, j * LANES : (j + 1) * LANES
            ]
        return 0

    lax.fori_loop(0, steps, widen, 0)
    lax.fori_loop(0, steps, narrow, 0)
    lax.fori_loop(0, count // SOME, gathered, 0)


def experts(arrived, gate, up, down):
    count, tiles, _ = arrived.shape
    model, inner = gate.shape
    return pl.pallas_call(
        expert_kernel,
        out_shape=jax.ShapeDtypeStruct(arrived.shape, jnp.bfloat16),
        in_specs=[pl.BlockSpec(memory_space=pltpu.VMEM)] * 4,
        out_specs=pl.BlockSpec(memory_space=pltpu.VMEM),
        scratch_shapes=[
            pltpu.VMEM((count * tiles, LANES), jnp.float32),
            pltpu.VMEM((count, model), jnp.bfloat16),
            pltpu.VMEM((count, inner), jnp.bfloat16),
        ],
        compiler_params=pltpu.CompilerParams(vmem_limit_bytes=28*1024*1024),
        name="experts",
    )(arrived, gate, up, down)


def combine_kernel(slot_of, share_of, returned, stream, out, flat):
    tokens, model = stream.shape
    tiles = model // LANES

    def one_token(token, _):
        total = share_of[2 * token] * returned[slot_of[2 * token]].astype(jnp.float32)
        total = total + share_of[2 * token + 1] * returned[slot_of[2 * token + 1]].astype(
            jnp.float32
        )
        flat[pl.ds(pl.multiple_of(token * tiles, tiles), tiles), :] = total
        return 0

    lax.fori_loop(0, tokens, one_token, 0, unroll=8)
    for j in range(tiles):
        lanes = slice(j * LANES, (j + 1) * LANES)
        out[:, lanes] = (
            stream[:, lanes].astype(jnp.float32) + flat[pl.ds(j, tokens, stride=tiles), :]
        ).astype(jnp.bfloat16)


def combine(slot_of, share_of, returned, stream):
    tokens, model = stream.shape
    return pl.pallas_call(
        combine_kernel,
        out_shape=jax.ShapeDtypeStruct(stream.shape, jnp.bfloat16),
        in_specs=[pl.BlockSpec(memory_space=pltpu.SMEM)] * 2
        + [pl.BlockSpec(memory_space=pltpu.VMEM)] * 2,
        out_specs=pl.BlockSpec(memory_space=pltpu.VMEM),
        scratch_shapes=[pltpu.VMEM((tokens * (model // LANES), LANES), jnp.float32)],
        compiler_params=pltpu.CompilerParams(vmem_limit_bytes=16 * 1024 * 1024),
        name="combine",
    )(slot_of, share_of, returned, stream)


def slot_tables(expert_ids, experts_all, capacity):
    flat_expert = expert_ids.reshape(-1)
    order = jnp.arange(flat_expert.shape[0], dtype=jnp.int32)
    earlier = (flat_expert[:, None] == flat_expert[None, :]) & (order[None, :] < order[:, None])
    slot_of = flat_expert * capacity + jnp.sum(earlier.astype(jnp.int32), axis=1)
    slot_ids = jnp.arange(experts_all * capacity, dtype=jnp.int32)
    placed = slot_ids[:, None] == slot_of[None, :]
    token_of = jnp.sum(jnp.where(placed, order[None, :] // 2, 0), axis=1)
    return slot_of, token_of


def shards(
    query_wide,
    key_wide,
    value_wide,
    query_narrow,
    key_narrow,
    value_narrow,
    mix_lambda,
    residual_in,
    out_wide,
    out_narrow,
    ffn_gain,
    expert_ids,
    expert_weights,
    gate_weight,
    up_weight,
    down_weight,
):
    heads = attention(
        query_wide[:, 0],
        key_wide[:, 0],
        value_wide[:, 0],
        query_narrow[:, 0],
        key_narrow[:, 0],
        value_narrow[:, 0],
        mix_lambda,
    )
    tp_size = lax.axis_size(TP)
    local_rows = heads.shape[0] // tp_size
    experts_all = lax.axis_size(SP_TP)
    capacity = max(2, 4 * local_rows // experts_all)
    slot_of, token_of = slot_tables(expert_ids, experts_all, capacity)
    whole_wide = lax.all_gather(out_wide, TP, axis=0, tiled=True)
    whole_narrow = lax.all_gather(out_narrow, TP, axis=0, tiled=True)
    mine = lax.all_to_all(
        heads.reshape(tp_size, local_rows, -1), TP, split_axis=0, concat_axis=0, tiled=True
    )
    stream, outgoing = project(
        token_of, mine, whole_wide, whole_narrow, residual_in, ffn_gain[None, :]
    )

    def exchanged(rows):
        shape = rows.shape
        moved = lax.all_to_all(
            rows.reshape(experts_all, -1, LANES), SP_TP, split_axis=0, concat_axis=0, tiled=True
        )
        return moved.reshape(shape)

    result = experts(exchanged(outgoing), gate_weight[0], up_weight[0], down_weight[0])
    return combine(slot_of, expert_weights.reshape(-1), exchanged(result), stream)


def solution(mesh):
    finer = Mesh(mesh.devices.reshape(4, 4, 4, 2), SP_TP)
    sp = ("z", "x")
    placed = (
        P(sp, TP, None),
        P(sp, TP, None),
        P(sp, TP, None),
        P(sp, TP, None),
        P(sp, TP, None),
        P(sp, TP, None),
        P(None, TP),
        P(SP_TP, None),
        P(TP, None),
        P(TP, None),
        P(),
        P(SP_TP, None),
        P(SP_TP, None),
        P(SP_TP, None, None),
        P(SP_TP, None, None),
        P(SP_TP, None, None),
    )
    return jax.shard_map(
        shards, mesh=finer, in_specs=placed, out_specs=P(SP_TP, None), check_vma=False
    )
```

```python
import jax
import jax.numpy as jnp
from jax import lax
from jax.experimental import pallas as pl
from jax.experimental.pallas import tpu as pltpu
from jax.sharding import Mesh
from jax.sharding import PartitionSpec as P

TP = ("y", "c")
SP_TP = ("z", "x", "y", "c")
RING = 4
LOG2E = 1.4426950408889634
NEG_FILL = -1e30
STAT_ROWS = 16
LANES = 128
BLOCK = 256
SOME = 48
WIDE_ORDER = (2, 1, 3)
NARROW_ORDER = (3, 1, 2)
LEAST_TOTAL = 2.0**-60
MOST_TOTAL = 2.0**100


def pack_kernel(
    q_wide, v_wide, q_narrow, k_narrow, v_narrow, v_out, kv_out, plus_out, minus_out, two_out
):
    z = lax.axis_index("z")
    chunk, width = v_wide.shape
    half = chunk // 2
    width_narrow = v_narrow.shape[1]
    behind = chunk // BLOCK * width
    for j in range(chunk // BLOCK):
        rows = slice(j * BLOCK, (j + 1) * BLOCK)
        v_out[j * width : (j + 1) * width, :] = v_wide[rows, :].T
        begin = half + j * width_narrow
        kv_out[begin : begin + width_narrow, :] = v_narrow[rows, :].T
    for side in range(2):
        lanes = slice(side * LANES, (side + 1) * LANES)
        rows = slice(side * half, (side + 1) * half)
        kv_out[:half, lanes] = k_narrow[rows, :]
        v_out[behind : behind + half, lanes] = q_narrow[rows, :]
    for out, gives_queries in (
        (plus_out, z == RING - 1),
        (minus_out, z > 0),
        (two_out, z >= RING // 2),
    ):

        @pl.when(gives_queries)
        def _(out=out):
            out[...] = q_wide[...]

        @pl.when(jnp.logical_not(gives_queries))
        def _(out=out):
            out[...] = kv_out[...]


def pack(q_wide, v_wide, q_narrow, k_narrow, v_narrow):
    chunk, width = v_wide.shape
    half = chunk // 2
    both = jax.ShapeDtypeStruct(q_wide.shape, jnp.bfloat16)
    assert half + chunk // BLOCK * v_narrow.shape[1] == chunk
    return pl.pallas_call(
        pack_kernel,
        out_shape=(
            jax.ShapeDtypeStruct((chunk // BLOCK * width + half, BLOCK), jnp.bfloat16),
            both,
            both,
            both,
            both,
        ),
        name="pack",
    )(q_wide, v_wide, q_narrow, k_narrow, v_narrow)


def attend_kernel(place, *refs, plans, slots, pieces, wide, diagonal, fill, size, width, chunk):
    chunks = len(plans)
    q_refs = refs[:chunks]
    src_refs = refs[chunks : chunks + slots * pieces]
    out_refs = refs[chunks + slots * pieces : 2 * chunks + slots * pieces]
    q_scr, kv_scr, acc, out_scr, sems, q_sems, out_sems = refs[2 * chunks + slots * pieces :]
    plans = [plan(place[0], place[1]) for plan in plans]
    scale = size ** (-0.5) * LOG2E
    key_rows = chunk if wide else chunk // 2
    halves = key_rows // LANES

    def slot_copies(slot):
        made = []
        begin = 0
        for k in range(pieces):
            rows = kv_scr.shape[1] // pieces
            source = src_refs[slot * pieces + k].at[pl.ds(0, rows), :]
            made.append(
                pltpu.make_async_copy(
                    source, kv_scr.at[slot, pl.ds(begin, rows), :], sems.at[slot, k]
                )
            )
            begin += rows
        return made

    def wait_slot(slot):
        begin = 0
        for k in range(pieces):
            rows = kv_scr.shape[1] // pieces
            source = src_refs[k].at[pl.ds(0, rows), :]
            pltpu.make_async_copy(
                source, kv_scr.at[slot, pl.ds(begin, rows), :], sems.at[slot, k]
            ).wait()
            begin += rows

    def only_map(rows, m):
        lane = lax.broadcasted_iota(jnp.int32, rows.shape, 1)
        return jnp.where((lane >= m * size) & (lane < (m + 1) * size), rows, 0)

    def dot_nt(left, right):
        return lax.dot_general(
            left, right, (((1,), (1,)), ((), ())), preferred_element_type=jnp.float32
        )

    def value_block(slot, j):
        return kv_scr[slot, pl.ds(key_rows + j * width, width), :]

    def store_result(n, m, columns, read, total, level):
        out_scr[n, pl.ds(m * width, width), columns] = (read * (1.0 / total)).astype(jnp.bfloat16)
        row = lax.broadcasted_iota(jnp.int32, (8, total.shape[1]), 0)
        packed = jnp.zeros((8, total.shape[1]), jnp.float32)
        for k in range(3):
            term = level.astype(jnp.bfloat16).astype(jnp.float32)
            packed = jnp.where(row == k, term, packed)
            level = level - term
        return packed

    def query_copy(source, n):
        rows = q_scr.shape[1]
        begin = 0 if wide else q_refs[source].shape[0] - rows
        return pltpu.make_async_copy(
            q_refs[source].at[pl.ds(begin, rows), :], q_scr.at[n], q_sems.at[n]
        )

    def within(slot, plan):
        active, count, offset = plan
        return (active > 0) & (slot >= offset) & (slot < offset + count)

    for n in range(chunks):

        @pl.when(plans[n][0] > 0)
        def _(n=n):
            query_copy(n, n).start()

    for slot in range(slots):
        used = within(slot, plans[0])
        for plan in plans[1:]:
            used = used | within(slot, plan)

        @pl.when(used)
        def _(slot=slot):
            for made in slot_copies(slot):
                made.start()

    def one_chunk(n, _):
        active, count, offset = plans[0]
        for k in range(1, chunks):
            active, count, offset = (
                jnp.where(n == k, new, old) for new, old in zip(plans[k], (active, count, offset))
            )
        pl.when(active > 0)(lambda: attend_chunk(n, count, offset))
        if fill:

            @pl.when(active == 0)
            def _():
                out_scr[n] = jnp.zeros(out_scr.shape[1:], out_scr.dtype)

        for k in range(chunks):

            @pl.when((n == k) & ((active > 0) | fill))
            def _(k=k):
                pltpu.make_async_copy(out_scr.at[k], out_refs[k], out_sems.at[k]).start()

        return 0

    def attend_chunk(n, count, offset):
        acc[...] = jnp.zeros_like(acc)
        query_copy(0, n).wait()

        def add_slot(number, totals):
            slot = 0 if diagonal else number + offset
            if chunks > 1:
                pl.when((n == 0) | jnp.logical_not(within(slot, plans[0])))(
                    lambda: wait_slot(slot)
                )
            else:
                wait_slot(slot)
            values = jnp.concatenate(
                [value_block(slot, j) for j in range(chunk // BLOCK)], axis=1
            )
            result = []
            for m in range(2):
                if wide:
                    lanes = slice(m * size, (m + 1) * size)
                    scores = dot_nt(kv_scr[slot, :key_rows, lanes], q_scr[n, :, lanes])
                else:
                    queries = only_map(
                        jnp.concatenate([q_scr[n, :, :LANES], q_scr[n, :, LANES:]], axis=0), m
                    )
                    scores = jnp.concatenate(
                        [
                            dot_nt(kv_scr[slot, :key_rows, side * LANES : (side + 1) * LANES], queries)
                            for side in range(2)
                        ],
                        axis=0,
                    )
                scores = scores * scale
                if diagonal:
                    key_pos = lax.broadcasted_iota(jnp.int32, scores.shape, 0)
                    query_pos = lax.broadcasted_iota(jnp.int32, scores.shape, 1)
                    scores = jnp.where(key_pos <= query_pos, scores, NEG_FILL)
                weights = jnp.exp2(scores)
                result.append(totals[m] + jnp.sum(weights.reshape(chunk // 8, 8, chunk), axis=0))
                acc[m] = acc[m] + jnp.dot(
                    values, weights.astype(jnp.bfloat16), preferred_element_type=jnp.float32
                )
            return tuple(result)

        none = jnp.zeros((8, chunk), jnp.float32)
        if diagonal:
            totals = add_slot(0, (none, none))
        else:
            totals = lax.fori_loop(0, count, add_slot, (none, none))
        outside = jnp.zeros((1, chunk), jnp.float32)
        stats = []
        for m in range(2):
            total = jnp.sum(totals[m], axis=0, keepdims=True)
            inside = (total >= LEAST_TOTAL) & (total <= MOST_TOTAL)
            outside = jnp.maximum(outside, jnp.where(inside, 0.0, 1.0))
            stats.append(store_result(n, m, slice(None), acc[m], total, jnp.log2(total)))
        out_scr[n, 2 * width :, :] = jnp.concatenate(stats, axis=0).astype(jnp.bfloat16)

        @pl.when(jnp.max(outside) > 0)
        def _():
            def packed_rows(take, number):
                made = []
                for k in range(2):
                    piece = number * 2 + k
                    place = pl.ds(pl.multiple_of(lax.rem(piece, halves) * LANES, LANES), LANES)
                    first, second = take(place)
                    made.append(jnp.where(piece < halves, first, second))
                return jnp.concatenate(made, axis=0)

            def keys_at(slot, number):
                return packed_rows(
                    lambda place: (kv_scr[slot, place, :LANES], kv_scr[slot, place, LANES:]), number
                )

            def queries_at(number):
                return packed_rows(
                    lambda place: (q_scr[n, place, :LANES], q_scr[n, place, LANES:]), number
                )

            def one_query_block(number, _):
                begin = pl.multiple_of(number * BLOCK, BLOCK)
                columns = pl.ds(begin, BLOCK)

                def one_map(m, packed):
                    acc[m, :, columns] = jnp.zeros((width, BLOCK), jnp.float32)

                    def careful(index, state):
                        peak, total = state
                        slot = index // (chunk // BLOCK) + offset
                        block = lax.rem(index, chunk // BLOCK)
                        place = pl.ds(pl.multiple_of(block * BLOCK, BLOCK), BLOCK)
                        if wide:
                            lanes = pl.ds(pl.multiple_of(m * size, size), size)
                            scores = dot_nt(kv_scr[slot, place, lanes], q_scr[n, columns, lanes])
                        else:
                            scores = dot_nt(keys_at(slot, block), only_map(queries_at(number), m))
                        scores = scores * scale
                        if diagonal:
                            key_pos = block * BLOCK + lax.broadcasted_iota(
                                jnp.int32, scores.shape, 0
                            )
                            query_pos = begin + lax.broadcasted_iota(jnp.int32, scores.shape, 1)
                            scores = jnp.where(key_pos <= query_pos, scores, NEG_FILL)
                        new_peak = jnp.maximum(peak, jnp.max(scores, axis=0, keepdims=True))
                        factor = jnp.exp2(peak - new_peak)
                        weights = jnp.exp2(scores - new_peak)
                        acc[m, :, columns] = factor * acc[m, :, columns] + jnp.dot(
                            value_block(slot, block),
                            weights.astype(jnp.bfloat16),
                            preferred_element_type=jnp.float32,
                        )
                        return new_peak, factor * total + jnp.sum(weights, axis=0, keepdims=True)

                    peak, total = lax.fori_loop(
                        0,
                        count * (chunk // BLOCK),
                        careful,
                        (
                            jnp.full((1, BLOCK), NEG_FILL, jnp.float32),
                            jnp.zeros((1, BLOCK), jnp.float32),
                        ),
                    )
                    rows = store_result(
                        n, m, columns, acc[m, :, columns], total, peak + jnp.log2(total)
                    )
                    both = jnp.concatenate([rows, rows], axis=0)
                    row = lax.broadcasted_iota(jnp.int32, both.shape, 0)
                    return jnp.where((row >= 8 * m) & (row < 8 * m + 8), both, packed)

                packed = lax.fori_loop(
                    0, 2, one_map, jnp.zeros((STAT_ROWS, BLOCK), jnp.float32)
                )
                out_scr[n, 2 * width :, columns] = packed.astype(jnp.bfloat16)
                return 0

            lax.fori_loop(0, chunk // BLOCK, one_query_block, 0)

    if chunks > 1:
        lax.fori_loop(0, chunks, one_chunk, 0)
    else:
        one_chunk(0, 0)
    for n in range(chunks):

        @pl.when((plans[n][0] > 0) | fill)
        def _(n=n):
            pltpu.make_async_copy(out_scr.at[n], out_refs[n], out_sems.at[n]).wait()


def attend(place, plans, queries, sources, wide, diagonal, fill, size, width, chunk):
    pieces = len(sources[0])
    flat = [array for group in sources for array in group]
    kv_rows = pieces * chunk
    chunks = len(plans)
    q_rows = chunk if wide else chunk // 2
    body = lambda *refs: attend_kernel(
        *refs,
        plans=plans,
        slots=len(sources),
        pieces=pieces,
        wide=wide,
        diagonal=diagonal,
        fill=fill,
        size=size,
        width=width,
        chunk=chunk,
    )
    area = chunk * chunk * 2 * 2 * chunks
    out = jax.ShapeDtypeStruct((2 * width + STAT_ROWS, chunk), jnp.bfloat16)
    return pl.pallas_call(
        body,
        out_shape=[out] * chunks,
        in_specs=[pl.BlockSpec(memory_space=pltpu.SMEM)]
        + [pl.BlockSpec(memory_space=pl.ANY)] * (chunks + len(flat)),
        out_specs=[pl.BlockSpec(memory_space=pl.ANY)] * chunks,
        scratch_shapes=[
            pltpu.VMEM((chunks, q_rows, BLOCK), jnp.bfloat16),
            pltpu.VMEM((len(sources), kv_rows, BLOCK), jnp.bfloat16),
            pltpu.VMEM((2, width, chunk), jnp.float32),
            pltpu.VMEM((chunks,) + out.shape, jnp.bfloat16),
            pltpu.SemaphoreType.DMA((len(sources), pieces)),
            pltpu.SemaphoreType.DMA((chunks,)),
            pltpu.SemaphoreType.DMA((chunks,)),
        ],
        cost_estimate=pl.CostEstimate(
            flops=2 * area * (size + width),
            transcendentals=area,
            bytes_accessed=len(sources) * kv_rows * 512,
        ),
    )(place, *queries, *flat)


def merge_kernel(place, lam, *refs, widths, counts):
    z, x = place[0], place[1]
    wide_valid = [z >= 0, x > 0] + [z >= d for d in WIDE_ORDER]
    narrow_valid = [z >= 0, z > 0] + [
        (z > 0) | (lax.rem(x + s, RING) < x) for s in NARROW_ORDER
    ]
    valid = (wide_valid, narrow_valid)
    out_ref = refs[-1]
    guarded = (1, None)
    begin = 0
    column = 0
    for group, (width, count) in enumerate(zip(widths, counts)):
        parts = refs[begin : begin + count]
        begin += count
        reads = []
        for m in range(2):
            levels = []
            for k, part in enumerate(parts):
                stats = part[2 * width :, :].astype(jnp.float32)
                level = stats[8 * m : 8 * m + 1] + stats[8 * m + 1 : 8 * m + 2] + stats[
                    8 * m + 2 : 8 * m + 3
                ]
                levels.append(jnp.where(valid[group][k], level, NEG_FILL))
            top = levels[0]
            for level in levels[1:]:
                top = jnp.maximum(top, level)
            shares = [jnp.exp2(level - top) for level in levels]
            whole = shares[0]
            for share in shares[1:]:
                whole = whole + share
            read = None
            for k, (share, part) in enumerate(zip(shares, parts)):
                term = part[m * width : (m + 1) * width, :].astype(jnp.float32) * (share / whole)
                if read is None:
                    read = term
                elif guarded[group] == k:
                    read = read + jnp.where(valid[group][k], term, 0.0)
                else:
                    read = read + term
            reads.append(read)
        mixed = reads[0] - lam[group, 0] * reads[1]
        normed = mixed * lax.rsqrt(jnp.mean(mixed * mixed, axis=0, keepdims=True) + 1e-06)
        out_ref[:, column : column + width] = normed.T.astype(jnp.bfloat16)
        column += width


def merge(place, lam, groups, widths):
    chunk = groups[0][0].shape[1]
    counts = [len(parts) for parts in groups]
    flat = [part for parts in groups for part in parts]
    body = lambda *refs: merge_kernel(*refs, widths=widths, counts=counts)
    return pl.pallas_call(
        body,
        grid=(chunk // BLOCK,),
        out_shape=jax.ShapeDtypeStruct((chunk, sum(widths)), jnp.bfloat16),
        in_specs=[pl.BlockSpec(memory_space=pltpu.SMEM)] * 2
        + [pl.BlockSpec((part.shape[0], BLOCK), lambda i: (0, i)) for part in flat],
        out_specs=pl.BlockSpec((BLOCK, sum(widths)), lambda i: (i, 0)),
        name="merge_reads",
    )(place, lam, *flat)


def around(array, axis, by):
    return lax.ppermute(array, axis, [(k, (k + by) % RING) for k in range(RING)])


def onward(array, axis, by):
    return lax.ppermute(
        array, axis, [(k, k + by) for k in range(RING) if 0 <= k + by < RING]
    )


def after(array, *others):
    return lax.optimization_barrier((array,) + others)[0]


def attention(
    query_wide, key_wide, value_wide, query_narrow, key_narrow, value_narrow, mix_lambda
):
    z = lax.axis_index("z")
    x = lax.axis_index("x")
    place = jnp.stack([z, x]).astype(jnp.int32)
    chunk = query_wide.shape[0]
    size_wide = query_wide.shape[1] // 2
    size_narrow = query_narrow.shape[1] // 2
    width_wide, width_narrow = value_wide.shape[1], value_narrow.shape[1]

    xk_near = around(key_wide, "x", 1)
    xk_back = around(key_wide, "x", -1)
    values, kv_narrow, plus, minus, two = pack(
        query_wide, value_wide, query_narrow, key_narrow, value_narrow
    )
    xv_back = around(values, "x", -1)
    xv_near = around(values, "x", 1)
    z_two = around(two, "z", 2)
    z_plus = around(plus, "z", 1)
    z_minus = around(minus, "z", -1)
    xv_far = around(xv_back[:chunk], "x", -1)
    xk_far = around(xk_near, "x", 1)
    xq_far = around(xv_near[chunk:], "x", 1)

    wide_sources = [(key_wide, values), (xk_near, xv_near), (xk_far, xv_far), (xk_back, xv_back)]
    narrow_sources = [(kv_narrow,), (z_plus,), (z_two,), (z_minus,)]
    q_later = {1: z_minus, 2: z_two, 3: z_plus}
    q_side = {1: xv_near, 2: xq_far, 3: xv_back}

    def wide_plan(d):
        return lambda z, x: ((z + d < RING).astype(jnp.int32), jnp.int32(RING), jnp.int32(0))

    def narrow_plan(s):
        def plan(z, x):
            level = (lax.rem(x - s + RING, RING) > x).astype(jnp.int32)
            return ((z > 0) | (level > 0)).astype(jnp.int32), z + level, 1 - level

        return plan

    def diag_plan(z, x):
        return jnp.int32(1), jnp.int32(1), jnp.int32(0)

    def wide_rest_plan(z, x):
        return (x > 0).astype(jnp.int32), x, jnp.int32(1)

    def narrow_rest_plan(z, x):
        return (z > 0).astype(jnp.int32), z, jnp.int32(1)

    def wide(last, plans, queries, sources, diagonal):
        given = after(place, last) if last is not None else place
        return attend(
            given, plans, queries, sources, True, diagonal, False, size_wide, width_wide, chunk
        )

    def narrow(last, plans, queries, sources, diagonal):
        return attend(
            after(place, last), plans, queries, sources, False, diagonal, not diagonal, size_narrow,
            width_narrow, chunk,
        )

    diag_wide = wide(None, (diag_plan,), [query_wide], wide_sources[:1], True)[0]
    diag_narrow = narrow(diag_wide, (diag_plan,), [values], narrow_sources[:1], True)[0]
    side, sent = {}, {}
    side[3] = narrow(diag_narrow, (narrow_plan(3),), [q_side[3]], narrow_sources, False)[0]
    sent[2] = wide(side[3], (wide_plan(2),), [q_later[2]], wide_sources, False)[0]
    relayed = lax.ppermute(sent[2], "z", [(0, 3), (1, 2)])
    sent[1], sent[3] = wide(
        sent[2], (wide_plan(1), wide_plan(3)), [q_later[1], q_later[3]], wide_sources, False,
    )
    side[1], side[2] = narrow(
        sent[1], (narrow_plan(1), narrow_plan(2)), [q_side[1], q_side[2]], narrow_sources, False,
    )
    for d in (1, 3):
        sent[d] = onward(sent[d], "z", d)
    rest_narrow = narrow(side[1], (narrow_rest_plan,), [values], narrow_sources, False)[0]
    sent[2] = lax.ppermute(after(relayed, rest_narrow), "z", [(3, 2), (2, 3)])
    rest_wide = wide(rest_narrow, (wide_rest_plan,), [query_wide], wide_sources, False)[0]
    side = {s: around(side[s], "x", -s) for s in NARROW_ORDER}
    made = merge(
        place,
        mix_lambda,
        (
            [diag_wide, rest_wide] + [sent[d] for d in WIDE_ORDER],
            [diag_narrow, rest_narrow] + [side[s] for s in NARROW_ORDER],
        ),
        (width_wide, width_narrow),
    )
    return made, values


def project_kernel(
    token_of, mine, weight_wide, weight_narrow, residual, gain, stream_out, rows_out,
    weights, left, total, flat_scr, rows, sems,
):
    heads, tokens, _ = mine.shape
    depth, model = weight_wide.shape
    wide = depth // heads
    tiles = model // LANES
    part = weights.shape[1]
    parts = weights.shape[0]
    for k in range(parts):
        if k * part < depth:
            source = weight_wide.at[pl.ds(k * part, part), :]
        else:
            source = weight_narrow.at[pl.ds(k * part - depth, part), :]
        pltpu.make_async_copy(source, weights.at[k], sems.at[k]).start()
    joined = jnp.concatenate(
        [mine[h, :, :wide] for h in range(heads)] + [mine[h, :, wide:] for h in range(heads)], axis=1
    )
    for k in range(parts):
        left[k] = joined[:, k * part : (k + 1) * part]
    total[...] = residual[...].astype(jnp.float32)

    def add_part(k, _):
        pltpu.make_async_copy(
            weight_wide.at[pl.ds(0, part), :], weights.at[k], sems.at[k]
        ).wait()
        total[...] = total[...] + jnp.dot(
            left[k], weights[k], preferred_element_type=jnp.float32
        )
        return 0

    lax.fori_loop(0, parts, add_part, 0)
    rounded = total[...].astype(jnp.bfloat16)
    stream_out[...] = rounded
    stream = rounded.astype(jnp.float32)
    inverse = lax.rsqrt(jnp.mean(stream * stream, axis=1, keepdims=True) + 1e-06)
    for j in range(tiles):
        lanes = slice(j * LANES, (j + 1) * LANES)
        flat_scr[pl.ds(j, tokens, stride=tiles), :] = stream[:, lanes] * inverse * gain[:, lanes]
    rows[...] = flat_scr[...].reshape(tokens, tiles, LANES).astype(jnp.bfloat16)

    def copy_row(slot, _):
        rows_out[slot] = rows[token_of[slot]]
        return 0

    lax.fori_loop(0, rows_out.shape[0], copy_row, 0, unroll=16)


def project(token_of, mine, weight_wide, weight_narrow, residual, gain):
    heads, tokens, depth = mine.shape
    model = weight_wide.shape[1]
    slots = token_of.shape[0]
    tiles = model // LANES
    part = 2 * BLOCK
    parts = heads * depth // part
    return pl.pallas_call(
        project_kernel,
        out_shape=(
            jax.ShapeDtypeStruct((tokens, model), jnp.bfloat16),
            jax.ShapeDtypeStruct((slots, tiles, LANES), jnp.bfloat16),
        ),
        in_specs=[
            pl.BlockSpec(memory_space=pltpu.SMEM),
            pl.BlockSpec(memory_space=pltpu.VMEM),
            pl.BlockSpec(memory_space=pltpu.HBM),
            pl.BlockSpec(memory_space=pltpu.HBM),
            pl.BlockSpec(memory_space=pltpu.VMEM),
            pl.BlockSpec(memory_space=pltpu.VMEM),
        ],
        out_specs=(pl.BlockSpec(memory_space=pltpu.VMEM),) * 2,
        scratch_shapes=[
            pltpu.VMEM((parts, part, model), jnp.bfloat16),
            pltpu.VMEM((parts, tokens, part), jnp.bfloat16),
            pltpu.VMEM((tokens, model), jnp.float32),
            pltpu.VMEM((tokens * tiles, LANES), jnp.float32),
            pltpu.VMEM((tokens, tiles, LANES), jnp.bfloat16),
            pltpu.SemaphoreType.DMA((parts,)),
        ],
        compiler_params=pltpu.CompilerParams(vmem_limit_bytes=48 * 1024 * 1024),
        name="project",
    )(token_of, mine, weight_wide, weight_narrow, residual, gain)


def expert_kernel(arrived, gate, up, down, out, flat, rows, hidden):
    count, tiles, _ = arrived.shape
    model, inner = gate.shape
    steps = inner // BLOCK
    columns = model // steps

    def spread(k, _):
        some = arrived[pl.ds(k * SOME, SOME)].astype(jnp.float32)
        flat[pl.ds(pl.multiple_of(k * SOME * tiles, LANES), SOME * tiles), :] = some.reshape(
            SOME * tiles, LANES
        )
        return 0

    def gathered(k, _):
        some = flat[pl.ds(pl.multiple_of(k * SOME * tiles, LANES), SOME * tiles), :]
        out[pl.ds(k * SOME, SOME)] = some.reshape(SOME, tiles, LANES).astype(jnp.bfloat16)
        return 0

    lax.fori_loop(0, count // SOME, spread, 0)
    for j in range(tiles):
        rows[:, j * LANES : (j + 1) * LANES] = flat[pl.ds(j, count, stride=tiles), :].astype(
            jnp.bfloat16
        )

    def widen(k, _):
        part = pl.ds(pl.multiple_of(k * BLOCK, BLOCK), BLOCK)
        gate_part = jnp.dot(rows[...], gate[:, part], preferred_element_type=jnp.float32)
        up_part = jnp.dot(rows[...], up[:, part], preferred_element_type=jnp.float32)
        hidden[:, part] = (gate_part * jax.nn.sigmoid(gate_part) * up_part).astype(jnp.bfloat16)
        return 0

    def narrow(k, _):
        result = jnp.dot(
            hidden[...],
            down[:, pl.ds(pl.multiple_of(k * columns, columns), columns)],
            preferred_element_type=jnp.float32,
        )
        for j in range(columns // LANES):
            flat[pl.ds(k * (columns // LANES) + j, count, stride=tiles), :] = result[
                :, j * LANES : (j + 1) * LANES
            ]
        return 0

    lax.fori_loop(0, steps, widen, 0)
    lax.fori_loop(0, steps, narrow, 0)
    lax.fori_loop(0, count // SOME, gathered, 0)


def experts(arrived, gate, up, down):
    count, tiles, _ = arrived.shape
    model, inner = gate.shape
    return pl.pallas_call(
        expert_kernel,
        out_shape=jax.ShapeDtypeStruct(arrived.shape, jnp.bfloat16),
        in_specs=[pl.BlockSpec(memory_space=pltpu.VMEM)] * 4,
        out_specs=pl.BlockSpec(memory_space=pltpu.VMEM),
        scratch_shapes=[
            pltpu.VMEM((count * tiles, LANES), jnp.float32),
            pltpu.VMEM((count, model), jnp.bfloat16),
            pltpu.VMEM((count, inner), jnp.bfloat16),
        ],
        compiler_params=pltpu.CompilerParams(vmem_limit_bytes=28*1024*1024),
        name="experts",
    )(arrived, gate, up, down)


def combine_kernel(slot_of, share_of, returned, stream, out, flat):
    tokens, model = stream.shape
    tiles = model // LANES

    def one_token(token, _):
        total = share_of[2 * token] * returned[slot_of[2 * token]].astype(jnp.float32)
        total = total + share_of[2 * token + 1] * returned[slot_of[2 * token + 1]].astype(
            jnp.float32
        )
        flat[pl.ds(pl.multiple_of(token * tiles, tiles), tiles), :] = total
        return 0

    lax.fori_loop(0, tokens, one_token, 0, unroll=8)
    for j in range(tiles):
        lanes = slice(j * LANES, (j + 1) * LANES)
        out[:, lanes] = (
            stream[:, lanes].astype(jnp.float32) + flat[pl.ds(j, tokens, stride=tiles), :]
        ).astype(jnp.bfloat16)


def combine(slot_of, share_of, returned, stream):
    tokens, model = stream.shape
    return pl.pallas_call(
        combine_kernel,
        out_shape=jax.ShapeDtypeStruct(stream.shape, jnp.bfloat16),
        in_specs=[pl.BlockSpec(memory_space=pltpu.SMEM)] * 2
        + [pl.BlockSpec(memory_space=pltpu.VMEM)] * 2,
        out_specs=pl.BlockSpec(memory_space=pltpu.VMEM),
        scratch_shapes=[pltpu.VMEM((tokens * (model // LANES), LANES), jnp.float32)],
        compiler_params=pltpu.CompilerParams(vmem_limit_bytes=16 * 1024 * 1024),
        name="combine",
    )(slot_of, share_of, returned, stream)


def slot_tables(expert_ids, experts_all, capacity):
    flat_expert = expert_ids.reshape(-1)
    order = jnp.arange(flat_expert.shape[0], dtype=jnp.int32)
    earlier = (flat_expert[:, None] == flat_expert[None, :]) & (order[None, :] < order[:, None])
    slot_of = flat_expert * capacity + jnp.sum(earlier.astype(jnp.int32), axis=1)
    slot_ids = jnp.arange(experts_all * capacity, dtype=jnp.int32)
    placed = slot_ids[:, None] == slot_of[None, :]
    token_of = jnp.sum(jnp.where(placed, order[None, :] // 2, 0), axis=1)
    return slot_of, token_of


def shards(
    query_wide,
    key_wide,
    value_wide,
    query_narrow,
    key_narrow,
    value_narrow,
    mix_lambda,
    residual_in,
    out_wide,
    out_narrow,
    ffn_gain,
    expert_ids,
    expert_weights,
    gate_weight,
    up_weight,
    down_weight,
):
    heads, packed = attention(
        query_wide[:, 0],
        key_wide[:, 0],
        value_wide[:, 0],
        query_narrow[:, 0],
        key_narrow[:, 0],
        value_narrow[:, 0],
        mix_lambda,
    )
    tp_size = lax.axis_size(TP)
    local_rows = heads.shape[0] // tp_size
    experts_all = lax.axis_size(SP_TP)
    capacity = max(2, 4 * local_rows // experts_all)
    slot_of, token_of = slot_tables(expert_ids, experts_all, capacity)
    out_wide, out_narrow, _ = lax.optimization_barrier((out_wide, out_narrow, packed))
    whole_wide = lax.all_gather(out_wide, TP, axis=0, tiled=True)
    whole_narrow = lax.all_gather(out_narrow, TP, axis=0, tiled=True)
    mine = lax.all_to_all(
        heads.reshape(tp_size, local_rows, -1), TP, split_axis=0, concat_axis=0, tiled=True
    )
    stream, outgoing = project(
        token_of, mine, whole_wide, whole_narrow, residual_in, ffn_gain[None, :]
    )

    def exchanged(rows):
        shape = rows.shape
        moved = lax.all_to_all(
            rows.reshape(experts_all, -1, LANES), SP_TP, split_axis=0, concat_axis=0, tiled=True
        )
        return moved.reshape(shape)

    result = experts(exchanged(outgoing), gate_weight[0], up_weight[0], down_weight[0])
    return combine(slot_of, expert_weights.reshape(-1), exchanged(result), stream)


def solution(mesh):
    finer = Mesh(mesh.devices.reshape(4, 4, 4, 2), SP_TP)
    sp = ("z", "x")
    placed = (
        P(sp, TP, None),
        P(sp, TP, None),
        P(sp, TP, None),
        P(sp, TP, None),
        P(sp, TP, None),
        P(sp, TP, None),
        P(None, TP),
        P(SP_TP, None),
        P(TP, None),
        P(TP, None),
        P(),
        P(SP_TP, None),
        P(SP_TP, None),
        P(SP_TP, None, None),
        P(SP_TP, None, None),
        P(SP_TP, None, None),
    )
    return jax.shard_map(
        shards, mesh=finer, in_specs=placed, out_specs=P(SP_TP, None), check_vma=False
    )
```

```python
import jax
import jax.numpy as jnp
from jax import lax
from jax.experimental import pallas as pl
from jax.experimental.pallas import tpu as pltpu
from jax.sharding import Mesh
from jax.sharding import PartitionSpec as P

TP = ("y", "c")
SP_TP = ("z", "x", "y", "c")
RING = 4
LOG2E = 1.4426950408889634
NEG_FILL = -1e30
STAT_ROWS = 16
LANES = 128
BLOCK = 256
SOME = 48
WIDE_ORDER = (2, 1, 3)
NARROW_ORDER = (3, 1, 2)
LEAST_TOTAL = 2.0**-60
MOST_TOTAL = 2.0**100


def pack_kernel(
    q_wide, v_wide, q_narrow, k_narrow, v_narrow, v_out, kv_out, plus_out, minus_out, two_out
):
    z = lax.axis_index("z")
    chunk, width = v_wide.shape
    half = chunk // 2
    width_narrow = v_narrow.shape[1]
    behind = chunk // BLOCK * width
    for j in range(chunk // BLOCK):
        rows = slice(j * BLOCK, (j + 1) * BLOCK)
        v_out[j * width : (j + 1) * width, :] = v_wide[rows, :].T
        begin = half + j * width_narrow
        kv_out[begin : begin + width_narrow, :] = v_narrow[rows, :].T
    for side in range(2):
        lanes = slice(side * LANES, (side + 1) * LANES)
        rows = slice(side * half, (side + 1) * half)
        kv_out[:half, lanes] = k_narrow[rows, :]
        v_out[behind : behind + half, lanes] = q_narrow[rows, :]
    for out, gives_queries in (
        (plus_out, z == RING - 1),
        (minus_out, z > 0),
        (two_out, z >= RING // 2),
    ):

        @pl.when(gives_queries)
        def _(out=out):
            out[...] = q_wide[...]

        @pl.when(jnp.logical_not(gives_queries))
        def _(out=out):
            out[...] = kv_out[...]


def pack(q_wide, v_wide, q_narrow, k_narrow, v_narrow):
    chunk, width = v_wide.shape
    half = chunk // 2
    both = jax.ShapeDtypeStruct(q_wide.shape, jnp.bfloat16)
    assert half + chunk // BLOCK * v_narrow.shape[1] == chunk
    return pl.pallas_call(
        pack_kernel,
        out_shape=(
            jax.ShapeDtypeStruct((chunk // BLOCK * width + half, BLOCK), jnp.bfloat16),
            both,
            both,
            both,
            both,
        ),
        name="pack",
    )(q_wide, v_wide, q_narrow, k_narrow, v_narrow)


def attend_kernel(place, *refs, plans, slots, pieces, wide, diagonal, fill, size, width, chunk):
    chunks = len(plans)
    q_refs = refs[:chunks]
    src_refs = refs[chunks : chunks + slots * pieces]
    out_refs = refs[chunks + slots * pieces : 2 * chunks + slots * pieces]
    q_scr, kv_scr, acc, out_scr, sems, q_sems, out_sems = refs[2 * chunks + slots * pieces :]
    plans = [plan(place[0], place[1]) for plan in plans]
    scale = size ** (-0.5) * LOG2E
    key_rows = chunk if wide else chunk // 2
    halves = key_rows // LANES

    def slot_copies(slot):
        made = []
        begin = 0
        for k in range(pieces):
            rows = kv_scr.shape[1] // pieces
            source = src_refs[slot * pieces + k].at[pl.ds(0, rows), :]
            made.append(
                pltpu.make_async_copy(
                    source, kv_scr.at[slot, pl.ds(begin, rows), :], sems.at[slot, k]
                )
            )
            begin += rows
        return made

    def wait_slot(slot):
        begin = 0
        for k in range(pieces):
            rows = kv_scr.shape[1] // pieces
            source = src_refs[k].at[pl.ds(0, rows), :]
            pltpu.make_async_copy(
                source, kv_scr.at[slot, pl.ds(begin, rows), :], sems.at[slot, k]
            ).wait()
            begin += rows

    def only_map(rows, m):
        lane = lax.broadcasted_iota(jnp.int32, rows.shape, 1)
        return jnp.where((lane >= m * size) & (lane < (m + 1) * size), rows, 0)

    def dot_nt(left, right):
        return lax.dot_general(
            left, right, (((1,), (1,)), ((), ())), preferred_element_type=jnp.float32
        )

    def value_block(slot, j):
        return kv_scr[slot, pl.ds(key_rows + j * width, width), :]

    def store_result(n, m, columns, read, total, level):
        out_scr[n, pl.ds(m * width, width), columns] = (read * (1.0 / total)).astype(jnp.bfloat16)
        row = lax.broadcasted_iota(jnp.int32, (8, total.shape[1]), 0)
        packed = jnp.zeros((8, total.shape[1]), jnp.float32)
        for k in range(3):
            term = level.astype(jnp.bfloat16).astype(jnp.float32)
            packed = jnp.where(row == k, term, packed)
            level = level - term
        return packed

    def query_copy(source, n):
        rows = q_scr.shape[1]
        begin = 0 if wide else q_refs[source].shape[0] - rows
        return pltpu.make_async_copy(
            q_refs[source].at[pl.ds(begin, rows), :], q_scr.at[n], q_sems.at[n]
        )

    def within(slot, plan):
        active, count, offset = plan
        return (active > 0) & (slot >= offset) & (slot < offset + count)

    for n in range(chunks):

        @pl.when(plans[n][0] > 0)
        def _(n=n):
            query_copy(n, n).start()

    for slot in range(slots):
        used = within(slot, plans[0])
        for plan in plans[1:]:
            used = used | within(slot, plan)

        @pl.when(used)
        def _(slot=slot):
            for made in slot_copies(slot):
                made.start()

    def one_chunk(n, _):
        active, count, offset = plans[0]
        for k in range(1, chunks):
            active, count, offset = (
                jnp.where(n == k, new, old) for new, old in zip(plans[k], (active, count, offset))
            )
        pl.when(active > 0)(lambda: attend_chunk(n, count, offset))
        if fill:

            @pl.when(active == 0)
            def _():
                out_scr[n] = jnp.zeros(out_scr.shape[1:], out_scr.dtype)

        for k in range(chunks):

            @pl.when((n == k) & ((active > 0) | fill))
            def _(k=k):
                pltpu.make_async_copy(out_scr.at[k], out_refs[k], out_sems.at[k]).start()

        return 0

    def attend_chunk(n, count, offset):
        acc[...] = jnp.zeros_like(acc)
        query_copy(0, n).wait()

        def add_slot(number, totals):
            slot = 0 if diagonal else number + offset
            if chunks > 1:
                pl.when((n == 0) | jnp.logical_not(within(slot, plans[0])))(
                    lambda: wait_slot(slot)
                )
            else:
                wait_slot(slot)
            values = jnp.concatenate(
                [value_block(slot, j) for j in range(chunk // BLOCK)], axis=1
            )
            result = []
            for m in range(2):
                if wide:
                    lanes = slice(m * size, (m + 1) * size)
                    scores = dot_nt(kv_scr[slot, :key_rows, lanes], q_scr[n, :, lanes])
                else:
                    queries = only_map(
                        jnp.concatenate([q_scr[n, :, :LANES], q_scr[n, :, LANES:]], axis=0), m
                    )
                    scores = jnp.concatenate(
                        [
                            dot_nt(kv_scr[slot, :key_rows, side * LANES : (side + 1) * LANES], queries)
                            for side in range(2)
                        ],
                        axis=0,
                    )
                scores = scores * scale
                if diagonal:
                    key_pos = lax.broadcasted_iota(jnp.int32, scores.shape, 0)
                    query_pos = lax.broadcasted_iota(jnp.int32, scores.shape, 1)
                    scores = jnp.where(key_pos <= query_pos, scores, NEG_FILL)
                weights = jnp.exp2(scores)
                result.append(totals[m] + jnp.sum(weights.reshape(chunk // 8, 8, chunk), axis=0))
                acc[m] = acc[m] + jnp.dot(
                    values, weights.astype(jnp.bfloat16), preferred_element_type=jnp.float32
                )
            return tuple(result)

        none = jnp.zeros((8, chunk), jnp.float32)
        if diagonal:
            totals = add_slot(0, (none, none))
        else:
            totals = lax.fori_loop(0, count, add_slot, (none, none))
        outside = jnp.zeros((1, chunk), jnp.float32)
        stats = []
        for m in range(2):
            total = jnp.sum(totals[m], axis=0, keepdims=True)
            inside = (total >= LEAST_TOTAL) & (total <= MOST_TOTAL)
            outside = jnp.maximum(outside, jnp.where(inside, 0.0, 1.0))
            stats.append(store_result(n, m, slice(None), acc[m], total, jnp.log2(total)))
        out_scr[n, 2 * width :, :] = jnp.concatenate(stats, axis=0).astype(jnp.bfloat16)

        @pl.when(jnp.max(outside) > 0)
        def _():
            def packed_rows(take, number):
                made = []
                for k in range(2):
                    piece = number * 2 + k
                    place = pl.ds(pl.multiple_of(lax.rem(piece, halves) * LANES, LANES), LANES)
                    first, second = take(place)
                    made.append(jnp.where(piece < halves, first, second))
                return jnp.concatenate(made, axis=0)

            def keys_at(slot, number):
                return packed_rows(
                    lambda place: (kv_scr[slot, place, :LANES], kv_scr[slot, place, LANES:]), number
                )

            def queries_at(number):
                return packed_rows(
                    lambda place: (q_scr[n, place, :LANES], q_scr[n, place, LANES:]), number
                )

            def one_query_block(number, _):
                begin = pl.multiple_of(number * BLOCK, BLOCK)
                columns = pl.ds(begin, BLOCK)

                def one_map(m, packed):
                    acc[m, :, columns] = jnp.zeros((width, BLOCK), jnp.float32)

                    def careful(index, state):
                        peak, total = state
                        slot = index // (chunk // BLOCK) + offset
                        block = lax.rem(index, chunk // BLOCK)
                        place = pl.ds(pl.multiple_of(block * BLOCK, BLOCK), BLOCK)
                        if wide:
                            lanes = pl.ds(pl.multiple_of(m * size, size), size)
                            scores = dot_nt(kv_scr[slot, place, lanes], q_scr[n, columns, lanes])
                        else:
                            scores = dot_nt(keys_at(slot, block), only_map(queries_at(number), m))
                        scores = scores * scale
                        if diagonal:
                            key_pos = block * BLOCK + lax.broadcasted_iota(
                                jnp.int32, scores.shape, 0
                            )
                            query_pos = begin + lax.broadcasted_iota(jnp.int32, scores.shape, 1)
                            scores = jnp.where(key_pos <= query_pos, scores, NEG_FILL)
                        new_peak = jnp.maximum(peak, jnp.max(scores, axis=0, keepdims=True))
                        factor = jnp.exp2(peak - new_peak)
                        weights = jnp.exp2(scores - new_peak)
                        acc[m, :, columns] = factor * acc[m, :, columns] + jnp.dot(
                            value_block(slot, block),
                            weights.astype(jnp.bfloat16),
                            preferred_element_type=jnp.float32,
                        )
                        return new_peak, factor * total + jnp.sum(weights, axis=0, keepdims=True)

                    peak, total = lax.fori_loop(
                        0,
                        count * (chunk // BLOCK),
                        careful,
                        (
                            jnp.full((1, BLOCK), NEG_FILL, jnp.float32),
                            jnp.zeros((1, BLOCK), jnp.float32),
                        ),
                    )
                    rows = store_result(
                        n, m, columns, acc[m, :, columns], total, peak + jnp.log2(total)
                    )
                    both = jnp.concatenate([rows, rows], axis=0)
                    row = lax.broadcasted_iota(jnp.int32, both.shape, 0)
                    return jnp.where((row >= 8 * m) & (row < 8 * m + 8), both, packed)

                packed = lax.fori_loop(
                    0, 2, one_map, jnp.zeros((STAT_ROWS, BLOCK), jnp.float32)
                )
                out_scr[n, 2 * width :, columns] = packed.astype(jnp.bfloat16)
                return 0

            lax.fori_loop(0, chunk // BLOCK, one_query_block, 0)

    if chunks > 1:
        lax.fori_loop(0, chunks, one_chunk, 0)
    else:
        one_chunk(0, 0)
    for n in range(chunks):

        @pl.when((plans[n][0] > 0) | fill)
        def _(n=n):
            pltpu.make_async_copy(out_scr.at[n], out_refs[n], out_sems.at[n]).wait()


def attend(place, plans, queries, sources, wide, diagonal, fill, size, width, chunk):
    pieces = len(sources[0])
    flat = [array for group in sources for array in group]
    kv_rows = pieces * chunk
    chunks = len(plans)
    q_rows = chunk if wide else chunk // 2
    body = lambda *refs: attend_kernel(
        *refs,
        plans=plans,
        slots=len(sources),
        pieces=pieces,
        wide=wide,
        diagonal=diagonal,
        fill=fill,
        size=size,
        width=width,
        chunk=chunk,
    )
    area = chunk * chunk * 2 * 2 * chunks
    out = jax.ShapeDtypeStruct((2 * width + STAT_ROWS, chunk), jnp.bfloat16)
    return pl.pallas_call(
        body,
        out_shape=[out] * chunks,
        in_specs=[pl.BlockSpec(memory_space=pltpu.SMEM)]
        + [pl.BlockSpec(memory_space=pl.ANY)] * (chunks + len(flat)),
        out_specs=[pl.BlockSpec(memory_space=pl.ANY)] * chunks,
        scratch_shapes=[
            pltpu.VMEM((chunks, q_rows, BLOCK), jnp.bfloat16),
            pltpu.VMEM((len(sources), kv_rows, BLOCK), jnp.bfloat16),
            pltpu.VMEM((2, width, chunk), jnp.float32),
            pltpu.VMEM((chunks,) + out.shape, jnp.bfloat16),
            pltpu.SemaphoreType.DMA((len(sources), pieces)),
            pltpu.SemaphoreType.DMA((chunks,)),
            pltpu.SemaphoreType.DMA((chunks,)),
        ],
        cost_estimate=pl.CostEstimate(
            flops=2 * area * (size + width),
            transcendentals=area,
            bytes_accessed=len(sources) * kv_rows * 512,
        ),
    )(place, *queries, *flat)


def merge_kernel(place, lam, *refs, widths, counts):
    z, x = place[0], place[1]
    wide_valid = [z >= 0, x > 0] + [z >= d for d in WIDE_ORDER]
    narrow_valid = [z >= 0, z > 0] + [
        (z > 0) | (lax.rem(x + s, RING) < x) for s in NARROW_ORDER
    ]
    valid = (wide_valid, narrow_valid)
    out_ref = refs[-1]
    guarded = (1, None)
    begin = 0
    column = 0
    for group, (width, count) in enumerate(zip(widths, counts)):
        parts = refs[begin : begin + count]
        begin += count
        reads = []
        for m in range(2):
            levels = []
            for k, part in enumerate(parts):
                stats = part[2 * width :, :].astype(jnp.float32)
                level = stats[8 * m : 8 * m + 1] + stats[8 * m + 1 : 8 * m + 2] + stats[
                    8 * m + 2 : 8 * m + 3
                ]
                levels.append(jnp.where(valid[group][k], level, NEG_FILL))
            top = levels[0]
            for level in levels[1:]:
                top = jnp.maximum(top, level)
            shares = [jnp.exp2(level - top) for level in levels]
            whole = shares[0]
            for share in shares[1:]:
                whole = whole + share
            read = None
            for k, (share, part) in enumerate(zip(shares, parts)):
                term = part[m * width : (m + 1) * width, :].astype(jnp.float32) * (share / whole)
                if read is None:
                    read = term
                elif guarded[group] == k:
                    read = read + jnp.where(valid[group][k], term, 0.0)
                else:
                    read = read + term
            reads.append(read)
        mixed = reads[0] - lam[group, 0] * reads[1]
        normed = mixed * lax.rsqrt(jnp.mean(mixed * mixed, axis=0, keepdims=True) + 1e-06)
        out_ref[:, column : column + width] = normed.T.astype(jnp.bfloat16)
        column += width


def merge(place, lam, groups, widths):
    chunk = groups[0][0].shape[1]
    block = chunk // 2
    counts = [len(parts) for parts in groups]
    flat = [part for parts in groups for part in parts]
    body = lambda *refs: merge_kernel(*refs, widths=widths, counts=counts)
    return pl.pallas_call(
        body,
        grid=(chunk // block,),
        out_shape=jax.ShapeDtypeStruct((chunk, sum(widths)), jnp.bfloat16),
        in_specs=[pl.BlockSpec(memory_space=pltpu.SMEM)] * 2
        + [pl.BlockSpec((part.shape[0], block), lambda i: (0, i)) for part in flat],
        out_specs=pl.BlockSpec((block, sum(widths)), lambda i: (i, 0)),
        name="merge_reads",
    )(place, lam, *flat)


def around(array, axis, by):
    return lax.ppermute(array, axis, [(k, (k + by) % RING) for k in range(RING)])


def onward(array, axis, by):
    return lax.ppermute(
        array, axis, [(k, k + by) for k in range(RING) if 0 <= k + by < RING]
    )


def after(array, *others):
    return lax.optimization_barrier((array,) + others)[0]


def attention(
    query_wide, key_wide, value_wide, query_narrow, key_narrow, value_narrow, mix_lambda
):
    z = lax.axis_index("z")
    x = lax.axis_index("x")
    place = jnp.stack([z, x]).astype(jnp.int32)
    chunk = query_wide.shape[0]
    size_wide = query_wide.shape[1] // 2
    size_narrow = query_narrow.shape[1] // 2
    width_wide, width_narrow = value_wide.shape[1], value_narrow.shape[1]

    xk_near = around(key_wide, "x", 1)
    xk_back = around(key_wide, "x", -1)
    values, kv_narrow, plus, minus, two = pack(
        query_wide, value_wide, query_narrow, key_narrow, value_narrow
    )
    xv_back = around(values, "x", -1)
    xv_near = around(values, "x", 1)
    z_two = around(two, "z", 2)
    z_plus = around(plus, "z", 1)
    z_minus = around(minus, "z", -1)
    xv_far = around(xv_back[:chunk], "x", -1)
    xk_far = around(xk_near, "x", 1)
    xq_far = around(xv_near[chunk:], "x", 1)

    wide_sources = [(key_wide, values), (xk_near, xv_near), (xk_far, xv_far), (xk_back, xv_back)]
    narrow_sources = [(kv_narrow,), (z_plus,), (z_two,), (z_minus,)]
    q_later = {1: z_minus, 2: z_two, 3: z_plus}
    q_side = {1: xv_near, 2: xq_far, 3: xv_back}

    def wide_plan(d):
        return lambda z, x: ((z + d < RING).astype(jnp.int32), jnp.int32(RING), jnp.int32(0))

    def narrow_plan(s):
        def plan(z, x):
            level = (lax.rem(x - s + RING, RING) > x).astype(jnp.int32)
            return ((z > 0) | (level > 0)).astype(jnp.int32), z + level, 1 - level

        return plan

    def diag_plan(z, x):
        return jnp.int32(1), jnp.int32(1), jnp.int32(0)

    def wide_rest_plan(z, x):
        return (x > 0).astype(jnp.int32), x, jnp.int32(1)

    def narrow_rest_plan(z, x):
        return (z > 0).astype(jnp.int32), z, jnp.int32(1)

    def wide(last, plans, queries, sources, diagonal):
        given = after(place, last) if last is not None else place
        return attend(
            given, plans, queries, sources, True, diagonal, False, size_wide, width_wide, chunk
        )

    def narrow(last, plans, queries, sources, diagonal):
        return attend(
            after(place, last), plans, queries, sources, False, diagonal, not diagonal, size_narrow,
            width_narrow, chunk,
        )

    diag_wide = wide(None, (diag_plan,), [query_wide], wide_sources[:1], True)[0]
    diag_narrow = narrow(diag_wide, (diag_plan,), [values], narrow_sources[:1], True)[0]
    side, sent = {}, {}
    side[3] = narrow(diag_narrow, (narrow_plan(3),), [q_side[3]], narrow_sources, False)[0]
    sent[2] = wide(side[3], (wide_plan(2),), [q_later[2]], wide_sources, False)[0]
    relayed = lax.ppermute(sent[2], "z", [(0, 3), (1, 2)])
    sent[1], sent[3] = wide(
        sent[2], (wide_plan(1), wide_plan(3)), [q_later[1], q_later[3]], wide_sources, False,
    )
    side[1], side[2] = narrow(
        sent[1], (narrow_plan(1), narrow_plan(2)), [q_side[1], q_side[2]], narrow_sources, False,
    )
    for d in (1, 3):
        sent[d] = onward(sent[d], "z", d)
    sent[2] = lax.ppermute(after(relayed, side[1]), "z", [(3, 2), (2, 3)])
    rest_narrow = narrow(side[1], (narrow_rest_plan,), [values], narrow_sources, False)[0]
    rest_wide = wide(rest_narrow, (wide_rest_plan,), [query_wide], wide_sources, False)[0]
    side = {s: around(side[s], "x", -s) for s in NARROW_ORDER}
    made = merge(
        place,
        mix_lambda,
        (
            [diag_wide, rest_wide] + [sent[d] for d in WIDE_ORDER],
            [diag_narrow, rest_narrow] + [side[s] for s in NARROW_ORDER],
        ),
        (width_wide, width_narrow),
    )
    return made, values


def project_kernel(
    token_of, mine, weight_wide, weight_narrow, residual, gain, stream_out, rows_out,
    weights, left, total, flat_scr, rows, sems,
):
    heads, tokens, _ = mine.shape
    depth, model = weight_wide.shape
    wide = depth // heads
    tiles = model // LANES
    part = weights.shape[1]
    parts = weights.shape[0]
    for k in range(parts):
        if k * part < depth:
            source = weight_wide.at[pl.ds(k * part, part), :]
        else:
            source = weight_narrow.at[pl.ds(k * part - depth, part), :]
        pltpu.make_async_copy(source, weights.at[k], sems.at[k]).start()
    joined = jnp.concatenate(
        [mine[h, :, :wide] for h in range(heads)] + [mine[h, :, wide:] for h in range(heads)], axis=1
    )
    for k in range(parts):
        left[k] = joined[:, k * part : (k + 1) * part]
    total[...] = residual[...].astype(jnp.float32)

    def add_part(k, _):
        pltpu.make_async_copy(
            weight_wide.at[pl.ds(0, part), :], weights.at[k], sems.at[k]
        ).wait()
        total[...] = total[...] + jnp.dot(
            left[k], weights[k], preferred_element_type=jnp.float32
        )
        return 0

    lax.fori_loop(0, parts, add_part, 0)
    rounded = total[...].astype(jnp.bfloat16)
    stream_out[...] = rounded
    stream = rounded.astype(jnp.float32)
    inverse = lax.rsqrt(jnp.mean(stream * stream, axis=1, keepdims=True) + 1e-06)
    for j in range(tiles):
        lanes = slice(j * LANES, (j + 1) * LANES)
        flat_scr[pl.ds(j, tokens, stride=tiles), :] = stream[:, lanes] * inverse * gain[:, lanes]
    rows[...] = flat_scr[...].reshape(tokens, tiles, LANES).astype(jnp.bfloat16)

    def copy_row(slot, _):
        rows_out[slot] = rows[token_of[slot]]
        return 0

    lax.fori_loop(0, rows_out.shape[0], copy_row, 0, unroll=16)


def project(token_of, mine, weight_wide, weight_narrow, residual, gain):
    heads, tokens, depth = mine.shape
    model = weight_wide.shape[1]
    slots = token_of.shape[0]
    tiles = model // LANES
    part = 2 * BLOCK
    parts = heads * depth // part
    return pl.pallas_call(
        project_kernel,
        out_shape=(
            jax.ShapeDtypeStruct((tokens, model), jnp.bfloat16),
            jax.ShapeDtypeStruct((slots, tiles, LANES), jnp.bfloat16),
        ),
        in_specs=[
            pl.BlockSpec(memory_space=pltpu.SMEM),
            pl.BlockSpec(memory_space=pltpu.VMEM),
            pl.BlockSpec(memory_space=pltpu.HBM),
            pl.BlockSpec(memory_space=pltpu.HBM),
            pl.BlockSpec(memory_space=pltpu.VMEM),
            pl.BlockSpec(memory_space=pltpu.VMEM),
        ],
        out_specs=(pl.BlockSpec(memory_space=pltpu.VMEM),) * 2,
        scratch_shapes=[
            pltpu.VMEM((parts, part, model), jnp.bfloat16),
            pltpu.VMEM((parts, tokens, part), jnp.bfloat16),
            pltpu.VMEM((tokens, model), jnp.float32),
            pltpu.VMEM((tokens * tiles, LANES), jnp.float32),
            pltpu.VMEM((tokens, tiles, LANES), jnp.bfloat16),
            pltpu.SemaphoreType.DMA((parts,)),
        ],
        compiler_params=pltpu.CompilerParams(vmem_limit_bytes=48 * 1024 * 1024),
        name="project",
    )(token_of, mine, weight_wide, weight_narrow, residual, gain)


def expert_kernel(arrived, gate, up, down, out, flat, rows, hidden):
    count, tiles, _ = arrived.shape

    def spread(k, _):
        some = arrived[pl.ds(k * SOME, SOME)].astype(jnp.float32)
        flat[pl.ds(pl.multiple_of(k * SOME * tiles, LANES), SOME * tiles), :] = some.reshape(
            SOME * tiles, LANES
        )
        return 0

    def gathered(k, _):
        some = flat[pl.ds(pl.multiple_of(k * SOME * tiles, LANES), SOME * tiles), :]
        out[pl.ds(k * SOME, SOME)] = some.reshape(SOME, tiles, LANES).astype(jnp.bfloat16)
        return 0

    lax.fori_loop(0, count // SOME, spread, 0)
    for j in range(tiles):
        rows[:, j * LANES : (j + 1) * LANES] = flat[pl.ds(j, count, stride=tiles), :].astype(
            jnp.bfloat16
        )

    gate_part = jnp.dot(rows[...], gate[...], preferred_element_type=jnp.float32)
    up_part = jnp.dot(rows[...], up[...], preferred_element_type=jnp.float32)
    hidden[...] = (gate_part * jax.nn.sigmoid(gate_part) * up_part).astype(jnp.bfloat16)
    result = jnp.dot(hidden[...], down[...], preferred_element_type=jnp.float32)
    for j in range(tiles):
        flat[pl.ds(j, count, stride=tiles), :] = result[:, j * LANES : (j + 1) * LANES]
    lax.fori_loop(0, count // SOME, gathered, 0)


def experts(arrived, gate, up, down):
    count, tiles, _ = arrived.shape
    model, inner = gate.shape
    return pl.pallas_call(
        expert_kernel,
        out_shape=jax.ShapeDtypeStruct(arrived.shape, jnp.bfloat16),
        in_specs=[pl.BlockSpec(memory_space=pltpu.VMEM)] * 4,
        out_specs=pl.BlockSpec(memory_space=pltpu.VMEM),
        scratch_shapes=[
            pltpu.VMEM((count * tiles, LANES), jnp.float32),
            pltpu.VMEM((count, model), jnp.bfloat16),
            pltpu.VMEM((count, inner), jnp.bfloat16),
        ],
        compiler_params=pltpu.CompilerParams(vmem_limit_bytes=28*1024*1024),
        name="experts",
    )(arrived, gate, up, down)


def combine_kernel(slot_of, share_of, returned, stream, out, flat):
    tokens, model = stream.shape
    tiles = model // LANES

    def one_token(token, _):
        total = share_of[2 * token] * returned[slot_of[2 * token]].astype(jnp.float32)
        total = total + share_of[2 * token + 1] * returned[slot_of[2 * token + 1]].astype(
            jnp.float32
        )
        flat[pl.ds(pl.multiple_of(token * tiles, tiles), tiles), :] = total
        return 0

    lax.fori_loop(0, tokens, one_token, 0, unroll=8)
    for j in range(tiles):
        lanes = slice(j * LANES, (j + 1) * LANES)
        out[:, lanes] = (
            stream[:, lanes].astype(jnp.float32) + flat[pl.ds(j, tokens, stride=tiles), :]
        ).astype(jnp.bfloat16)


def combine(slot_of, share_of, returned, stream):
    tokens, model = stream.shape
    return pl.pallas_call(
        combine_kernel,
        out_shape=jax.ShapeDtypeStruct(stream.shape, jnp.bfloat16),
        in_specs=[pl.BlockSpec(memory_space=pltpu.SMEM)] * 2
        + [pl.BlockSpec(memory_space=pltpu.VMEM)] * 2,
        out_specs=pl.BlockSpec(memory_space=pltpu.VMEM),
        scratch_shapes=[pltpu.VMEM((tokens * (model // LANES), LANES), jnp.float32)],
        compiler_params=pltpu.CompilerParams(vmem_limit_bytes=16 * 1024 * 1024),
        name="combine",
    )(slot_of, share_of, returned, stream)


def slot_tables(expert_ids, experts_all, capacity):
    flat_expert = expert_ids.reshape(-1)
    order = jnp.arange(flat_expert.shape[0], dtype=jnp.int32)
    earlier = (flat_expert[:, None] == flat_expert[None, :]) & (order[None, :] < order[:, None])
    slot_of = flat_expert * capacity + jnp.sum(earlier.astype(jnp.int32), axis=1)
    slot_ids = jnp.arange(experts_all * capacity, dtype=jnp.int32)
    placed = slot_ids[:, None] == slot_of[None, :]
    token_of = jnp.sum(jnp.where(placed, order[None, :] // 2, 0), axis=1)
    return slot_of, token_of


def shards(
    query_wide,
    key_wide,
    value_wide,
    query_narrow,
    key_narrow,
    value_narrow,
    mix_lambda,
    residual_in,
    out_wide,
    out_narrow,
    ffn_gain,
    expert_ids,
    expert_weights,
    gate_weight,
    up_weight,
    down_weight,
):
    heads, packed = attention(
        query_wide[:, 0],
        key_wide[:, 0],
        value_wide[:, 0],
        query_narrow[:, 0],
        key_narrow[:, 0],
        value_narrow[:, 0],
        mix_lambda,
    )
    tp_size = lax.axis_size(TP)
    local_rows = heads.shape[0] // tp_size
    experts_all = lax.axis_size(SP_TP)
    capacity = max(2, 4 * local_rows // experts_all)
    slot_of, token_of = slot_tables(expert_ids, experts_all, capacity)
    out_wide, out_narrow, _ = lax.optimization_barrier((out_wide, out_narrow, packed))
    whole_wide = lax.all_gather(out_wide, TP, axis=0, tiled=True)
    whole_narrow = lax.all_gather(out_narrow, TP, axis=0, tiled=True)
    mine = lax.all_to_all(
        heads.reshape(tp_size, local_rows, -1), TP, split_axis=0, concat_axis=0, tiled=True
    )
    stream, outgoing = project(
        token_of, mine, whole_wide, whole_narrow, residual_in, ffn_gain[None, :]
    )

    def exchanged(rows):
        shape = rows.shape
        moved = lax.all_to_all(
            rows.reshape(experts_all, -1, LANES), SP_TP, split_axis=0, concat_axis=0, tiled=True
        )
        return moved.reshape(shape)

    result = experts(exchanged(outgoing), gate_weight[0], up_weight[0], down_weight[0])
    return combine(slot_of, expert_weights.reshape(-1), exchanged(result), stream)


def solution(mesh):
    finer = Mesh(mesh.devices.reshape(4, 4, 4, 2), SP_TP)
    sp = ("z", "x")
    placed = (
        P(sp, TP, None),
        P(sp, TP, None),
        P(sp, TP, None),
        P(sp, TP, None),
        P(sp, TP, None),
        P(sp, TP, None),
        P(None, TP),
        P(SP_TP, None),
        P(TP, None),
        P(TP, None),
        P(),
        P(SP_TP, None),
        P(SP_TP, None),
        P(SP_TP, None, None),
        P(SP_TP, None, None),
        P(SP_TP, None, None),
    )
    return jax.shard_map(
        shards, mesh=finer, in_specs=placed, out_specs=P(SP_TP, None), check_vma=False
    )
```

```python
import jax
import jax.numpy as jnp
from jax import lax
from jax.experimental import pallas as pl
from jax.experimental.pallas import tpu as pltpu
from jax.sharding import Mesh
from jax.sharding import PartitionSpec as P

TP = ("y", "c")
SP_TP = ("z", "x", "y", "c")
RING = 4
LOG2E = 1.4426950408889634
NEG_FILL = -1e30
STAT_ROWS = 16
LANES = 128
BLOCK = 256
SOME = 48
WIDE_ORDER = (2, 1, 3)
NARROW_ORDER = (3, 1, 2)
LEAST_TOTAL = 2.0**-60
MOST_TOTAL = 2.0**100


def pack_kernel(
    q_wide, v_wide, q_narrow, k_narrow, v_narrow, v_out, kv_out, plus_out, minus_out, two_out
):
    z = lax.axis_index("z")
    chunk, width = v_wide.shape
    half = chunk // 2
    width_narrow = v_narrow.shape[1]
    behind = chunk // BLOCK * width
    for j in range(chunk // BLOCK):
        rows = slice(j * BLOCK, (j + 1) * BLOCK)
        v_out[j * width : (j + 1) * width, :] = v_wide[rows, :].T
        begin = half + j * width_narrow
        kv_out[begin : begin + width_narrow, :] = v_narrow[rows, :].T
    for side in range(2):
        lanes = slice(side * LANES, (side + 1) * LANES)
        rows = slice(side * half, (side + 1) * half)
        kv_out[:half, lanes] = k_narrow[rows, :]
        v_out[behind : behind + half, lanes] = q_narrow[rows, :]
    for out, gives_queries in (
        (plus_out, z == RING - 1),
        (minus_out, z > 0),
        (two_out, z >= RING // 2),
    ):

        @pl.when(gives_queries)
        def _(out=out):
            out[...] = q_wide[...]

        @pl.when(jnp.logical_not(gives_queries))
        def _(out=out):
            out[...] = kv_out[...]


def pack(q_wide, v_wide, q_narrow, k_narrow, v_narrow):
    chunk, width = v_wide.shape
    half = chunk // 2
    both = jax.ShapeDtypeStruct(q_wide.shape, jnp.bfloat16)
    assert half + chunk // BLOCK * v_narrow.shape[1] == chunk
    return pl.pallas_call(
        pack_kernel,
        out_shape=(
            jax.ShapeDtypeStruct((chunk // BLOCK * width + half, BLOCK), jnp.bfloat16),
            both,
            both,
            both,
            both,
        ),
        name="pack",
    )(q_wide, v_wide, q_narrow, k_narrow, v_narrow)


def attend_kernel(place, *refs, plans, slots, pieces, wide, diagonal, fill, size, width, chunk):
    chunks = len(plans)
    q_refs = refs[:chunks]
    src_refs = refs[chunks : chunks + slots * pieces]
    out_refs = refs[chunks + slots * pieces : 2 * chunks + slots * pieces]
    q_scr, kv_scr, acc, out_scr, sems, q_sems, out_sems = refs[2 * chunks + slots * pieces :]
    plans = [plan(place[0], place[1]) for plan in plans]
    scale = size ** (-0.5) * LOG2E
    key_rows = chunk if wide else chunk // 2
    halves = key_rows // LANES

    def slot_copies(slot):
        made = []
        begin = 0
        for k in range(pieces):
            rows = kv_scr.shape[1] // pieces
            source = src_refs[slot * pieces + k].at[pl.ds(0, rows), :]
            made.append(
                pltpu.make_async_copy(
                    source, kv_scr.at[slot, pl.ds(begin, rows), :], sems.at[slot, k]
                )
            )
            begin += rows
        return made

    def wait_slot(slot):
        begin = 0
        for k in range(pieces):
            rows = kv_scr.shape[1] // pieces
            source = src_refs[k].at[pl.ds(0, rows), :]
            pltpu.make_async_copy(
                source, kv_scr.at[slot, pl.ds(begin, rows), :], sems.at[slot, k]
            ).wait()
            begin += rows

    def only_map(rows, m):
        lane = lax.broadcasted_iota(jnp.int32, rows.shape, 1)
        return jnp.where((lane >= m * size) & (lane < (m + 1) * size), rows, 0)

    def dot_nt(left, right):
        return lax.dot_general(
            left, right, (((1,), (1,)), ((), ())), preferred_element_type=jnp.float32
        )

    def value_block(slot, j):
        return kv_scr[slot, pl.ds(key_rows + j * width, width), :]

    def store_result(n, m, columns, read, total, level):
        out_scr[n, pl.ds(m * width, width), columns] = (read * (1.0 / total)).astype(jnp.bfloat16)
        row = lax.broadcasted_iota(jnp.int32, (8, total.shape[1]), 0)
        packed = jnp.zeros((8, total.shape[1]), jnp.float32)
        for k in range(3):
            term = level.astype(jnp.bfloat16).astype(jnp.float32)
            packed = jnp.where(row == k, term, packed)
            level = level - term
        return packed

    def query_copy(source, n):
        rows = q_scr.shape[1]
        begin = 0 if wide else q_refs[source].shape[0] - rows
        return pltpu.make_async_copy(
            q_refs[source].at[pl.ds(begin, rows), :], q_scr.at[n], q_sems.at[n]
        )

    def within(slot, plan):
        active, count, offset = plan
        return (active > 0) & (slot >= offset) & (slot < offset + count)

    for n in range(chunks):

        @pl.when(plans[n][0] > 0)
        def _(n=n):
            query_copy(n, n).start()

    for slot in range(slots):
        used = within(slot, plans[0])
        for plan in plans[1:]:
            used = used | within(slot, plan)

        @pl.when(used)
        def _(slot=slot):
            for made in slot_copies(slot):
                made.start()

    def one_chunk(n, _):
        active, count, offset = plans[0]
        for k in range(1, chunks):
            active, count, offset = (
                jnp.where(n == k, new, old) for new, old in zip(plans[k], (active, count, offset))
            )
        pl.when(active > 0)(lambda: attend_chunk(n, count, offset))
        if fill:

            @pl.when(active == 0)
            def _():
                out_scr[n] = jnp.zeros(out_scr.shape[1:], out_scr.dtype)

        for k in range(chunks):

            @pl.when((n == k) & ((active > 0) | fill))
            def _(k=k):
                pltpu.make_async_copy(out_scr.at[k], out_refs[k], out_sems.at[k]).start()

        return 0

    def attend_chunk(n, count, offset):
        acc[...] = jnp.zeros_like(acc)
        query_copy(0, n).wait()

        def add_slot(number, totals):
            slot = 0 if diagonal else number + offset
            if chunks > 1:
                pl.when((n == 0) | jnp.logical_not(within(slot, plans[0])))(
                    lambda: wait_slot(slot)
                )
            else:
                wait_slot(slot)
            values = jnp.concatenate(
                [value_block(slot, j) for j in range(chunk // BLOCK)], axis=1
            )
            result = []
            for m in range(2):
                if wide:
                    lanes = slice(m * size, (m + 1) * size)
                    scores = dot_nt(kv_scr[slot, :key_rows, lanes], q_scr[n, :, lanes])
                else:
                    queries = only_map(
                        jnp.concatenate([q_scr[n, :, :LANES], q_scr[n, :, LANES:]], axis=0), m
                    )
                    scores = jnp.concatenate(
                        [
                            dot_nt(kv_scr[slot, :key_rows, side * LANES : (side + 1) * LANES], queries)
                            for side in range(2)
                        ],
                        axis=0,
                    )
                scores = scores * scale
                if diagonal:
                    key_pos = lax.broadcasted_iota(jnp.int32, scores.shape, 0)
                    query_pos = lax.broadcasted_iota(jnp.int32, scores.shape, 1)
                    scores = jnp.where(key_pos <= query_pos, scores, NEG_FILL)
                weights = jnp.exp2(scores)
                result.append(totals[m] + jnp.sum(weights.reshape(chunk // 8, 8, chunk), axis=0))
                acc[m] = acc[m] + jnp.dot(
                    values, weights.astype(jnp.bfloat16), preferred_element_type=jnp.float32
                )
            return tuple(result)

        none = jnp.zeros((8, chunk), jnp.float32)
        if diagonal:
            totals = add_slot(0, (none, none))
        else:
            totals = lax.fori_loop(0, count, add_slot, (none, none))
        outside = jnp.zeros((1, chunk), jnp.float32)
        stats = []
        for m in range(2):
            total = jnp.sum(totals[m], axis=0, keepdims=True)
            inside = (total >= LEAST_TOTAL) & (total <= MOST_TOTAL)
            outside = jnp.maximum(outside, jnp.where(inside, 0.0, 1.0))
            stats.append(store_result(n, m, slice(None), acc[m], total, jnp.log2(total)))
        out_scr[n, 2 * width :, :] = jnp.concatenate(stats, axis=0).astype(jnp.bfloat16)

        @pl.when(jnp.max(outside) > 0)
        def _():
            def packed_rows(take, number):
                made = []
                for k in range(2):
                    piece = number * 2 + k
                    place = pl.ds(pl.multiple_of(lax.rem(piece, halves) * LANES, LANES), LANES)
                    first, second = take(place)
                    made.append(jnp.where(piece < halves, first, second))
                return jnp.concatenate(made, axis=0)

            def keys_at(slot, number):
                return packed_rows(
                    lambda place: (kv_scr[slot, place, :LANES], kv_scr[slot, place, LANES:]), number
                )

            def queries_at(number):
                return packed_rows(
                    lambda place: (q_scr[n, place, :LANES], q_scr[n, place, LANES:]), number
                )

            def one_query_block(number, _):
                begin = pl.multiple_of(number * BLOCK, BLOCK)
                columns = pl.ds(begin, BLOCK)

                def one_map(m, packed):
                    acc[m, :, columns] = jnp.zeros((width, BLOCK), jnp.float32)

                    def careful(index, state):
                        peak, total = state
                        slot = index // (chunk // BLOCK) + offset
                        block = lax.rem(index, chunk // BLOCK)
                        place = pl.ds(pl.multiple_of(block * BLOCK, BLOCK), BLOCK)
                        if wide:
                            lanes = pl.ds(pl.multiple_of(m * size, size), size)
                            scores = dot_nt(kv_scr[slot, place, lanes], q_scr[n, columns, lanes])
                        else:
                            scores = dot_nt(keys_at(slot, block), only_map(queries_at(number), m))
                        scores = scores * scale
                        if diagonal:
                            key_pos = block * BLOCK + lax.broadcasted_iota(
                                jnp.int32, scores.shape, 0
                            )
                            query_pos = begin + lax.broadcasted_iota(jnp.int32, scores.shape, 1)
                            scores = jnp.where(key_pos <= query_pos, scores, NEG_FILL)
                        new_peak = jnp.maximum(peak, jnp.max(scores, axis=0, keepdims=True))
                        factor = jnp.exp2(peak - new_peak)
                        weights = jnp.exp2(scores - new_peak)
                        acc[m, :, columns] = factor * acc[m, :, columns] + jnp.dot(
                            value_block(slot, block),
                            weights.astype(jnp.bfloat16),
                            preferred_element_type=jnp.float32,
                        )
                        return new_peak, factor * total + jnp.sum(weights, axis=0, keepdims=True)

                    peak, total = lax.fori_loop(
                        0,
                        count * (chunk // BLOCK),
                        careful,
                        (
                            jnp.full((1, BLOCK), NEG_FILL, jnp.float32),
                            jnp.zeros((1, BLOCK), jnp.float32),
                        ),
                    )
                    rows = store_result(
                        n, m, columns, acc[m, :, columns], total, peak + jnp.log2(total)
                    )
                    both = jnp.concatenate([rows, rows], axis=0)
                    row = lax.broadcasted_iota(jnp.int32, both.shape, 0)
                    return jnp.where((row >= 8 * m) & (row < 8 * m + 8), both, packed)

                packed = lax.fori_loop(
                    0, 2, one_map, jnp.zeros((STAT_ROWS, BLOCK), jnp.float32)
                )
                out_scr[n, 2 * width :, columns] = packed.astype(jnp.bfloat16)
                return 0

            lax.fori_loop(0, chunk // BLOCK, one_query_block, 0)

    if chunks > 1:
        lax.fori_loop(0, chunks, one_chunk, 0)
    else:
        one_chunk(0, 0)
    for n in range(chunks):

        @pl.when((plans[n][0] > 0) | fill)
        def _(n=n):
            pltpu.make_async_copy(out_scr.at[n], out_refs[n], out_sems.at[n]).wait()


def attend(place, plans, queries, sources, wide, diagonal, fill, size, width, chunk):
    pieces = len(sources[0])
    flat = [array for group in sources for array in group]
    kv_rows = pieces * chunk
    chunks = len(plans)
    q_rows = chunk if wide else chunk // 2
    body = lambda *refs: attend_kernel(
        *refs,
        plans=plans,
        slots=len(sources),
        pieces=pieces,
        wide=wide,
        diagonal=diagonal,
        fill=fill,
        size=size,
        width=width,
        chunk=chunk,
    )
    area = chunk * chunk * 2 * 2 * chunks
    out = jax.ShapeDtypeStruct((2 * width + STAT_ROWS, chunk), jnp.bfloat16)
    return pl.pallas_call(
        body,
        out_shape=[out] * chunks,
        in_specs=[pl.BlockSpec(memory_space=pltpu.SMEM)]
        + [pl.BlockSpec(memory_space=pl.ANY)] * (chunks + len(flat)),
        out_specs=[pl.BlockSpec(memory_space=pl.ANY)] * chunks,
        scratch_shapes=[
            pltpu.VMEM((chunks, q_rows, BLOCK), jnp.bfloat16),
            pltpu.VMEM((len(sources), kv_rows, BLOCK), jnp.bfloat16),
            pltpu.VMEM((2, width, chunk), jnp.float32),
            pltpu.VMEM((chunks,) + out.shape, jnp.bfloat16),
            pltpu.SemaphoreType.DMA((len(sources), pieces)),
            pltpu.SemaphoreType.DMA((chunks,)),
            pltpu.SemaphoreType.DMA((chunks,)),
        ],
        cost_estimate=pl.CostEstimate(
            flops=2 * area * (size + width),
            transcendentals=area,
            bytes_accessed=len(sources) * kv_rows * 512,
        ),
    )(place, *queries, *flat)


def merge_kernel(place, lam, *refs, widths, counts):
    z, x = place[0], place[1]
    wide_valid = [z >= 0, x > 0] + [z >= d for d in WIDE_ORDER]
    narrow_valid = [z >= 0, z > 0] + [
        (z > 0) | (lax.rem(x + s, RING) < x) for s in NARROW_ORDER
    ]
    valid = (wide_valid, narrow_valid)
    out_ref = refs[-1]
    guarded = (1, None)
    begin = 0
    column = 0
    for group, (width, count) in enumerate(zip(widths, counts)):
        parts = refs[begin : begin + count]
        begin += count
        reads = []
        for m in range(2):
            levels = []
            for k, part in enumerate(parts):
                stats = part[2 * width :, :].astype(jnp.float32)
                level = stats[8 * m : 8 * m + 1] + stats[8 * m + 1 : 8 * m + 2] + stats[
                    8 * m + 2 : 8 * m + 3
                ]
                levels.append(jnp.where(valid[group][k], level, NEG_FILL))
            top = levels[0]
            for level in levels[1:]:
                top = jnp.maximum(top, level)
            shares = [jnp.exp2(level - top) for level in levels]
            whole = shares[0]
            for share in shares[1:]:
                whole = whole + share
            read = None
            for k, (share, part) in enumerate(zip(shares, parts)):
                term = part[m * width : (m + 1) * width, :].astype(jnp.float32) * (share / whole)
                if read is None:
                    read = term
                elif guarded[group] == k:
                    read = read + jnp.where(valid[group][k], term, 0.0)
                else:
                    read = read + term
            reads.append(read)
        mixed = reads[0] - lam[group, 0] * reads[1]
        normed = mixed * lax.rsqrt(jnp.mean(mixed * mixed, axis=0, keepdims=True) + 1e-06)
        out_ref[:, column : column + width] = normed.T.astype(jnp.bfloat16)
        column += width


def merge(place, lam, groups, widths):
    chunk = groups[0][0].shape[1]
    block = chunk // 2
    counts = [len(parts) for parts in groups]
    flat = [part for parts in groups for part in parts]
    body = lambda *refs: merge_kernel(*refs, widths=widths, counts=counts)
    return pl.pallas_call(
        body,
        grid=(chunk // block,),
        out_shape=jax.ShapeDtypeStruct((chunk, sum(widths)), jnp.bfloat16),
        in_specs=[pl.BlockSpec(memory_space=pltpu.SMEM)] * 2
        + [pl.BlockSpec((part.shape[0], block), lambda i: (0, i)) for part in flat],
        out_specs=pl.BlockSpec((block, sum(widths)), lambda i: (i, 0)),
        name="merge_reads",
    )(place, lam, *flat)


def around(array, axis, by):
    return lax.ppermute(array, axis, [(k, (k + by) % RING) for k in range(RING)])


def onward(array, axis, by):
    return lax.ppermute(
        array, axis, [(k, k + by) for k in range(RING) if 0 <= k + by < RING]
    )


def after(array, *others):
    return lax.optimization_barrier((array,) + others)[0]


def attention(
    query_wide, key_wide, value_wide, query_narrow, key_narrow, value_narrow, mix_lambda
):
    z = lax.axis_index("z")
    x = lax.axis_index("x")
    place = jnp.stack([z, x]).astype(jnp.int32)
    chunk = query_wide.shape[0]
    size_wide = query_wide.shape[1] // 2
    size_narrow = query_narrow.shape[1] // 2
    width_wide, width_narrow = value_wide.shape[1], value_narrow.shape[1]

    xk_near = around(key_wide, "x", 1)
    xk_back = around(key_wide, "x", -1)
    values, kv_narrow, plus, minus, two = pack(
        query_wide, value_wide, query_narrow, key_narrow, value_narrow
    )
    xv_back = around(values, "x", -1)
    xv_near = around(values, "x", 1)
    z_two = around(two, "z", 2)
    z_plus = around(plus, "z", 1)
    z_minus = around(minus, "z", -1)
    xv_far = around(xv_back[:chunk], "x", -1)
    xk_far = around(xk_near, "x", 1)
    xq_far = around(xv_near[chunk:], "x", 1)

    wide_sources = [(key_wide, values), (xk_near, xv_near), (xk_far, xv_far), (xk_back, xv_back)]
    narrow_sources = [(kv_narrow,), (z_plus,), (z_two,), (z_minus,)]
    q_later = {1: z_minus, 2: z_two, 3: z_plus}
    q_side = {1: xv_near, 2: xq_far, 3: xv_back}

    def wide_plan(d):
        return lambda z, x: ((z + d < RING).astype(jnp.int32), jnp.int32(RING), jnp.int32(0))

    def narrow_plan(s):
        def plan(z, x):
            level = (lax.rem(x - s + RING, RING) > x).astype(jnp.int32)
            return ((z > 0) | (level > 0)).astype(jnp.int32), z + level, 1 - level

        return plan

    def diag_plan(z, x):
        return jnp.int32(1), jnp.int32(1), jnp.int32(0)

    def wide_rest_plan(z, x):
        return (x > 0).astype(jnp.int32), x, jnp.int32(1)

    def narrow_rest_plan(z, x):
        return (z > 0).astype(jnp.int32), z, jnp.int32(1)

    def wide(last, plans, queries, sources, diagonal):
        given = after(place, last) if last is not None else place
        return attend(
            given, plans, queries, sources, True, diagonal, False, size_wide, width_wide, chunk
        )

    def narrow(last, plans, queries, sources, diagonal):
        return attend(
            after(place, last), plans, queries, sources, False, diagonal, not diagonal, size_narrow,
            width_narrow, chunk,
        )

    diag_wide = wide(None, (diag_plan,), [query_wide], wide_sources[:1], True)[0]
    diag_narrow = narrow(diag_wide, (diag_plan,), [values], narrow_sources[:1], True)[0]
    side, sent = {}, {}
    side[3] = narrow(diag_narrow, (narrow_plan(3),), [q_side[3]], narrow_sources, False)[0]
    sent[2] = wide(side[3], (wide_plan(2),), [q_later[2]], wide_sources, False)[0]
    first_sent = sent[2]
    sent[2] = onward(sent[2], "z", 2)
    sent[1], sent[3] = wide(
        first_sent, (wide_plan(1), wide_plan(3)), [q_later[1], q_later[3]], wide_sources, False,
    )
    side[1], side[2] = narrow(
        sent[1], (narrow_plan(1), narrow_plan(2)), [q_side[1], q_side[2]], narrow_sources, False,
    )
    for d in (1, 3):
        sent[d] = onward(sent[d], "z", d)
    rest_narrow = narrow(side[1], (narrow_rest_plan,), [values], narrow_sources, False)[0]
    rest_wide = wide(rest_narrow, (wide_rest_plan,), [query_wide], wide_sources, False)[0]
    side = {s: around(side[s], "x", -s) for s in NARROW_ORDER}
    made = merge(
        place,
        mix_lambda,
        (
            [diag_wide, rest_wide] + [sent[d] for d in WIDE_ORDER],
            [diag_narrow, rest_narrow] + [side[s] for s in NARROW_ORDER],
        ),
        (width_wide, width_narrow),
    )
    return made, values


def project_kernel(
    token_of, mine, weight_wide, weight_narrow, residual, gain, stream_out, rows_out,
    weights, left, total, flat_scr, rows, sems,
):
    heads, tokens, _ = mine.shape
    depth, model = weight_wide.shape
    wide = depth // heads
    tiles = model // LANES
    part = weights.shape[1]
    parts = weights.shape[0]
    for k in range(parts):
        if k * part < depth:
            source = weight_wide.at[pl.ds(k * part, part), :]
        else:
            source = weight_narrow.at[pl.ds(k * part - depth, part), :]
        pltpu.make_async_copy(source, weights.at[k], sems.at[k]).start()
    joined = jnp.concatenate(
        [mine[h, :, :wide] for h in range(heads)] + [mine[h, :, wide:] for h in range(heads)], axis=1
    )
    for k in range(parts):
        left[k] = joined[:, k * part : (k + 1) * part]
    total[...] = residual[...].astype(jnp.float32)

    def add_part(k, _):
        pltpu.make_async_copy(
            weight_wide.at[pl.ds(0, part), :], weights.at[k], sems.at[k]
        ).wait()
        total[...] = total[...] + jnp.dot(
            left[k], weights[k], preferred_element_type=jnp.float32
        )
        return 0

    lax.fori_loop(0, parts, add_part, 0)
    rounded = total[...].astype(jnp.bfloat16)
    stream_out[...] = rounded
    stream = rounded.astype(jnp.float32)
    inverse = lax.rsqrt(jnp.mean(stream * stream, axis=1, keepdims=True) + 1e-06)
    for j in range(tiles):
        lanes = slice(j * LANES, (j + 1) * LANES)
        flat_scr[pl.ds(j, tokens, stride=tiles), :] = stream[:, lanes] * inverse * gain[:, lanes]
    rows[...] = flat_scr[...].reshape(tokens, tiles, LANES).astype(jnp.bfloat16)

    def copy_row(slot, _):
        rows_out[slot] = rows[token_of[slot]]
        return 0

    lax.fori_loop(0, rows_out.shape[0], copy_row, 0, unroll=16)


def project(token_of, mine, weight_wide, weight_narrow, residual, gain):
    heads, tokens, depth = mine.shape
    model = weight_wide.shape[1]
    slots = token_of.shape[0]
    tiles = model // LANES
    part = 2 * BLOCK
    parts = heads * depth // part
    return pl.pallas_call(
        project_kernel,
        out_shape=(
            jax.ShapeDtypeStruct((tokens, model), jnp.bfloat16),
            jax.ShapeDtypeStruct((slots, tiles, LANES), jnp.bfloat16),
        ),
        in_specs=[
            pl.BlockSpec(memory_space=pltpu.SMEM),
            pl.BlockSpec(memory_space=pltpu.VMEM),
            pl.BlockSpec(memory_space=pltpu.HBM),
            pl.BlockSpec(memory_space=pltpu.HBM),
            pl.BlockSpec(memory_space=pltpu.VMEM),
            pl.BlockSpec(memory_space=pltpu.VMEM),
        ],
        out_specs=(pl.BlockSpec(memory_space=pltpu.VMEM),) * 2,
        scratch_shapes=[
            pltpu.VMEM((parts, part, model), jnp.bfloat16),
            pltpu.VMEM((parts, tokens, part), jnp.bfloat16),
            pltpu.VMEM((tokens, model), jnp.float32),
            pltpu.VMEM((tokens * tiles, LANES), jnp.float32),
            pltpu.VMEM((tokens, tiles, LANES), jnp.bfloat16),
            pltpu.SemaphoreType.DMA((parts,)),
        ],
        compiler_params=pltpu.CompilerParams(vmem_limit_bytes=48 * 1024 * 1024),
        name="project",
    )(token_of, mine, weight_wide, weight_narrow, residual, gain)


def expert_kernel(arrived, gate, up, down, out, flat, rows, hidden):
    count, tiles, _ = arrived.shape

    def spread(k, _):
        some = arrived[pl.ds(k * SOME, SOME)].astype(jnp.float32)
        flat[pl.ds(pl.multiple_of(k * SOME * tiles, LANES), SOME * tiles), :] = some.reshape(
            SOME * tiles, LANES
        )
        return 0

    def gathered(k, _):
        some = flat[pl.ds(pl.multiple_of(k * SOME * tiles, LANES), SOME * tiles), :]
        out[pl.ds(k * SOME, SOME)] = some.reshape(SOME, tiles, LANES).astype(jnp.bfloat16)
        return 0

    lax.fori_loop(0, count // SOME, spread, 0)
    for j in range(tiles):
        rows[:, j * LANES : (j + 1) * LANES] = flat[pl.ds(j, count, stride=tiles), :].astype(
            jnp.bfloat16
        )

    gate_part = jnp.dot(rows[...], gate[...], preferred_element_type=jnp.float32)
    up_part = jnp.dot(rows[...], up[...], preferred_element_type=jnp.float32)
    hidden[...] = (gate_part * jax.nn.sigmoid(gate_part) * up_part).astype(jnp.bfloat16)
    result = jnp.dot(hidden[...], down[...], preferred_element_type=jnp.float32)
    for j in range(tiles):
        flat[pl.ds(j, count, stride=tiles), :] = result[:, j * LANES : (j + 1) * LANES]
    lax.fori_loop(0, count // SOME, gathered, 0)


def experts(arrived, gate, up, down):
    count, tiles, _ = arrived.shape
    model, inner = gate.shape
    return pl.pallas_call(
        expert_kernel,
        out_shape=jax.ShapeDtypeStruct(arrived.shape, jnp.bfloat16),
        in_specs=[pl.BlockSpec(memory_space=pltpu.VMEM)] * 4,
        out_specs=pl.BlockSpec(memory_space=pltpu.VMEM),
        scratch_shapes=[
            pltpu.VMEM((count * tiles, LANES), jnp.float32),
            pltpu.VMEM((count, model), jnp.bfloat16),
            pltpu.VMEM((count, inner), jnp.bfloat16),
        ],
        compiler_params=pltpu.CompilerParams(vmem_limit_bytes=28*1024*1024),
        name="experts",
    )(arrived, gate, up, down)


def combine_kernel(slot_of, share_of, returned, stream, out, flat):
    tokens, model = stream.shape
    tiles = model // LANES

    def one_token(token, _):
        total = share_of[2 * token] * returned[slot_of[2 * token]].astype(jnp.float32)
        total = total + share_of[2 * token + 1] * returned[slot_of[2 * token + 1]].astype(
            jnp.float32
        )
        flat[pl.ds(pl.multiple_of(token * tiles, tiles), tiles), :] = total
        return 0

    lax.fori_loop(0, tokens, one_token, 0, unroll=8)
    for j in range(tiles):
        lanes = slice(j * LANES, (j + 1) * LANES)
        out[:, lanes] = (
            stream[:, lanes].astype(jnp.float32) + flat[pl.ds(j, tokens, stride=tiles), :]
        ).astype(jnp.bfloat16)


def combine(slot_of, share_of, returned, stream):
    tokens, model = stream.shape
    return pl.pallas_call(
        combine_kernel,
        out_shape=jax.ShapeDtypeStruct(stream.shape, jnp.bfloat16),
        in_specs=[pl.BlockSpec(memory_space=pltpu.SMEM)] * 2
        + [pl.BlockSpec(memory_space=pltpu.VMEM)] * 2,
        out_specs=pl.BlockSpec(memory_space=pltpu.VMEM),
        scratch_shapes=[pltpu.VMEM((tokens * (model // LANES), LANES), jnp.float32)],
        compiler_params=pltpu.CompilerParams(vmem_limit_bytes=16 * 1024 * 1024),
        name="combine",
    )(slot_of, share_of, returned, stream)


def slot_tables(expert_ids, experts_all, capacity):
    flat_expert = expert_ids.reshape(-1)
    order = jnp.arange(flat_expert.shape[0], dtype=jnp.int32)
    earlier = (flat_expert[:, None] == flat_expert[None, :]) & (order[None, :] < order[:, None])
    slot_of = flat_expert * capacity + jnp.sum(earlier.astype(jnp.int32), axis=1)
    slot_ids = jnp.arange(experts_all * capacity, dtype=jnp.int32)
    placed = slot_ids[:, None] == slot_of[None, :]
    token_of = jnp.sum(jnp.where(placed, order[None, :] // 2, 0), axis=1)
    return slot_of, token_of


def shards(
    query_wide,
    key_wide,
    value_wide,
    query_narrow,
    key_narrow,
    value_narrow,
    mix_lambda,
    residual_in,
    out_wide,
    out_narrow,
    ffn_gain,
    expert_ids,
    expert_weights,
    gate_weight,
    up_weight,
    down_weight,
):
    heads, packed = attention(
        query_wide[:, 0],
        key_wide[:, 0],
        value_wide[:, 0],
        query_narrow[:, 0],
        key_narrow[:, 0],
        value_narrow[:, 0],
        mix_lambda,
    )
    tp_size = lax.axis_size(TP)
    local_rows = heads.shape[0] // tp_size
    experts_all = lax.axis_size(SP_TP)
    capacity = max(2, 4 * local_rows // experts_all)
    slot_of, token_of = slot_tables(expert_ids, experts_all, capacity)
    out_wide, out_narrow, _ = lax.optimization_barrier((out_wide, out_narrow, packed))
    whole_wide = lax.all_gather(out_wide, TP, axis=0, tiled=True)
    whole_narrow = lax.all_gather(out_narrow, TP, axis=0, tiled=True)
    mine = lax.all_to_all(
        heads.reshape(tp_size, local_rows, -1), TP, split_axis=0, concat_axis=0, tiled=True
    )
    stream, outgoing = project(
        token_of, mine, whole_wide, whole_narrow, residual_in, ffn_gain[None, :]
    )

    def exchanged(rows):
        shape = rows.shape
        moved = lax.all_to_all(
            rows.reshape(experts_all, -1, LANES), SP_TP, split_axis=0, concat_axis=0, tiled=True
        )
        return moved.reshape(shape)

    result = experts(exchanged(outgoing), gate_weight[0], up_weight[0], down_weight[0])
    return combine(slot_of, expert_weights.reshape(-1), exchanged(result), stream)


def solution(mesh):
    finer = Mesh(mesh.devices.reshape(4, 4, 4, 2), SP_TP)
    sp = ("z", "x")
    placed = (
        P(sp, TP, None),
        P(sp, TP, None),
        P(sp, TP, None),
        P(sp, TP, None),
        P(sp, TP, None),
        P(sp, TP, None),
        P(None, TP),
        P(SP_TP, None),
        P(TP, None),
        P(TP, None),
        P(),
        P(SP_TP, None),
        P(SP_TP, None),
        P(SP_TP, None, None),
        P(SP_TP, None, None),
        P(SP_TP, None, None),
    )
    return jax.shard_map(
        shards, mesh=finer, in_specs=placed, out_specs=P(SP_TP, None), check_vma=False
    )
```

```python
import jax
import jax.numpy as jnp
from jax import lax
from jax.experimental import pallas as pl
from jax.experimental.pallas import tpu as pltpu
from jax.sharding import Mesh
from jax.sharding import PartitionSpec as P

TP = ("y", "c")
SP_TP = ("z", "x", "y", "c")
RING = 4
LOG2E = 1.4426950408889634
NEG_FILL = -1e30
STAT_ROWS = 16
LANES = 128
BLOCK = 256
SOME = 48
WIDE_ORDER = (2, 1, 3)
NARROW_ORDER = (3, 1, 2)
LEAST_TOTAL = 2.0**-60
MOST_TOTAL = 2.0**100


def pack_kernel(
    q_wide, v_wide, q_narrow, k_narrow, v_narrow, v_out, kv_out, plus_out, minus_out, two_out
):
    z = lax.axis_index("z")
    chunk, width = v_wide.shape
    half = chunk // 2
    width_narrow = v_narrow.shape[1]
    behind = chunk // BLOCK * width
    for j in range(chunk // BLOCK):
        rows = slice(j * BLOCK, (j + 1) * BLOCK)
        v_out[j * width : (j + 1) * width, :] = v_wide[rows, :].T
        begin = half + j * width_narrow
        kv_out[begin : begin + width_narrow, :] = v_narrow[rows, :].T
    for side in range(2):
        lanes = slice(side * LANES, (side + 1) * LANES)
        rows = slice(side * half, (side + 1) * half)
        kv_out[:half, lanes] = k_narrow[rows, :]
        v_out[behind : behind + half, lanes] = q_narrow[rows, :]
    for out, gives_queries in (
        (plus_out, z == RING - 1),
        (minus_out, z > 0),
        (two_out, z >= RING // 2),
    ):

        @pl.when(gives_queries)
        def _(out=out):
            out[...] = q_wide[...]

        @pl.when(jnp.logical_not(gives_queries))
        def _(out=out):
            out[...] = kv_out[...]


def pack(q_wide, v_wide, q_narrow, k_narrow, v_narrow):
    chunk, width = v_wide.shape
    half = chunk // 2
    both = jax.ShapeDtypeStruct(q_wide.shape, jnp.bfloat16)
    assert half + chunk // BLOCK * v_narrow.shape[1] == chunk
    return pl.pallas_call(
        pack_kernel,
        out_shape=(
            jax.ShapeDtypeStruct((chunk // BLOCK * width + half, BLOCK), jnp.bfloat16),
            both,
            both,
            both,
            both,
        ),
        name="pack",
    )(q_wide, v_wide, q_narrow, k_narrow, v_narrow)


def attend_kernel(place, *refs, plans, slots, pieces, wide, diagonal, fill, size, width, chunk):
    chunks = len(plans)
    q_refs = refs[:chunks]
    src_refs = refs[chunks : chunks + slots * pieces]
    out_refs = refs[chunks + slots * pieces : 2 * chunks + slots * pieces]
    q_scr, kv_scr, acc, out_scr, sems, q_sems, out_sems = refs[2 * chunks + slots * pieces :]
    plans = [plan(place[0], place[1]) for plan in plans]
    scale = size ** (-0.5) * LOG2E
    key_rows = chunk if wide else chunk // 2
    halves = key_rows // LANES

    def slot_copies(slot):
        made = []
        begin = 0
        for k in range(pieces):
            rows = kv_scr.shape[1] // pieces
            source = src_refs[slot * pieces + k].at[pl.ds(0, rows), :]
            made.append(
                pltpu.make_async_copy(
                    source, kv_scr.at[slot, pl.ds(begin, rows), :], sems.at[slot, k]
                )
            )
            begin += rows
        return made

    def wait_slot(slot):
        begin = 0
        for k in range(pieces):
            rows = kv_scr.shape[1] // pieces
            source = src_refs[k].at[pl.ds(0, rows), :]
            pltpu.make_async_copy(
                source, kv_scr.at[slot, pl.ds(begin, rows), :], sems.at[slot, k]
            ).wait()
            begin += rows

    def only_map(rows, m):
        lane = lax.broadcasted_iota(jnp.int32, rows.shape, 1)
        return jnp.where((lane >= m * size) & (lane < (m + 1) * size), rows, 0)

    def dot_nt(left, right):
        return lax.dot_general(
            left, right, (((1,), (1,)), ((), ())), preferred_element_type=jnp.float32
        )

    def value_block(slot, j):
        return kv_scr[slot, pl.ds(key_rows + j * width, width), :]

    def store_result(n, m, columns, read, total, level):
        out_scr[n, pl.ds(m * width, width), columns] = (read * (1.0 / total)).astype(jnp.bfloat16)
        row = lax.broadcasted_iota(jnp.int32, (8, total.shape[1]), 0)
        packed = jnp.zeros((8, total.shape[1]), jnp.float32)
        for k in range(3):
            term = level.astype(jnp.bfloat16).astype(jnp.float32)
            packed = jnp.where(row == k, term, packed)
            level = level - term
        return packed

    def query_copy(source, n):
        rows = q_scr.shape[1]
        begin = 0 if wide else q_refs[source].shape[0] - rows
        return pltpu.make_async_copy(
            q_refs[source].at[pl.ds(begin, rows), :], q_scr.at[n], q_sems.at[n]
        )

    def within(slot, plan):
        active, count, offset = plan
        return (active > 0) & (slot >= offset) & (slot < offset + count)

    for n in range(chunks):

        @pl.when(plans[n][0] > 0)
        def _(n=n):
            query_copy(n, n).start()

    for slot in range(slots):
        used = within(slot, plans[0])
        for plan in plans[1:]:
            used = used | within(slot, plan)

        @pl.when(used)
        def _(slot=slot):
            for made in slot_copies(slot):
                made.start()

    def one_chunk(n, _):
        active, count, offset = plans[0]
        for k in range(1, chunks):
            active, count, offset = (
                jnp.where(n == k, new, old) for new, old in zip(plans[k], (active, count, offset))
            )
        pl.when(active > 0)(lambda: attend_chunk(n, count, offset))
        if fill:

            @pl.when(active == 0)
            def _():
                out_scr[n] = jnp.zeros(out_scr.shape[1:], out_scr.dtype)

        for k in range(chunks):

            @pl.when((n == k) & ((active > 0) | fill))
            def _(k=k):
                pltpu.make_async_copy(out_scr.at[k], out_refs[k], out_sems.at[k]).start()

        return 0

    def attend_chunk(n, count, offset):
        acc[...] = jnp.zeros_like(acc)
        query_copy(0, n).wait()

        def add_slot(number, totals):
            slot = 0 if diagonal else number + offset
            if chunks > 1:
                pl.when((n == 0) | jnp.logical_not(within(slot, plans[0])))(
                    lambda: wait_slot(slot)
                )
            else:
                wait_slot(slot)
            values = jnp.concatenate(
                [value_block(slot, j) for j in range(chunk // BLOCK)], axis=1
            )
            result = []
            for m in range(2):
                if wide:
                    lanes = slice(m * size, (m + 1) * size)
                    scores = dot_nt(kv_scr[slot, :key_rows, lanes], q_scr[n, :, lanes])
                else:
                    queries = only_map(
                        jnp.concatenate([q_scr[n, :, :LANES], q_scr[n, :, LANES:]], axis=0), m
                    )
                    scores = jnp.concatenate(
                        [
                            dot_nt(kv_scr[slot, :key_rows, side * LANES : (side + 1) * LANES], queries)
                            for side in range(2)
                        ],
                        axis=0,
                    )
                scores = scores * scale
                if diagonal:
                    key_pos = lax.broadcasted_iota(jnp.int32, scores.shape, 0)
                    query_pos = lax.broadcasted_iota(jnp.int32, scores.shape, 1)
                    scores = jnp.where(key_pos <= query_pos, scores, NEG_FILL)
                weights = jnp.exp2(scores)
                result.append(totals[m] + jnp.sum(weights.reshape(chunk // 8, 8, chunk), axis=0))
                acc[m] = acc[m] + jnp.dot(
                    values, weights.astype(jnp.bfloat16), preferred_element_type=jnp.float32
                )
            return tuple(result)

        none = jnp.zeros((8, chunk), jnp.float32)
        if diagonal:
            totals = add_slot(0, (none, none))
        else:
            totals = lax.fori_loop(0, count, add_slot, (none, none))
        outside = jnp.zeros((1, chunk), jnp.float32)
        stats = []
        for m in range(2):
            total = jnp.sum(totals[m], axis=0, keepdims=True)
            inside = (total >= LEAST_TOTAL) & (total <= MOST_TOTAL)
            outside = jnp.maximum(outside, jnp.where(inside, 0.0, 1.0))
            stats.append(store_result(n, m, slice(None), acc[m], total, jnp.log2(total)))
        out_scr[n, 2 * width :, :] = jnp.concatenate(stats, axis=0).astype(jnp.bfloat16)

        @pl.when(jnp.max(outside) > 0)
        def _():
            def packed_rows(take, number):
                made = []
                for k in range(2):
                    piece = number * 2 + k
                    place = pl.ds(pl.multiple_of(lax.rem(piece, halves) * LANES, LANES), LANES)
                    first, second = take(place)
                    made.append(jnp.where(piece < halves, first, second))
                return jnp.concatenate(made, axis=0)

            def keys_at(slot, number):
                return packed_rows(
                    lambda place: (kv_scr[slot, place, :LANES], kv_scr[slot, place, LANES:]), number
                )

            def queries_at(number):
                return packed_rows(
                    lambda place: (q_scr[n, place, :LANES], q_scr[n, place, LANES:]), number
                )

            def one_query_block(number, _):
                begin = pl.multiple_of(number * BLOCK, BLOCK)
                columns = pl.ds(begin, BLOCK)

                def one_map(m, packed):
                    acc[m, :, columns] = jnp.zeros((width, BLOCK), jnp.float32)

                    def careful(index, state):
                        peak, total = state
                        slot = index // (chunk // BLOCK) + offset
                        block = lax.rem(index, chunk // BLOCK)
                        place = pl.ds(pl.multiple_of(block * BLOCK, BLOCK), BLOCK)
                        if wide:
                            lanes = pl.ds(pl.multiple_of(m * size, size), size)
                            scores = dot_nt(kv_scr[slot, place, lanes], q_scr[n, columns, lanes])
                        else:
                            scores = dot_nt(keys_at(slot, block), only_map(queries_at(number), m))
                        scores = scores * scale
                        if diagonal:
                            key_pos = block * BLOCK + lax.broadcasted_iota(
                                jnp.int32, scores.shape, 0
                            )
                            query_pos = begin + lax.broadcasted_iota(jnp.int32, scores.shape, 1)
                            scores = jnp.where(key_pos <= query_pos, scores, NEG_FILL)
                        new_peak = jnp.maximum(peak, jnp.max(scores, axis=0, keepdims=True))
                        factor = jnp.exp2(peak - new_peak)
                        weights = jnp.exp2(scores - new_peak)
                        acc[m, :, columns] = factor * acc[m, :, columns] + jnp.dot(
                            value_block(slot, block),
                            weights.astype(jnp.bfloat16),
                            preferred_element_type=jnp.float32,
                        )
                        return new_peak, factor * total + jnp.sum(weights, axis=0, keepdims=True)

                    peak, total = lax.fori_loop(
                        0,
                        count * (chunk // BLOCK),
                        careful,
                        (
                            jnp.full((1, BLOCK), NEG_FILL, jnp.float32),
                            jnp.zeros((1, BLOCK), jnp.float32),
                        ),
                    )
                    rows = store_result(
                        n, m, columns, acc[m, :, columns], total, peak + jnp.log2(total)
                    )
                    both = jnp.concatenate([rows, rows], axis=0)
                    row = lax.broadcasted_iota(jnp.int32, both.shape, 0)
                    return jnp.where((row >= 8 * m) & (row < 8 * m + 8), both, packed)

                packed = lax.fori_loop(
                    0, 2, one_map, jnp.zeros((STAT_ROWS, BLOCK), jnp.float32)
                )
                out_scr[n, 2 * width :, columns] = packed.astype(jnp.bfloat16)
                return 0

            lax.fori_loop(0, chunk // BLOCK, one_query_block, 0)

    if chunks > 1:
        lax.fori_loop(0, chunks, one_chunk, 0)
    else:
        one_chunk(0, 0)
    for n in range(chunks):

        @pl.when((plans[n][0] > 0) | fill)
        def _(n=n):
            pltpu.make_async_copy(out_scr.at[n], out_refs[n], out_sems.at[n]).wait()


def attend(place, plans, queries, sources, wide, diagonal, fill, size, width, chunk):
    pieces = len(sources[0])
    flat = [array for group in sources for array in group]
    kv_rows = pieces * chunk
    chunks = len(plans)
    q_rows = chunk if wide else chunk // 2
    body = lambda *refs: attend_kernel(
        *refs,
        plans=plans,
        slots=len(sources),
        pieces=pieces,
        wide=wide,
        diagonal=diagonal,
        fill=fill,
        size=size,
        width=width,
        chunk=chunk,
    )
    area = chunk * chunk * 2 * 2 * chunks
    out = jax.ShapeDtypeStruct((2 * width + STAT_ROWS, chunk), jnp.bfloat16)
    return pl.pallas_call(
        body,
        out_shape=[out] * chunks,
        in_specs=[pl.BlockSpec(memory_space=pltpu.SMEM)]
        + [pl.BlockSpec(memory_space=pl.ANY)] * (chunks + len(flat)),
        out_specs=[pl.BlockSpec(memory_space=pl.ANY)] * chunks,
        scratch_shapes=[
            pltpu.VMEM((chunks, q_rows, BLOCK), jnp.bfloat16),
            pltpu.VMEM((len(sources), kv_rows, BLOCK), jnp.bfloat16),
            pltpu.VMEM((2, width, chunk), jnp.float32),
            pltpu.VMEM((chunks,) + out.shape, jnp.bfloat16),
            pltpu.SemaphoreType.DMA((len(sources), pieces)),
            pltpu.SemaphoreType.DMA((chunks,)),
            pltpu.SemaphoreType.DMA((chunks,)),
        ],
        cost_estimate=pl.CostEstimate(
            flops=2 * area * (size + width),
            transcendentals=area,
            bytes_accessed=len(sources) * kv_rows * 512,
        ),
    )(place, *queries, *flat)


def merge_kernel(place, lam, *refs, widths, counts):
    z, x = place[0], place[1]
    wide_valid = [z >= 0, x > 0] + [z >= d for d in WIDE_ORDER]
    narrow_valid = [z >= 0, z > 0] + [
        (z > 0) | (lax.rem(x + s, RING) < x) for s in NARROW_ORDER
    ]
    valid = (wide_valid, narrow_valid)
    out_ref = refs[-1]
    lax.fori_loop(
        0,
        out_ref.shape[0] // BLOCK,
        lambda k, _: merge_block(
            pl.ds(pl.multiple_of(k * BLOCK, BLOCK), BLOCK), valid, lam, refs, widths, counts
        ),
        0,
    )


def merge_block(block, valid, lam, refs, widths, counts):
    out_ref = refs[-1]
    guarded = (1, None)
    begin = 0
    column = 0
    for group, (width, count) in enumerate(zip(widths, counts)):
        parts = refs[begin : begin + count]
        begin += count
        reads = []
        for m in range(2):
            levels = []
            for k, part in enumerate(parts):
                stats = part[2 * width :, block].astype(jnp.float32)
                level = stats[8 * m : 8 * m + 1] + stats[8 * m + 1 : 8 * m + 2] + stats[
                    8 * m + 2 : 8 * m + 3
                ]
                levels.append(jnp.where(valid[group][k], level, NEG_FILL))
            top = levels[0]
            for level in levels[1:]:
                top = jnp.maximum(top, level)
            shares = [jnp.exp2(level - top) for level in levels]
            whole = shares[0]
            for share in shares[1:]:
                whole = whole + share
            read = None
            for k, (share, part) in enumerate(zip(shares, parts)):
                term = part[m * width : (m + 1) * width, block].astype(jnp.float32) * (share / whole)
                if read is None:
                    read = term
                elif guarded[group] == k:
                    read = read + jnp.where(valid[group][k], term, 0.0)
                else:
                    read = read + term
            reads.append(read)
        mixed = reads[0] - lam[group, 0] * reads[1]
        normed = mixed * lax.rsqrt(jnp.mean(mixed * mixed, axis=0, keepdims=True) + 1e-06)
        out_ref[block, column : column + width] = normed.T.astype(jnp.bfloat16)
        column += width
    return 0


def merge(place, lam, groups, widths):
    chunk = groups[0][0].shape[1]
    counts = [len(parts) for parts in groups]
    flat = [part for parts in groups for part in parts]
    body = lambda *refs: merge_kernel(*refs, widths=widths, counts=counts)
    return pl.pallas_call(
        body,
        out_shape=jax.ShapeDtypeStruct((chunk, sum(widths)), jnp.bfloat16),
        in_specs=[pl.BlockSpec(memory_space=pltpu.SMEM)] * 2
        + [pl.BlockSpec(memory_space=pltpu.VMEM)] * len(flat),
        out_specs=pl.BlockSpec(memory_space=pltpu.VMEM),
        compiler_params=pltpu.CompilerParams(vmem_limit_bytes=16 * 1024 * 1024),
        name="merge_reads",
    )(place, lam, *flat)


def around(array, axis, by):
    return lax.ppermute(array, axis, [(k, (k + by) % RING) for k in range(RING)])


def onward(array, axis, by):
    return lax.ppermute(
        array, axis, [(k, k + by) for k in range(RING) if 0 <= k + by < RING]
    )


def after(array, *others):
    return lax.optimization_barrier((array,) + others)[0]


def attention(
    query_wide, key_wide, value_wide, query_narrow, key_narrow, value_narrow, mix_lambda
):
    z = lax.axis_index("z")
    x = lax.axis_index("x")
    place = jnp.stack([z, x]).astype(jnp.int32)
    chunk = query_wide.shape[0]
    size_wide = query_wide.shape[1] // 2
    size_narrow = query_narrow.shape[1] // 2
    width_wide, width_narrow = value_wide.shape[1], value_narrow.shape[1]

    xk_near = around(key_wide, "x", 1)
    xk_back = around(key_wide, "x", -1)
    values, kv_narrow, plus, minus, two = pack(
        query_wide, value_wide, query_narrow, key_narrow, value_narrow
    )
    xv_back = around(values, "x", -1)
    xv_near = around(values, "x", 1)
    z_two = around(two, "z", 2)
    z_plus = around(plus, "z", 1)
    z_minus = around(minus, "z", -1)
    xv_far = around(xv_back[:chunk], "x", -1)
    xk_far = around(xk_near, "x", 1)
    xq_far = around(xv_near[chunk:], "x", 1)

    wide_sources = [(key_wide, values), (xk_near, xv_near), (xk_far, xv_far), (xk_back, xv_back)]
    narrow_sources = [(kv_narrow,), (z_plus,), (z_two,), (z_minus,)]
    q_later = {1: z_minus, 2: z_two, 3: z_plus}
    q_side = {1: xv_near, 2: xq_far, 3: xv_back}

    def wide_plan(d):
        return lambda z, x: ((z + d < RING).astype(jnp.int32), jnp.int32(RING), jnp.int32(0))

    def narrow_plan(s):
        def plan(z, x):
            level = (lax.rem(x - s + RING, RING) > x).astype(jnp.int32)
            return ((z > 0) | (level > 0)).astype(jnp.int32), z + level, 1 - level

        return plan

    def diag_plan(z, x):
        return jnp.int32(1), jnp.int32(1), jnp.int32(0)

    def wide_rest_plan(z, x):
        return (x > 0).astype(jnp.int32), x, jnp.int32(1)

    def narrow_rest_plan(z, x):
        return (z > 0).astype(jnp.int32), z, jnp.int32(1)

    def wide(last, plans, queries, sources, diagonal):
        given = after(place, last) if last is not None else place
        return attend(
            given, plans, queries, sources, True, diagonal, False, size_wide, width_wide, chunk
        )

    def narrow(last, plans, queries, sources, diagonal):
        return attend(
            after(place, last), plans, queries, sources, False, diagonal, not diagonal, size_narrow,
            width_narrow, chunk,
        )

    diag_wide = wide(None, (diag_plan,), [query_wide], wide_sources[:1], True)[0]
    diag_narrow = narrow(diag_wide, (diag_plan,), [values], narrow_sources[:1], True)[0]
    side, sent = {}, {}
    side[3] = narrow(diag_narrow, (narrow_plan(3),), [q_side[3]], narrow_sources, False)[0]
    sent[2] = wide(side[3], (wide_plan(2),), [q_later[2]], wide_sources, False)[0]
    first_sent = sent[2]
    sent[2] = onward(sent[2], "z", 2)
    sent[1], sent[3] = wide(
        first_sent, (wide_plan(1), wide_plan(3)), [q_later[1], q_later[3]], wide_sources, False,
    )
    side[1], side[2] = narrow(
        sent[1], (narrow_plan(1), narrow_plan(2)), [q_side[1], q_side[2]], narrow_sources, False,
    )
    for d in (1, 3):
        sent[d] = onward(sent[d], "z", d)
    rest_narrow = narrow(side[1], (narrow_rest_plan,), [values], narrow_sources, False)[0]
    rest_wide = wide(rest_narrow, (wide_rest_plan,), [query_wide], wide_sources, False)[0]
    side = {s: around(side[s], "x", -s) for s in NARROW_ORDER}
    made = merge(
        place,
        mix_lambda,
        (
            [diag_wide, rest_wide] + [sent[d] for d in WIDE_ORDER],
            [diag_narrow, rest_narrow] + [side[s] for s in NARROW_ORDER],
        ),
        (width_wide, width_narrow),
    )
    return made, values


def project_kernel(
    token_of, mine, weight_wide, weight_narrow, residual, gain, stream_out, rows_out,
    weights, left, total, flat_scr, rows, sems,
):
    heads, tokens, _ = mine.shape
    depth, model = weight_wide.shape
    wide = depth // heads
    tiles = model // LANES
    part = weights.shape[1]
    parts = weights.shape[0]
    for k in range(parts):
        if k * part < depth:
            source = weight_wide.at[pl.ds(k * part, part), :]
        else:
            source = weight_narrow.at[pl.ds(k * part - depth, part), :]
        pltpu.make_async_copy(source, weights.at[k], sems.at[k]).start()
    joined = jnp.concatenate(
        [mine[h, :, :wide] for h in range(heads)] + [mine[h, :, wide:] for h in range(heads)], axis=1
    )
    for k in range(parts):
        left[k] = joined[:, k * part : (k + 1) * part]
    total[...] = residual[...].astype(jnp.float32)

    def add_part(k, _):
        pltpu.make_async_copy(
            weight_wide.at[pl.ds(0, part), :], weights.at[k], sems.at[k]
        ).wait()
        total[...] = total[...] + jnp.dot(
            left[k], weights[k], preferred_element_type=jnp.float32
        )
        return 0

    lax.fori_loop(0, parts, add_part, 0)
    rounded = total[...].astype(jnp.bfloat16)
    stream_out[...] = rounded
    stream = rounded.astype(jnp.float32)
    inverse = lax.rsqrt(jnp.mean(stream * stream, axis=1, keepdims=True) + 1e-06)
    for j in range(tiles):
        lanes = slice(j * LANES, (j + 1) * LANES)
        flat_scr[pl.ds(j, tokens, stride=tiles), :] = stream[:, lanes] * inverse * gain[:, lanes]
    rows[...] = flat_scr[...].reshape(tokens, tiles, LANES).astype(jnp.bfloat16)

    def copy_row(slot, _):
        rows_out[slot] = rows[token_of[slot]]
        return 0

    lax.fori_loop(0, rows_out.shape[0], copy_row, 0, unroll=16)


def project(token_of, mine, weight_wide, weight_narrow, residual, gain):
    heads, tokens, depth = mine.shape
    model = weight_wide.shape[1]
    slots = token_of.shape[0]
    tiles = model // LANES
    part = 2 * BLOCK
    parts = heads * depth // part
    return pl.pallas_call(
        project_kernel,
        out_shape=(
            jax.ShapeDtypeStruct((tokens, model), jnp.bfloat16),
            jax.ShapeDtypeStruct((slots, tiles, LANES), jnp.bfloat16),
        ),
        in_specs=[
            pl.BlockSpec(memory_space=pltpu.SMEM),
            pl.BlockSpec(memory_space=pltpu.VMEM),
            pl.BlockSpec(memory_space=pltpu.HBM),
            pl.BlockSpec(memory_space=pltpu.HBM),
            pl.BlockSpec(memory_space=pltpu.VMEM),
            pl.BlockSpec(memory_space=pltpu.VMEM),
        ],
        out_specs=(pl.BlockSpec(memory_space=pltpu.VMEM),) * 2,
        scratch_shapes=[
            pltpu.VMEM((parts, part, model), jnp.bfloat16),
            pltpu.VMEM((parts, tokens, part), jnp.bfloat16),
            pltpu.VMEM((tokens, model), jnp.float32),
            pltpu.VMEM((tokens * tiles, LANES), jnp.float32),
            pltpu.VMEM((tokens, tiles, LANES), jnp.bfloat16),
            pltpu.SemaphoreType.DMA((parts,)),
        ],
        compiler_params=pltpu.CompilerParams(vmem_limit_bytes=48 * 1024 * 1024),
        name="project",
    )(token_of, mine, weight_wide, weight_narrow, residual, gain)


def expert_kernel(arrived, gate, up, down, out, flat, rows, hidden):
    count, tiles, _ = arrived.shape

    def spread(k, _):
        some = arrived[pl.ds(k * SOME, SOME)].astype(jnp.float32)
        flat[pl.ds(pl.multiple_of(k * SOME * tiles, LANES), SOME * tiles), :] = some.reshape(
            SOME * tiles, LANES
        )
        return 0

    def gathered(k, _):
        some = flat[pl.ds(pl.multiple_of(k * SOME * tiles, LANES), SOME * tiles), :]
        out[pl.ds(k * SOME, SOME)] = some.reshape(SOME, tiles, LANES).astype(jnp.bfloat16)
        return 0

    lax.fori_loop(0, count // SOME, spread, 0)
    for j in range(tiles):
        rows[:, j * LANES : (j + 1) * LANES] = flat[pl.ds(j, count, stride=tiles), :].astype(
            jnp.bfloat16
        )

    gate_part = jnp.dot(rows[...], gate[...], preferred_element_type=jnp.float32)
    up_part = jnp.dot(rows[...], up[...], preferred_element_type=jnp.float32)
    hidden[...] = (gate_part * jax.nn.sigmoid(gate_part) * up_part).astype(jnp.bfloat16)
    result = jnp.dot(hidden[...], down[...], preferred_element_type=jnp.float32)
    for j in range(tiles):
        flat[pl.ds(j, count, stride=tiles), :] = result[:, j * LANES : (j + 1) * LANES]
    lax.fori_loop(0, count // SOME, gathered, 0)


def experts(arrived, gate, up, down):
    count, tiles, _ = arrived.shape
    model, inner = gate.shape
    return pl.pallas_call(
        expert_kernel,
        out_shape=jax.ShapeDtypeStruct(arrived.shape, jnp.bfloat16),
        in_specs=[pl.BlockSpec(memory_space=pltpu.VMEM)] * 4,
        out_specs=pl.BlockSpec(memory_space=pltpu.VMEM),
        scratch_shapes=[
            pltpu.VMEM((count * tiles, LANES), jnp.float32),
            pltpu.VMEM((count, model), jnp.bfloat16),
            pltpu.VMEM((count, inner), jnp.bfloat16),
        ],
        compiler_params=pltpu.CompilerParams(vmem_limit_bytes=28*1024*1024),
        name="experts",
    )(arrived, gate, up, down)


def combine_kernel(slot_of, share_of, returned, stream, out, flat):
    tokens, model = stream.shape
    tiles = model // LANES

    def one_token(token, _):
        total = share_of[2 * token] * returned[slot_of[2 * token]].astype(jnp.float32)
        total = total + share_of[2 * token + 1] * returned[slot_of[2 * token + 1]].astype(
            jnp.float32
        )
        flat[pl.ds(pl.multiple_of(token * tiles, tiles), tiles), :] = total
        return 0

    lax.fori_loop(0, tokens, one_token, 0, unroll=8)
    for j in range(tiles):
        lanes = slice(j * LANES, (j + 1) * LANES)
        out[:, lanes] = (
            stream[:, lanes].astype(jnp.float32) + flat[pl.ds(j, tokens, stride=tiles), :]
        ).astype(jnp.bfloat16)


def combine(slot_of, share_of, returned, stream):
    tokens, model = stream.shape
    return pl.pallas_call(
        combine_kernel,
        out_shape=jax.ShapeDtypeStruct(stream.shape, jnp.bfloat16),
        in_specs=[pl.BlockSpec(memory_space=pltpu.SMEM)] * 2
        + [pl.BlockSpec(memory_space=pltpu.VMEM)] * 2,
        out_specs=pl.BlockSpec(memory_space=pltpu.VMEM),
        scratch_shapes=[pltpu.VMEM((tokens * (model // LANES), LANES), jnp.float32)],
        compiler_params=pltpu.CompilerParams(vmem_limit_bytes=16 * 1024 * 1024),
        name="combine",
    )(slot_of, share_of, returned, stream)


def slot_tables(expert_ids, experts_all, capacity):
    flat_expert = expert_ids.reshape(-1)
    order = jnp.arange(flat_expert.shape[0], dtype=jnp.int32)
    earlier = (flat_expert[:, None] == flat_expert[None, :]) & (order[None, :] < order[:, None])
    slot_of = flat_expert * capacity + jnp.sum(earlier.astype(jnp.int32), axis=1)
    slot_ids = jnp.arange(experts_all * capacity, dtype=jnp.int32)
    placed = slot_ids[:, None] == slot_of[None, :]
    token_of = jnp.sum(jnp.where(placed, order[None, :] // 2, 0), axis=1)
    return slot_of, token_of


def shards(
    query_wide,
    key_wide,
    value_wide,
    query_narrow,
    key_narrow,
    value_narrow,
    mix_lambda,
    residual_in,
    out_wide,
    out_narrow,
    ffn_gain,
    expert_ids,
    expert_weights,
    gate_weight,
    up_weight,
    down_weight,
):
    heads, packed = attention(
        query_wide[:, 0],
        key_wide[:, 0],
        value_wide[:, 0],
        query_narrow[:, 0],
        key_narrow[:, 0],
        value_narrow[:, 0],
        mix_lambda,
    )
    tp_size = lax.axis_size(TP)
    local_rows = heads.shape[0] // tp_size
    experts_all = lax.axis_size(SP_TP)
    capacity = max(2, 4 * local_rows // experts_all)
    slot_of, token_of = slot_tables(expert_ids, experts_all, capacity)
    out_wide, out_narrow, _ = lax.optimization_barrier((out_wide, out_narrow, packed))
    whole_wide = lax.all_gather(out_wide, TP, axis=0, tiled=True)
    whole_narrow = lax.all_gather(out_narrow, TP, axis=0, tiled=True)
    mine = lax.all_to_all(
        heads.reshape(tp_size, local_rows, -1), TP, split_axis=0, concat_axis=0, tiled=True
    )
    stream, outgoing = project(
        token_of, mine, whole_wide, whole_narrow, residual_in, ffn_gain[None, :]
    )

    def exchanged(rows):
        shape = rows.shape
        moved = lax.all_to_all(
            rows.reshape(experts_all, -1, LANES), SP_TP, split_axis=0, concat_axis=0, tiled=True
        )
        return moved.reshape(shape)

    result = experts(exchanged(outgoing), gate_weight[0], up_weight[0], down_weight[0])
    return combine(slot_of, expert_weights.reshape(-1), exchanged(result), stream)


def solution(mesh):
    finer = Mesh(mesh.devices.reshape(4, 4, 4, 2), SP_TP)
    sp = ("z", "x")
    placed = (
        P(sp, TP, None),
        P(sp, TP, None),
        P(sp, TP, None),
        P(sp, TP, None),
        P(sp, TP, None),
        P(sp, TP, None),
        P(None, TP),
        P(SP_TP, None),
        P(TP, None),
        P(TP, None),
        P(),
        P(SP_TP, None),
        P(SP_TP, None),
        P(SP_TP, None, None),
        P(SP_TP, None, None),
        P(SP_TP, None, None),
    )
    return jax.shard_map(
        shards, mesh=finer, in_specs=placed, out_specs=P(SP_TP, None), check_vma=False
    )
```
